32 devices in a mesh: sp: 4 (over z), fs: 4 (over y, x), tp: 2 (over core).
Axes of the slice: x: 2, y: 2, z: 4, core: 2. Of those that a mesh axis runs over, the one named last changes fastest.
Arguments:
- tokens: bfloat16 [4, 1024, 2048], P('fs', ('sp', 'tp')), may hold values from -6 to 6
- query_weight: bfloat16 [2048, 2048], P(('sp', 'fs'), 'tp'), may hold values from -0.125 to 0.125
- forget_weight: bfloat16 [2048, 2048], P(('sp', 'fs'), 'tp'), may hold values from -0.125 to 0.125
- value_weight: bfloat16 [2048, 2048], P(('sp', 'fs'), 'tp'), may hold values from -0.125 to 0.125
- convolution_gate_weight: bfloat16 [2048, 1024], P(('sp', 'fs'), 'tp'), may hold values from -0.125 to 0.125
- convolution_multiplier_weight: bfloat16 [2048, 1024], P(('sp', 'fs'), 'tp'), may hold values from -0.125 to 0.125
- convolution_input_weight: bfloat16 [2048, 1024], P(('sp', 'fs'), 'tp'), may hold values from -0.125 to 0.125
- gate_headroom: float32 [2048], P('tp'), may hold values from 9.765625e-05 to 0.06
- added_log_rate: float32 [4, 16, 1024], P('fs', 'tp', 'sp'), may hold values from -1.6 to 0
- initial_state: float32 [4, 16, 128, 128], P('fs', 'tp'), may hold values from -0.5 to 0.5
- head_norm_gain: float32 [2048], P('tp'), may hold values from 0.1 to 1.9
- convolution_taps: float32 [3, 1024], P(None, 'tp'), may hold values from -3.5 to 3.5
- convolution_bias: float32 [1024], P('tp'), may hold values from -4 to 4
- recurrence_output_weight: bfloat16 [2048, 2048], P('tp', ('sp', 'fs')), may hold values from -0.109375 to 0.109375
- convolution_output_weight: bfloat16 [1024, 2048], P('tp', ('sp', 'fs')), may hold values from -0.109375 to 0.109375
Outputs:
- mixed: bfloat16 [4, 1024, 2048], P('fs', ('sp', 'tp'))
The draws below stay inside these ranges and needn't reach their ends.
All inputs are finite; a program needn't handle non-finite values.
Results may differ from the reference program's by a relative error of at most 0.018.
Values may be sent and summed in bfloat16 or wider, within the bound.
A program may use at most 64 MiB of HBM per device.

```python
import jax
import jax.numpy as jnp
from jax import lax

D = 2048
RECURRENCE_HEADS = 16
DK = 128
CV = 1024
KW = 3
BLOCK_POSITIONS = 64
TOK = 256
HK = 2048
SEQ = 1024
BATCH = 4
N_TP = 2


def draw_gate_headroom(key, part):
    key_order, key_slow, key_fast = jax.random.split(jax.random.fold_in(key, 11), 3)
    head_order = jax.random.permutation(key_order, RECURRENCE_HEADS)
    slow_count = RECURRENCE_HEADS // 2
    slow_low = 0.25
    slow_high = 1.0
    slow_head = head_order < slow_count
    unit_slow = jax.random.uniform(key_slow, (RECURRENCE_HEADS, DK), jnp.float32)
    unit_fast = jax.random.uniform(key_fast, (RECURRENCE_HEADS, DK), jnp.float32)
    slow_gap = jnp.exp(jnp.log(slow_low) + unit_slow * (jnp.log(slow_high) - jnp.log(slow_low))) / SEQ
    fast_gap = jnp.exp(jnp.log(0.02) + unit_fast * (jnp.log(0.06) - jnp.log(0.02)))
    return jnp.where(slow_head[:, None], slow_gap, fast_gap).reshape(RECURRENCE_HEADS * DK).astype(jnp.float32)


def draw_added_log_rate(key, part):
    key_rate, key_spot, key_kept = jax.random.split(jax.random.fold_in(key, 23), 3)
    span_count = SEQ // TOK
    rate_low = 0.25
    rate_high = 1.0
    block_unit = jax.random.uniform(key_rate, (BATCH, 1, span_count, 1), jnp.float32)
    block_rate = jnp.exp(jnp.log(rate_low) + block_unit * (jnp.log(rate_high) - jnp.log(rate_low))) / SEQ
    stable_part = jnp.broadcast_to(-block_rate, (BATCH, RECURRENCE_HEADS, span_count, TOK)).reshape(BATCH, RECURRENCE_HEADS, SEQ)
    spots = jax.random.randint(key_spot, (BATCH, RECURRENCE_HEADS, 2), 0, SEQ)
    retained_fraction = jax.random.uniform(key_kept, (BATCH, RECURRENCE_HEADS, 2), jnp.float32, minval=0.5, maxval=0.8)
    at_location = jnp.arange(SEQ)[None, None, :, None] == spots[:, :, None, :]
    extra_log_rate = jnp.sum(jnp.where(at_location, jnp.log(retained_fraction)[:, :, None, :], 0.0), axis=-1)
    return (stable_part + extra_log_rate).astype(jnp.float32)


def block_scale(own_key, extent, cuts, low, largest):
    loudness, own = 1.0, jax.random.fold_in(own_key, 6)
    for dim, shards_of in cuts:
        draws = jnp.exp(jax.random.uniform(jax.random.fold_in(own, dim), (shards_of,), jnp.float32, low / len(cuts), largest / len(cuts)))
        loudness = loudness * jnp.repeat(draws, extent[dim] // shards_of).reshape([-1 if axis == dim else 1 for axis in range(len(extent))])
    return loudness


def bell_draw(key, dims, scale, limit, cuts=(), kind=jnp.bfloat16):
    gain = block_scale(key, dims, cuts, -0.22, 0.18) if cuts else 1.0
    entries = jax.random.normal(key, dims, jnp.float32) * scale * gain
    return jnp.minimum(jnp.maximum(entries, -limit), limit).astype(kind)


def setup_inputs(seed: int = 0) -> dict:
    streams_of = jax.random.split(jax.random.key(seed), 16)
    tokens = bell_draw(streams_of[0], (BATCH, SEQ, D), 1.0, 6.0, ((0, 4), (1, 8)))
    query_weight = bell_draw(streams_of[1], (D, HK), D ** -0.5, 0.125, ((0, 16), (1, 2)))
    forget_weight = bell_draw(streams_of[2], (D, HK), D ** -0.5, 0.125, ((0, 16), (1, 2)))
    value_weight = bell_draw(streams_of[3], (D, HK), D ** -0.5, 0.125, ((0, 16), (1, 2)))
    convolution_gate_weight = bell_draw(streams_of[4], (D, CV), D ** -0.5, 0.125, ((0, 16), (1, 2)))
    convolution_multiplier_weight = bell_draw(streams_of[5], (D, CV), D ** -0.5, 0.125, ((0, 16), (1, 2)))
    convolution_input_weight = bell_draw(streams_of[6], (D, CV), D ** -0.5, 0.125, ((0, 16), (1, 2)))
    gate_headroom = draw_gate_headroom(jax.random.fold_in(streams_of[15], 71), 0)
    added_log_rate = draw_added_log_rate(jax.random.fold_in(streams_of[15], 71), 0)
    initial_state = bell_draw(streams_of[9], (BATCH, RECURRENCE_HEADS, DK, DK), (SEQ ** -0.5), 0.5, ((0, 4), (1, 2)), jnp.float32)
    head_norm_gain = jnp.clip(1.0 + 0.18 * jax.random.normal(streams_of[10], (HK,), jnp.float32), 0.1, 1.9)
    convolution_taps = bell_draw(streams_of[11], (KW, CV), KW ** -0.5, 3.5, ((1, 2),), jnp.float32)
    convolution_bias = bell_draw(streams_of[12], (CV,), 1.0, 4.0, ((0, 2),), jnp.float32)
    recurrence_output_weight = bell_draw(streams_of[13], (HK, D), (HK + CV) ** -0.5, 0.109375, ((0, 2), (1, 16)))
    convolution_output_weight = bell_draw(streams_of[14], (CV, D), (HK + CV) ** -0.5, 0.109375, ((0, 2), (1, 16)))
    return {"tokens": tokens, "query_weight": query_weight, "forget_weight": forget_weight, "value_weight": value_weight, "convolution_gate_weight": convolution_gate_weight, "convolution_multiplier_weight": convolution_multiplier_weight, "convolution_input_weight": convolution_input_weight, "gate_headroom": gate_headroom, "added_log_rate": added_log_rate, "initial_state": initial_state, "head_norm_gain": head_norm_gain, "convolution_taps": convolution_taps, "convolution_bias": convolution_bias, "recurrence_output_weight": recurrence_output_weight, "convolution_output_weight": convolution_output_weight}


def project(sequence_rows, weight):
    return jnp.dot(sequence_rows, weight, preferred_element_type=jnp.float32).astype(jnp.bfloat16)

def to_blocks(values, number_of_blocks):
    return jnp.transpose(values.reshape(number_of_blocks, BLOCK_POSITIONS, RECURRENCE_HEADS, DK), (2, 0, 1, 3))

def gated_recurrence(query_vectors, forget_logits, value_vectors, gate_headroom, extra_rates, opening_state):
    length = query_vectors.shape[0]
    number_of_blocks = length // BLOCK_POSITIONS
    query_scaled = to_blocks(query_vectors.astype(jnp.float32), number_of_blocks) * DK ** (-0.5)
    gated_key = to_blocks(gate_headroom[None, :] * jax.nn.sigmoid(-forget_logits.astype(jnp.float32)), number_of_blocks)
    forget_log_rate = jnp.log1p(-gated_key) + extra_rates.reshape(RECURRENCE_HEADS, number_of_blocks, BLOCK_POSITIONS)[..., None]
    values = to_blocks(value_vectors.astype(jnp.float32), number_of_blocks)
    cumulative = jnp.cumsum(forget_log_rate, axis=2)
    query_decayed = query_scaled * jnp.exp(cumulative)
    key_decayed = gated_key * jnp.exp(-cumulative)
    scores = jnp.einsum('hnik,hnjk->hnij', query_decayed, key_decayed, precision=lax.Precision.HIGHEST)
    causal = jnp.tril(jnp.ones((BLOCK_POSITIONS, BLOCK_POSITIONS), dtype=bool))
    scores = jnp.where(causal, scores, 0.0)
    within = jnp.einsum('hnij,hnjv->hniv', scores, values, precision=lax.Precision.HIGHEST)
    final_log = cumulative[:, :, -1:, :]
    contrib = jnp.einsum('hnck,hncv->hnkv', gated_key * jnp.exp(final_log - cumulative), values, precision=lax.Precision.HIGHEST)
    decays = jnp.exp(final_log[:, :, 0, :])

    def advance(current, block_pair):
        return (block_pair[0][..., None] * current + block_pair[1], current)
    _, entering = lax.scan(advance, opening_state, (jnp.moveaxis(decays, 1, 0), jnp.moveaxis(contrib, 1, 0)))
    entering = jnp.moveaxis(entering, 0, 1)
    carried_term = jnp.einsum('hnck,hnkv->hncv', query_decayed, entering, precision=lax.Precision.HIGHEST)
    return jnp.transpose(within + carried_term, (1, 2, 0, 3)).reshape(length, RECURRENCE_HEADS, DK)

def reference(tokens, query_weight, forget_weight, value_weight, convolution_gate_weight, convolution_multiplier_weight, convolution_input_weight, gate_headroom, added_log_rate, initial_state, head_norm_gain, convolution_taps, convolution_bias, recurrence_output_weight, convolution_output_weight):

    def single_sequence(input_rows):
        sequence_rows, extra_rates, opening_state = input_rows
        length = sequence_rows.shape[0]
        query_vectors = project(sequence_rows, query_weight)
        forget_logits = project(sequence_rows, forget_weight)
        value_vectors = project(sequence_rows, value_weight)
        conv_gate = project(sequence_rows, convolution_gate_weight)
        conv_mult = project(sequence_rows, convolution_multiplier_weight)
        conv_input = project(sequence_rows, convolution_input_weight)
        recurrence_unnormed = gated_recurrence(query_vectors, forget_logits, value_vectors, gate_headroom, extra_rates, opening_state)
        mean_square = lax.optimization_barrier(jnp.mean(recurrence_unnormed * recurrence_unnormed, axis=-1, keepdims=True))
        rec_out = recurrence_unnormed * lax.rsqrt(mean_square + 1e-06) * head_norm_gain.reshape(RECURRENCE_HEADS, DK)
        rec_out = rec_out.reshape(length, HK).astype(jnp.bfloat16)
        conv_prod = conv_mult.astype(jnp.float32) * conv_input.astype(jnp.float32)
        padded = jnp.concatenate([jnp.zeros((KW - 1, CV), jnp.float32), conv_prod], axis=0)
        conv_y = jnp.broadcast_to(convolution_bias[None, :], (length, CV))
        for j in range(KW):
            conv_y = conv_y + convolution_taps[j][None, :] * padded[j:j + length]
        conv_out = (conv_gate.astype(jnp.float32) * conv_y).astype(jnp.bfloat16)
        rec_group = HK // N_TP
        conv_group = CV // N_TP
        running = jnp.zeros((length, D), jnp.float32)
        for g in range(N_TP):
            partial_value = jnp.dot(rec_out[:, g * rec_group:(g + 1) * rec_group], recurrence_output_weight[g * rec_group:(g + 1) * rec_group], preferred_element_type=jnp.float32)
            partial_value = partial_value + jnp.dot(conv_out[:, g * conv_group:(g + 1) * conv_group], convolution_output_weight[g * conv_group:(g + 1) * conv_group], preferred_element_type=jnp.float32)
            running = running + lax.optimization_barrier(partial_value.astype(jnp.bfloat16)).astype(jnp.float32)
        return running.astype(jnp.bfloat16)
    return lax.map(single_sequence, (tokens, added_log_rate, initial_state))
```

```python
import functools

import jax
import jax.numpy as jnp
from jax import lax
from jax.experimental import pallas as pl
from jax.experimental.pallas import tpu as pltpu
from jax.sharding import PartitionSpec as P

DK = 128
KW = 3
BLOCK_POSITIONS = 64


def carried_in(part, axis, combine, identity):
    place = lax.axis_index(axis)
    gathered = jax.tree.map(lambda a: lax.all_gather(a, axis), part)
    state = jax.tree.map(lambda a, e: jnp.zeros_like(a) + jnp.asarray(e, a.dtype), part, identity)

    def one(hop, state):
        return combine(
            state, jax.tree.map(lambda a: lax.dynamic_index_in_dim(a, hop, 0, False), gathered)
        )

    return lax.fori_loop(0, place, one, state)


def from_behind(block, axis, distance):
    devices = range(lax.axis_size(axis))
    route = [(i - distance, i) for i in devices if i - distance in devices]
    return lax.ppermute(block, axis, route)


def to_blocks(values, number_of_heads):
    number_of_blocks = values.shape[0] // BLOCK_POSITIONS
    return jnp.transpose(
        values.reshape(number_of_blocks, BLOCK_POSITIONS, number_of_heads, DK), (2, 0, 1, 3)
    )


def within_block_recurrence(
    query_vectors, forget_logits, value_vectors, gate_headroom, extra_rates
):
    number_of_heads = extra_rates.shape[0]
    number_of_blocks = query_vectors.shape[0] // BLOCK_POSITIONS
    query_scaled = to_blocks(query_vectors.astype(jnp.float32), number_of_heads) * DK ** (-0.5)
    gated_key = to_blocks(
        gate_headroom[None, :] * jax.nn.sigmoid(-forget_logits.astype(jnp.float32)), number_of_heads
    )
    forget_log_rate = (
        jnp.log1p(-gated_key)
        + extra_rates.reshape(number_of_heads, number_of_blocks, BLOCK_POSITIONS)[..., None]
    )
    values = to_blocks(value_vectors.astype(jnp.float32), number_of_heads)
    cumulative = jnp.cumsum(forget_log_rate, axis=2)
    query_decayed = query_scaled * jnp.exp(cumulative)
    key_decayed = gated_key * jnp.exp(-cumulative)
    scores = jnp.einsum(
        "hnik,hnjk->hnij", query_decayed, key_decayed, precision=lax.Precision.HIGHEST
    )
    causal = jnp.tril(jnp.ones((BLOCK_POSITIONS, BLOCK_POSITIONS), dtype=bool))
    scores = jnp.where(causal, scores, 0.0)
    within = jnp.einsum("hnij,hnjv->hniv", scores, values, precision=lax.Precision.HIGHEST)
    final_log = cumulative[:, :, -1, :]
    contrib = jnp.einsum(
        "hnck,hncv->hnkv",
        gated_key * jnp.exp(final_log[:, :, None, :] - cumulative),
        values,
        precision=lax.Precision.HIGHEST,
    )
    decays = jnp.exp(final_log)

    def advance(current, block_pair):
        return (block_pair[0][..., None] * current + block_pair[1], current)

    empty_state = jnp.zeros((number_of_heads, DK, DK), jnp.float32)
    local_total, entering = lax.scan(
        advance, empty_state, (jnp.moveaxis(decays, 1, 0), jnp.moveaxis(contrib, 1, 0))
    )
    entering = jnp.moveaxis(entering, 0, 1)
    before = jnp.exp(jnp.cumsum(final_log, axis=1) - final_log)
    device_decay = jnp.exp(jnp.sum(final_log, axis=1))
    return (query_decayed, within, entering, before, device_decay, local_total)


def finish(query_decayed, within, entering, before, carried, head_norm_gain):
    number_of_heads = query_decayed.shape[0]
    states = entering + before[..., None] * carried[:, None]
    carried_term = jnp.einsum(
        "hnck,hnkv->hncv", query_decayed, states, precision=lax.Precision.HIGHEST
    )
    length = query_decayed.shape[1] * BLOCK_POSITIONS
    recurrence_unnormed = jnp.transpose(within + carried_term, (1, 2, 0, 3)).reshape(
        length, number_of_heads, DK
    )
    mean_square = jnp.mean(recurrence_unnormed * recurrence_unnormed, axis=-1, keepdims=True)
    rec_out = (
        recurrence_unnormed
        * lax.rsqrt(mean_square + 1e-06)
        * head_norm_gain.reshape(number_of_heads, DK)
    )
    return rec_out.reshape(length, number_of_heads * DK).astype(jnp.bfloat16)


def chain_combine(earlier_part, later_part):
    return (
        earlier_part[0] * later_part[0],
        later_part[0][..., None] * earlier_part[1] + later_part[1],
    )


def shards(
    tokens,
    query_weight,
    forget_weight,
    value_weight,
    convolution_gate_weight,
    convolution_multiplier_weight,
    convolution_input_weight,
    gate_headroom,
    added_log_rate,
    initial_state,
    head_norm_gain,
    convolution_taps,
    convolution_bias,
    recurrence_output_weight,
    convolution_output_weight,
):
    own_rows = tokens[0]
    gathered = (
        lax.all_gather(query_weight, ("sp", "fs"), axis=0, tiled=True),
        lax.all_gather(forget_weight, ("sp", "fs"), axis=0, tiled=True),
        lax.all_gather(value_weight, ("sp", "fs"), axis=0, tiled=True),
        lax.all_gather(convolution_gate_weight, ("sp", "fs"), axis=0, tiled=True),
        lax.all_gather(convolution_multiplier_weight, ("sp", "fs"), axis=0, tiled=True),
        lax.all_gather(convolution_input_weight, ("sp", "fs"), axis=0, tiled=True),
        lax.all_gather(recurrence_output_weight, ("sp", "fs"), axis=1, tiled=True),
        lax.all_gather(convolution_output_weight, ("sp", "fs"), axis=1, tiled=True),
    )
    in_weights = gathered[:6]
    out_rec = gathered[6]
    out_conv = gathered[7]
    block_rows = lax.all_gather(own_rows, "tp", axis=0, tiled=True)
    projected = jnp.concatenate(
        [
            jnp.dot(block_rows, weight, preferred_element_type=jnp.float32).astype(jnp.bfloat16)
            for weight in in_weights
        ],
        axis=1,
    )
    rec_width = query_weight.shape[1]
    conv_width = convolution_gate_weight.shape[1]
    query_vectors = projected[:, :rec_width]
    forget_logits = projected[:, rec_width : 2 * rec_width]
    value_vectors = projected[:, 2 * rec_width : 3 * rec_width]
    conv_base = 3 * rec_width
    conv_gate = projected[:, conv_base : conv_base + conv_width]
    conv_mult = projected[:, conv_base + conv_width : conv_base + 2 * conv_width]
    conv_input = projected[:, conv_base + 2 * conv_width : conv_base + 3 * conv_width]
    query_decayed, within, entering, before, device_decay, local_total = within_block_recurrence(
        query_vectors, forget_logits, value_vectors, gate_headroom, added_log_rate[0]
    )
    conv_prod = conv_mult.astype(jnp.float32) * conv_input.astype(jnp.float32)
    length = conv_prod.shape[0]
    tail_rows = conv_prod[length - (KW - 1) :]
    unit_decay = jnp.ones_like(device_decay)
    empty_state = jnp.zeros_like(local_total)
    prior_decay, prior_state = carried_in(
        (device_decay, local_total), "sp", chain_combine, (unit_decay, empty_state)
    )
    prior_rows = from_behind(tail_rows, "sp", 1)
    carried = prior_decay[..., None] * initial_state[0] + prior_state
    rec_out = finish(query_decayed, within, entering, before, carried, head_norm_gain)
    extended = jnp.concatenate([prior_rows, conv_prod], axis=0)
    conv_y = jnp.broadcast_to(convolution_bias[None, :], conv_prod.shape)
    for j in range(KW):
        conv_y = conv_y + convolution_taps[j][None, :] * extended[j : j + length]
    conv_out = (conv_gate.astype(jnp.float32) * conv_y).astype(jnp.bfloat16)
    mixed = lax.psum_scatter(
        (
            jnp.dot(rec_out, out_rec, preferred_element_type=jnp.float32)
            + jnp.dot(conv_out, out_conv, preferred_element_type=jnp.float32)
        ).astype(jnp.bfloat16),
        "tp",
        scatter_dimension=0,
        tiled=True,
    )
    return mixed[None]


MESH = pl.DeviceIdType.MESH
F32 = jnp.float32
BF16 = jnp.bfloat16
CONTRACT_LAST = (((1,), (1,)), ((), ()))
CONTRACT_FIRST = (((0,), (0,)), ((), ()))
TOKEN_PIECES = 4
OUT_PIECES = 4


def layer_kernel(
    n_sp, n_fs, tok, wq, wf, wv, cg, cm, ci, ro, co, rate, init, headroom, gain, taps, bias,
    out, tokens, win, wout, rates, first_state, state, ext, both, sib_send, sib_recv, mine, z_send,
    z_recv, rl_recv, loc_sem, send_sem, win_z, wout_z, win_f, wout_f, tok_z, tok_t, rate_z, up_send,
    down_send, own_send, tok_t_send, sib_sem, sib_out, zr_sem, rl_sem, rs_send,
):
    sp, fs, tp = lax.axis_index("sp"), lax.axis_index("fs"), lax.axis_index("tp")
    other = 1 - tp
    rows = wq.shape[0]
    rec = wq.shape[1] // n_sp
    con = cg.shape[1] // n_sp
    span = tok.shape[0]
    heads = rec // DK
    wide = tok.shape[1]
    lanes_out = ro.shape[1]
    chunks, chunk = mine.shape[1], mine.shape[3]
    sub = span // TOKEN_PIECES

    def peer(**where):
        return {"sp": where.get("sp", sp), "fs": where.get("fs", fs), "tp": where.get("tp", tp)}

    def z_at(k):
        place, bit = sp, 1
        while bit < n_sp:
            if k & bit:
                place = place + bit * (1 - 2 * lax.rem(sp // bit, 2))
            bit *= 2
        return place

    half_ring = n_fs // 2

    def ring(p):
        return p + (p // half_ring) * (3 * half_ring - 1 - 2 * p)

    at_ring = ring(fs)
    left = ring(lax.rem(at_ring + n_fs - 1, n_fs))
    right = ring(lax.rem(at_ring + 1, n_fs))
    across = ring(lax.rem(at_ring + 2, n_fs))
    sibling = peer(tp=other)

    parts = []
    at = 0
    for ref, width in ((wq, rec), (wf, rec), (wv, rec), (cg, con), (cm, con), (ci, con)):
        parts.append((ref, at, width))
        at += width

    def in_rows(s, f, first, count):
        return win.at[pl.ds(pl.multiple_of((s * n_fs + f) * rows + first, count), count)]

    def in_piece(s, f, at, width):
        first = pl.multiple_of((s * n_fs + f) * rows, rows)
        return win.at[pl.ds(first, rows), pl.ds(at, width)]

    def out_piece(s, f, at, width):
        first = pl.multiple_of((s * n_fs + f) * lanes_out, lanes_out)
        return wout.at[pl.ds(at, width), pl.ds(first, lanes_out)]

    def in_sources(s):
        return [
            (ref.at[:, pl.ds(pl.multiple_of(s * width, width), width)], at, width)
            for ref, at, width in parts
        ]

    def out_sources(s):
        return [
            (ro.at[pl.ds(pl.multiple_of(s * rec, rec), rec)], 0, rec),
            (co.at[pl.ds(pl.multiple_of(s * con, con), con)], rec, con),
        ]

    local = [(ref, in_piece(sp, fs, at, width)) for ref, at, width in in_sources(sp)]
    local += [(ref, out_piece(sp, fs, at, width)) for ref, at, width in out_sources(sp)]
    local.append((tok, tokens.at[sp * 2 + tp]))
    local.append((rate, rates.at[sp]))
    local.append((init.at[pl.ds(sp * heads, heads)], first_state))
    local = [pltpu.make_async_copy(*pair, loc_sem.at[i]) for i, pair in enumerate(local)]
    for copy in local:
        copy.start()

    barrier = pltpu.get_barrier_semaphore()
    for k in range(1, n_sp):
        pl.semaphore_signal(barrier, inc=1, device_id=peer(sp=z_at(k)), device_id_type=MESH)
    for f in (left, right):
        pl.semaphore_signal(barrier, inc=1, device_id=peer(fs=f), device_id_type=MESH)
    pl.semaphore_signal(barrier, inc=1, device_id=sibling, device_id_type=MESH)
    pl.semaphore_wait(barrier, n_sp + 2)

    sent = []

    def remote(src, dst, send, recv, to):
        return pltpu.make_async_remote_copy(
            src_ref=src, dst_ref=dst, send_sem=send, recv_sem=recv, device_id=to, device_id_type=MESH,
        )

    def push(src, dst, recv, to):
        copy = remote(src, dst, send_sem.at[len(sent)], recv, to)
        copy.start()
        sent.append(copy)

    def arrived(ref, recv):
        remote(ref, ref, send_sem.at[0], recv, sibling).wait_recv()

    def tok_piece(ref, c):
        return ref.at[pl.ds(c * sub, sub)]

    def token_slot(s, t, c):
        return tok_piece(tokens.at[s * 2 + t], c)

    def own_tokens(send, to):
        return [
            remote(tok_piece(tok, c), token_slot(sp, tp, c), send.at[c], tok_z.at[sp, c], to)
            for c in range(TOKEN_PIECES)
        ]

    def own_up():
        return own_tokens(own_send.at[0], peer(sp=sp + 1))

    def own_down():
        return own_tokens(own_send.at[1], peer(sp=sp - 1))

    def to_sibling(s, c, src=None):
        slot = token_slot(s, tp, c)
        return remote(slot if src is None else src, slot, tok_t_send.at[s, c], tok_t.at[s, c], sibling)

    def relayed(s, c, send, to):
        slot = token_slot(s, tp, c)
        return remote(slot, slot, send.at[s, c], tok_z.at[s, c], to)

    def start_all(copies):
        for copy in copies:
            copy.start()

    for k in range(1, n_sp):
        push(rate, rates.at[sp], rate_z.at[k], peer(sp=z_at(k)))
    for k in range(1, n_sp):
        to = peer(sp=z_at(k))
        for i, (ref, at, width) in enumerate(in_sources(z_at(k))):
            push(ref, in_piece(sp, fs, at, width), win_z.at[k, i], to)
    for c in range(TOKEN_PIECES):
        to_sibling(sp, c, tok_piece(tok, c)).start()

    @pl.when(sp == 0)
    def _():
        start_all(own_up())

    @pl.when(sp > 0)
    def _():
        start_all(own_down())

    for k in range(1, n_sp):
        to = peer(sp=z_at(k))
        for i, (ref, at, width) in enumerate(out_sources(z_at(k))):
            push(ref, out_piece(sp, fs, at, width), wout_z.at[k, i], to)

    for copy in local:
        copy.wait()

    def z_in(k):
        for i, (ref, at, width) in enumerate(parts):
            arrived(in_piece(z_at(k), fs, at, width), win_z.at[k, i])

    def z_out(k):
        for i, (at, width) in enumerate(((0, rec), (rec, con))):
            arrived(out_piece(z_at(k), fs, at, width), wout_z.at[k, i])

    def ring_in(k):
        piece = in_rows(z_at(k), fs, 0, rows)
        push(piece, piece, win_f.at[0, k], peer(fs=right))
        push(piece, piece, win_f.at[1, k], peer(fs=left))

    def ring_in_on(k):
        s, half = z_at(k), rows // 2
        arrived(in_rows(s, left, 0, rows), win_f.at[0, k])
        piece = in_rows(s, left, 0, half)
        push(piece, piece, win_f.at[2, k], peer(fs=right))
        arrived(in_rows(s, right, 0, rows), win_f.at[1, k])
        piece = in_rows(s, right, half, half)
        push(piece, piece, win_f.at[3, k], peer(fs=left))

    def ring_in_end(k):
        s, half = z_at(k), rows // 2
        arrived(in_rows(s, across, 0, half), win_f.at[2, k])
        arrived(in_rows(s, across, half, half), win_f.at[3, k])

    depth = rec + con

    def ring_out(k):
        piece = out_piece(z_at(k), fs, 0, depth)
        push(piece, piece, wout_f.at[0, k], peer(fs=right))
        push(piece, piece, wout_f.at[1, k], peer(fs=left))

    def ring_out_copies(k):
        s, half = z_at(k), depth // 2
        near = out_piece(s, left, 0, half)
        far = out_piece(s, right, half, half)
        return (
            remote(near, near, up_send.at[0, n_sp + k], wout_f.at[2, k], peer(fs=right)),
            remote(far, far, up_send.at[1, n_sp + k], wout_f.at[3, k], peer(fs=left)),
        )

    def ring_out_on(k):
        s = z_at(k)
        first, second = ring_out_copies(k)
        arrived(out_piece(s, left, 0, depth), wout_f.at[0, k])
        first.start()
        arrived(out_piece(s, right, 0, depth), wout_f.at[1, k])
        second.start()

    def ring_out_end(k):
        s, half = z_at(k), depth // 2
        arrived(out_piece(s, across, 0, half), wout_f.at[2, k])
        arrived(out_piece(s, across, half, half), wout_f.at[3, k])

    def relay_up(s):
        for c in range(TOKEN_PIECES):
            arrived(token_slot(s, tp, c), tok_z.at[s, c])

            @pl.when(sp < n_sp - 1)
            def _():
                relayed(s, c, down_send, peer(sp=sp + 1)).start()

            to_sibling(s, c).start()

    def relay_down(s):
        for c in range(TOKEN_PIECES):
            arrived(token_slot(s, tp, c), tok_z.at[s, c])

            @pl.when(sp > 0)
            def _():
                relayed(s, c, down_send, peer(sp=sp - 1)).start()

            to_sibling(s, c).start()

    def relays(j):
        later_up = jnp.logical_and(j < sp, sp > 1)

        @pl.when(later_up)
        def _():
            relay_up(j)

        @pl.when(jnp.logical_and(later_up, jnp.logical_and(j == sp - 1, sp < n_sp - 1)))
        def _():
            start_all(own_up())

        later = sp + 1 + j

        @pl.when(later < n_sp)
        def _():
            relay_down(later)

    ring_in(0)
    for k in range(1, n_sp):
        if k == n_sp - 1:
            @pl.when(sp == 1)
            def _():
                relay_up(0)
                start_all(own_up())

        z_in(k)
        ring_in(k)
        ring_in_on(k - 1)
    ring_in_on(n_sp - 1)
    for k in range(n_sp):
        if k:
            z_out(k)
        ring_out(k)
    for k in range(1, n_sp):
        arrived(rates.at[z_at(k)], rate_z.at[k])
    for k in range(n_sp):
        ring_in_end(k)

    for h in range(heads):
        state[h] = first_state[h].T
    ext[0:8] = jnp.zeros((8, con), F32)
    lane_rec = pl.ds(pl.multiple_of(sp * rec, rec), rec)
    lane_con = pl.ds(pl.multiple_of(sp * con, con), con)
    row_id = lax.broadcasted_iota(jnp.int32, (span, span), 0)
    col_id = lax.broadcasted_iota(jnp.int32, (span, span), 1)
    causal = row_id >= col_id
    lower = causal.astype(F32)
    upper = (row_id <= col_id).astype(F32)
    length = 2 * span

    def sib_copy(s, c):
        return remote(sib_send.at[s, c], sib_recv.at[s, c], sib_out.at[s, c], sib_sem.at[s, c], sibling)

    def z_copy(s, c):
        return remote(z_send.at[s, c], z_recv.at[sp, c], rs_send.at[s, c], zr_sem.at[sp, c], peer(sp=s))

    def edge_copy(s, c, to):
        return remote(z_send.at[s, c], rl_recv.at[s, c], rs_send.at[s, c], rl_sem.at[s, c], peer(sp=to))

    def through_low(s):
        return jnp.logical_and(sp == 0, s >= 2)

    def through_high(s):
        return jnp.logical_and(sp == n_sp - 1, s <= n_sp - 3)

    def joins(s):
        return jnp.logical_or(
            jnp.logical_and(sp == 1, s >= 2), jnp.logical_and(sp == n_sp - 2, s <= n_sp - 3)
        )

    def plain(s):
        edge = jnp.logical_or(through_low(s), through_high(s))
        return jnp.logical_not(jnp.logical_or(jnp.logical_or(edge, joins(s)), s == sp))

    def pass_on(s):
        for c in range(chunks):
            sib_copy(s, c).wait_recv()
            total = mine[s, c] + sib_recv[s, c].astype(F32)
            mine[s, c] = total

            @pl.when(jnp.logical_not(jnp.logical_or(joins(s), s == sp)))
            def _():
                z_send[s, c] = total.astype(BF16)

            @pl.when(plain(s))
            def _():
                z_copy(s, c).start()

            @pl.when(through_low(s))
            def _():
                edge_copy(s, c, 1).start()

            @pl.when(through_high(s))
            def _():
                edge_copy(s, c, n_sp - 2).start()

    def join(s):
        for c in range(chunks):
            arrived(rl_recv.at[s, c], rl_sem.at[s, c])
            z_send[s, c] = (mine[s, c] + rl_recv[s, c].astype(F32)).astype(BF16)
            z_copy(s, c).start()

    def project_out(s):
        for c in range(chunks):
            partial = jnp.dot(
                both[s], wout[:, c * chunk : (c + 1) * chunk], preferred_element_type=F32
            )
            first = partial[:span]
            second = partial[span:]
            mine[s, c] = jnp.where(tp == 0, first, second)
            sib_send[s, c] = jnp.where(tp == 0, second, first).astype(BF16)
            sib_copy(s, c).start()

    def step(s, carry):
        relays(s)
        for c in range(TOKEN_PIECES):
            arrived(token_slot(s, other, c), tok_t.at[s, c])
        block = jnp.concatenate([tokens[2 * s], tokens[2 * s + 1]], axis=0)

        def project(at, width):
            return jnp.dot(
                block, win[:, pl.ds(at, width)], preferred_element_type=F32
            ).astype(BF16)

        query = project(0, rec).astype(F32) * DK ** (-0.5)
        forget = project(rec, rec).astype(F32)
        value = project(2 * rec, rec)
        base = 3 * rec
        conv_gate = project(base, con).astype(F32)
        prod = project(base + con, con).astype(F32) * project(base + 2 * con, con).astype(F32)
        key_gate = headroom[:, lane_rec] * jax.nn.sigmoid(-forget)
        log_forget = jnp.log1p(-key_gate)
        gains = gain[:, lane_rec]
        mine_rate = [rates[s, pl.ds(sp * heads + h, 1), :] for h in range(heads)]
        if heads < 8:
            mine_rate.append(jnp.zeros((8 - heads, 2 * span), F32))
        mine_rate = jnp.concatenate(mine_rate, axis=0)
        halves = []
        for c in range(2):
            part = slice(c * span, (c + 1) * span)
            cum = jnp.dot(lower, log_forget[part], precision=lax.Precision.HIGHEST)
            extra = jnp.dot(mine_rate[:, part], upper, precision=lax.Precision.HIGHEST)
            extra_t = extra.T
            grow = jnp.exp(cum)
            query_grow = query[part] * grow
            key_grow = (key_gate[part] / grow).astype(BF16)
            last = cum[span - 1 :, :]
            key_last = key_gate[part] * jnp.exp(last - cum)
            last_decay = jnp.exp(last)
            pieces = []
            for h in range(heads):
                lanes = slice(h * DK, (h + 1) * DK)
                row = extra[h : h + 1]
                column = extra_t[:, h : h + 1]
                end = row[:, span - 1 :]
                scores = lax.dot_general(
                    query_grow[:, lanes].astype(BF16), key_grow[:, lanes], CONTRACT_LAST,
                    preferred_element_type=F32,
                )
                decay = jnp.exp(jnp.where(causal, column - row, 0.0))
                scores = jnp.where(causal, scores * decay, 0.0).astype(BF16)
                values = value[part, lanes]
                before = state[h]
                raw = jnp.dot(scores, values, preferred_element_type=F32)
                raw = raw + lax.dot_general(
                    (query_grow[:, lanes] * jnp.exp(column)).astype(BF16), before.astype(BF16),
                    CONTRACT_LAST, preferred_element_type=F32,
                )
                keys = (key_last[:, lanes] * jnp.exp(end - column)).astype(BF16)
                state[h] = before * (last_decay[:, lanes] * jnp.exp(end)) + lax.dot_general(
                    values, keys, CONTRACT_FIRST, preferred_element_type=F32
                )
                square = jnp.mean(raw * raw, axis=-1, keepdims=True)
                pieces.append((raw * lax.rsqrt(square + 1e-06) * gains[:, lanes]).astype(BF16))
            halves.append(jnp.concatenate(pieces, axis=1))
        ext[8:] = prod
        conv = jnp.broadcast_to(bias[:, lane_con], prod.shape)
        for j in range(KW):
            conv = conv + taps[j : j + 1, lane_con] * ext[pl.ds(8 - (KW - 1) + j, length)]
        ext[0:8] = ext[length:]
        conv_out = (conv_gate * conv).astype(BF16)
        both[s] = jnp.concatenate([jnp.concatenate(halves, axis=0), conv_out], axis=1)

        @pl.when(s == 0)
        def _():
            for k in range(n_sp):
                ring_out_on(k)

        @pl.when(s == 1)
        def _():
            for k in range(n_sp):
                ring_out_end(k)

        @pl.when(s > 0)
        def _():
            project_out(s - 1)
            pass_on(s - 1)

        return carry

    lax.fori_loop(0, n_sp, step, 0)
    project_out(n_sp - 1)
    pass_on(n_sp - 1)

    @pl.when(sp == 1)
    def _():
        for s in range(2, n_sp):
            join(s)

    @pl.when(sp == n_sp - 2)
    def _():
        for s in range(n_sp - 2):
            join(s)

    for d in range(n_sp):
        comes = sp != d
        if d == 0:
            comes = jnp.logical_and(comes, sp < 2)
        if d == n_sp - 1:
            comes = jnp.logical_and(comes, sp > n_sp - 3)

        @pl.when(comes)
        def _():
            for c in range(chunks):
                arrived(z_recv.at[d, c], zr_sem.at[d, c])
                mine[sp, c] = mine[sp, c] + z_recv[d, c].astype(F32)

    for c in range(chunks):
        out[:, c * chunk : (c + 1) * chunk] = mine[sp, c].astype(BF16)

    for copy in sent:
        copy.wait_send()
    for k in range(n_sp):
        for copy in ring_out_copies(k):
            copy.wait_send()

    @pl.when(sp < n_sp - 1)
    def _():
        for copy in own_up():
            copy.wait_send()

    @pl.when(sp > 0)
    def _():
        for copy in own_down():
            copy.wait_send()

    for s in range(n_sp):
        for c in range(TOKEN_PIECES):
            to_sibling(s, c).wait_send()
            forwarded = jnp.logical_or(
                jnp.logical_and(sp > s, sp < n_sp - 1), jnp.logical_and(sp < s, sp > 0)
            )

            @pl.when(forwarded)
            def _():
                relayed(s, c, down_send, sibling).wait_send()

        for c in range(chunks):
            sib_copy(s, c).wait_send()

            @pl.when(sp != s)
            def _():
                remote(
                    z_send.at[s, c], rl_recv.at[s, c], rs_send.at[s, c], rl_sem.at[s, c], sibling
                ).wait_send()


def sequence_shards(n_sp, n_fs, *arrays):
    (tok, wq, wf, wv, cg, cm, ci, headroom, rate, init, gain, taps, bias, ro, co) = arrays
    span, wide = tok.shape[1:]
    rec, con = wq.shape[1] // n_sp, cg.shape[1] // n_sp
    heads = rec // DK
    chunk = wide // OUT_PIECES
    hbm = pl.BlockSpec(memory_space=pl.ANY)
    vmem = pl.BlockSpec(memory_space=pltpu.VMEM)
    dma = pltpu.SemaphoreType.DMA
    flat = (n_sp, OUT_PIECES, span, chunk)
    mixed = pl.pallas_call(
        functools.partial(layer_kernel, n_sp, n_fs),
        out_shape=jax.ShapeDtypeStruct((span, wide), BF16),
        in_specs=[hbm] * 11 + [vmem] * 4,
        out_specs=vmem,
        scratch_shapes=[
            pltpu.VMEM((2 * n_sp, span, wide), BF16),
            pltpu.VMEM((wide, 3 * (rec + con)), BF16),
            pltpu.VMEM((rec + con, wide), BF16),
            pltpu.VMEM((n_sp,) + rate.shape[1:], F32),
            pltpu.VMEM((heads, DK, DK), F32),
            pltpu.VMEM((heads, DK, DK), F32),
            pltpu.VMEM((8 + 2 * span, con), F32),
            pltpu.VMEM((n_sp, 2 * span, rec + con), BF16),
            pltpu.VMEM(flat, BF16),
            pltpu.VMEM(flat, BF16),
            pltpu.VMEM(flat, F32),
            pltpu.VMEM(flat, BF16),
            pltpu.VMEM(flat, BF16),
            pltpu.VMEM(flat, BF16),
            dma((11,)),
            dma(((n_sp - 1) * 9 + n_sp * 6,)),
            dma((n_sp, 6)),
            dma((n_sp, 2)),
            dma((4, n_sp)),
            dma((4, n_sp)),
            dma((n_sp, TOKEN_PIECES)),
            dma((n_sp, TOKEN_PIECES)),
            dma((n_sp,)),
            dma((2, 2 * n_sp)),
            dma((n_sp, TOKEN_PIECES)),
            dma((2, TOKEN_PIECES)),
            dma((n_sp, TOKEN_PIECES)),
            dma((n_sp, OUT_PIECES)),
            dma((n_sp, OUT_PIECES)),
            dma((n_sp, OUT_PIECES)),
            dma((n_sp, OUT_PIECES)),
            dma((n_sp, OUT_PIECES)),
        ],
        compiler_params=pltpu.CompilerParams(
            collective_id=0, has_side_effects=True, vmem_limit_bytes=60 * 2**20
        ),
    )(
        tok[0], wq, wf, wv, cg, cm, ci, ro, co, rate[0], init[0], headroom[None], gain[None],
        taps, bias[None],
    )
    return mixed[None]


def choose_plan(sizes, *arrays):
    n_sp, n_fs = sizes["sp"], sizes["fs"]
    rows, rec = arrays[1].shape
    con = arrays[4].shape[1]
    span = arrays[0].shape[1]
    even = (
        sizes["tp"] == 2
        and n_fs == 4
        and n_sp >= 4
        and n_sp & (n_sp - 1) == 0
        and arrays[0].shape[2] % (128 * OUT_PIECES) == 0
        and arrays[0].shape[0] == 1
        and rec % (n_sp * DK) == 0
        and rec // (n_sp * DK) <= 8
        and arrays[8].shape[1] % 8 == 0
        and con % (n_sp * 128) == 0
        and rows % 128 == 0
        and span == DK
        and arrays[13].shape[1] % 128 == 0
    )
    return sequence_shards(n_sp, n_fs, *arrays) if even else shards(*arrays)


def solution(mesh):
    in_specs = (
        P("fs", ("sp", "tp"), None),
        P(("sp", "fs"), "tp"),
        P(("sp", "fs"), "tp"),
        P(("sp", "fs"), "tp"),
        P(("sp", "fs"), "tp"),
        P(("sp", "fs"), "tp"),
        P(("sp", "fs"), "tp"),
        P("tp"),
        P("fs", "tp", "sp"),
        P("fs", "tp", None, None),
        P("tp"),
        P(None, "tp"),
        P("tp"),
        P("tp", ("sp", "fs")),
        P("tp", ("sp", "fs")),
    )
    out_specs = P("fs", ("sp", "tp"), None)
    body = functools.partial(choose_plan, dict(mesh.shape))
    return jax.shard_map(body, mesh=mesh, in_specs=in_specs, out_specs=out_specs, check_vma=False)
```

```python
import functools

import jax
import jax.numpy as jnp
from jax import lax
from jax.experimental import pallas as pl
from jax.experimental.pallas import tpu as pltpu
from jax.sharding import PartitionSpec as P

DK = 128
KW = 3
BLOCK_POSITIONS = 64


def carried_in(part, axis, combine, identity):
    place = lax.axis_index(axis)
    gathered = jax.tree.map(lambda a: lax.all_gather(a, axis), part)
    state = jax.tree.map(lambda a, e: jnp.zeros_like(a) + jnp.asarray(e, a.dtype), part, identity)

    def one(hop, state):
        return combine(
            state, jax.tree.map(lambda a: lax.dynamic_index_in_dim(a, hop, 0, False), gathered)
        )

    return lax.fori_loop(0, place, one, state)


def from_behind(block, axis, distance):
    devices = range(lax.axis_size(axis))
    route = [(i - distance, i) for i in devices if i - distance in devices]
    return lax.ppermute(block, axis, route)


def to_blocks(values, number_of_heads):
    number_of_blocks = values.shape[0] // BLOCK_POSITIONS
    return jnp.transpose(
        values.reshape(number_of_blocks, BLOCK_POSITIONS, number_of_heads, DK), (2, 0, 1, 3)
    )


def within_block_recurrence(
    query_vectors, forget_logits, value_vectors, gate_headroom, extra_rates
):
    number_of_heads = extra_rates.shape[0]
    number_of_blocks = query_vectors.shape[0] // BLOCK_POSITIONS
    query_scaled = to_blocks(query_vectors.astype(jnp.float32), number_of_heads) * DK ** (-0.5)
    gated_key = to_blocks(
        gate_headroom[None, :] * jax.nn.sigmoid(-forget_logits.astype(jnp.float32)), number_of_heads
    )
    forget_log_rate = (
        jnp.log1p(-gated_key)
        + extra_rates.reshape(number_of_heads, number_of_blocks, BLOCK_POSITIONS)[..., None]
    )
    values = to_blocks(value_vectors.astype(jnp.float32), number_of_heads)
    cumulative = jnp.cumsum(forget_log_rate, axis=2)
    query_decayed = query_scaled * jnp.exp(cumulative)
    key_decayed = gated_key * jnp.exp(-cumulative)
    scores = jnp.einsum(
        "hnik,hnjk->hnij", query_decayed, key_decayed, precision=lax.Precision.HIGHEST
    )
    causal = jnp.tril(jnp.ones((BLOCK_POSITIONS, BLOCK_POSITIONS), dtype=bool))
    scores = jnp.where(causal, scores, 0.0)
    within = jnp.einsum("hnij,hnjv->hniv", scores, values, precision=lax.Precision.HIGHEST)
    final_log = cumulative[:, :, -1, :]
    contrib = jnp.einsum(
        "hnck,hncv->hnkv",
        gated_key * jnp.exp(final_log[:, :, None, :] - cumulative),
        values,
        precision=lax.Precision.HIGHEST,
    )
    decays = jnp.exp(final_log)

    def advance(current, block_pair):
        return (block_pair[0][..., None] * current + block_pair[1], current)

    empty_state = jnp.zeros((number_of_heads, DK, DK), jnp.float32)
    local_total, entering = lax.scan(
        advance, empty_state, (jnp.moveaxis(decays, 1, 0), jnp.moveaxis(contrib, 1, 0))
    )
    entering = jnp.moveaxis(entering, 0, 1)
    before = jnp.exp(jnp.cumsum(final_log, axis=1) - final_log)
    device_decay = jnp.exp(jnp.sum(final_log, axis=1))
    return (query_decayed, within, entering, before, device_decay, local_total)


def finish(query_decayed, within, entering, before, carried, head_norm_gain):
    number_of_heads = query_decayed.shape[0]
    states = entering + before[..., None] * carried[:, None]
    carried_term = jnp.einsum(
        "hnck,hnkv->hncv", query_decayed, states, precision=lax.Precision.HIGHEST
    )
    length = query_decayed.shape[1] * BLOCK_POSITIONS
    recurrence_unnormed = jnp.transpose(within + carried_term, (1, 2, 0, 3)).reshape(
        length, number_of_heads, DK
    )
    mean_square = jnp.mean(recurrence_unnormed * recurrence_unnormed, axis=-1, keepdims=True)
    rec_out = (
        recurrence_unnormed
        * lax.rsqrt(mean_square + 1e-06)
        * head_norm_gain.reshape(number_of_heads, DK)
    )
    return rec_out.reshape(length, number_of_heads * DK).astype(jnp.bfloat16)


def chain_combine(earlier_part, later_part):
    return (
        earlier_part[0] * later_part[0],
        later_part[0][..., None] * earlier_part[1] + later_part[1],
    )


def shards(
    tokens,
    query_weight,
    forget_weight,
    value_weight,
    convolution_gate_weight,
    convolution_multiplier_weight,
    convolution_input_weight,
    gate_headroom,
    added_log_rate,
    initial_state,
    head_norm_gain,
    convolution_taps,
    convolution_bias,
    recurrence_output_weight,
    convolution_output_weight,
):
    own_rows = tokens[0]
    gathered = (
        lax.all_gather(query_weight, ("sp", "fs"), axis=0, tiled=True),
        lax.all_gather(forget_weight, ("sp", "fs"), axis=0, tiled=True),
        lax.all_gather(value_weight, ("sp", "fs"), axis=0, tiled=True),
        lax.all_gather(convolution_gate_weight, ("sp", "fs"), axis=0, tiled=True),
        lax.all_gather(convolution_multiplier_weight, ("sp", "fs"), axis=0, tiled=True),
        lax.all_gather(convolution_input_weight, ("sp", "fs"), axis=0, tiled=True),
        lax.all_gather(recurrence_output_weight, ("sp", "fs"), axis=1, tiled=True),
        lax.all_gather(convolution_output_weight, ("sp", "fs"), axis=1, tiled=True),
    )
    in_weights = gathered[:6]
    out_rec = gathered[6]
    out_conv = gathered[7]
    block_rows = lax.all_gather(own_rows, "tp", axis=0, tiled=True)
    projected = jnp.concatenate(
        [
            jnp.dot(block_rows, weight, preferred_element_type=jnp.float32).astype(jnp.bfloat16)
            for weight in in_weights
        ],
        axis=1,
    )
    rec_width = query_weight.shape[1]
    conv_width = convolution_gate_weight.shape[1]
    query_vectors = projected[:, :rec_width]
    forget_logits = projected[:, rec_width : 2 * rec_width]
    value_vectors = projected[:, 2 * rec_width : 3 * rec_width]
    conv_base = 3 * rec_width
    conv_gate = projected[:, conv_base : conv_base + conv_width]
    conv_mult = projected[:, conv_base + conv_width : conv_base + 2 * conv_width]
    conv_input = projected[:, conv_base + 2 * conv_width : conv_base + 3 * conv_width]
    query_decayed, within, entering, before, device_decay, local_total = within_block_recurrence(
        query_vectors, forget_logits, value_vectors, gate_headroom, added_log_rate[0]
    )
    conv_prod = conv_mult.astype(jnp.float32) * conv_input.astype(jnp.float32)
    length = conv_prod.shape[0]
    tail_rows = conv_prod[length - (KW - 1) :]
    unit_decay = jnp.ones_like(device_decay)
    empty_state = jnp.zeros_like(local_total)
    prior_decay, prior_state = carried_in(
        (device_decay, local_total), "sp", chain_combine, (unit_decay, empty_state)
    )
    prior_rows = from_behind(tail_rows, "sp", 1)
    carried = prior_decay[..., None] * initial_state[0] + prior_state
    rec_out = finish(query_decayed, within, entering, before, carried, head_norm_gain)
    extended = jnp.concatenate([prior_rows, conv_prod], axis=0)
    conv_y = jnp.broadcast_to(convolution_bias[None, :], conv_prod.shape)
    for j in range(KW):
        conv_y = conv_y + convolution_taps[j][None, :] * extended[j : j + length]
    conv_out = (conv_gate.astype(jnp.float32) * conv_y).astype(jnp.bfloat16)
    mixed = lax.psum_scatter(
        (
            jnp.dot(rec_out, out_rec, preferred_element_type=jnp.float32)
            + jnp.dot(conv_out, out_conv, preferred_element_type=jnp.float32)
        ).astype(jnp.bfloat16),
        "tp",
        scatter_dimension=0,
        tiled=True,
    )
    return mixed[None]


MESH = pl.DeviceIdType.MESH
F32 = jnp.float32
BF16 = jnp.bfloat16
CONTRACT_LAST = (((1,), (1,)), ((), ()))
CONTRACT_FIRST = (((0,), (0,)), ((), ()))
TOKEN_PIECES = 4
OUT_PIECES = 4


def layer_kernel(
    n_sp, n_fs, tok, wq, wf, wv, cg, cm, ci, ro, co, rate, init, headroom, gain, taps, bias,
    out, tokens, win, wcon, wout, rates, first_state, state, ext, both, sib_send, sib_recv, mine,
    z_send, z_recv, rl_recv, stage_in, stage_con, stage_out, loc_in, loc_con, loc_out, loc_sem,
    send_sem, in_send, win_z, wcon_z, wout_z, win_f, late_f, tok_z, tok_t, rate_z, ring_send, late_send,
    down_send, own_send, tok_t_send, sib_sem, sib_out, zr_sem, rl_sem, rs_send,
):
    sp, fs, tp = lax.axis_index("sp"), lax.axis_index("fs"), lax.axis_index("tp")
    other = 1 - tp
    rows = wq.shape[0]
    rec = wq.shape[1] // n_sp
    con = cg.shape[1] // n_sp
    span = tok.shape[0]
    heads = rec // DK
    wide = tok.shape[1]
    lanes_out = ro.shape[1]
    chunks, chunk = mine.shape[1], mine.shape[3]
    sub = span // TOKEN_PIECES
    shards_in = chunk // lanes_out

    def peer(**where):
        return {"sp": where.get("sp", sp), "fs": where.get("fs", fs), "tp": where.get("tp", tp)}

    half_ring = n_fs // 2

    def ring(p):
        return p + (p // half_ring) * (3 * half_ring - 1 - 2 * p)

    at_ring = ring(fs)
    left = ring(lax.rem(at_ring + n_fs - 1, n_fs))
    right = ring(lax.rem(at_ring + 1, n_fs))
    across = ring(lax.rem(at_ring + 2, n_fs))
    sibling = peer(tp=other)

    rec_parts = [(ref, i * rec, rec) for i, ref in enumerate((wq, wf, wv))]
    con_parts = [(ref, i * con, con) for i, ref in enumerate((cg, cm, ci))]

    def in_rows(s, f, first, count):
        return win.at[pl.ds(pl.multiple_of((s * n_fs + f) * rows + first, count), count)]

    def con_rows(s, f):
        return wcon.at[pl.ds(pl.multiple_of((s * n_fs + f) * rows, rows), rows)]

    def out_slot(s, f):
        return wout.at[s * n_fs + f]

    def stage(z, in_to, con_to, out_to, place):
        copies = []
        for some, to, sem in ((rec_parts, in_to, loc_in), (con_parts, con_to, loc_con)):
            for ref, at, width in some:
                src = ref.at[:, pl.ds(pl.multiple_of(z * width, width), width)]
                copies.append((src, to.at[:, pl.ds(at, width)], sem.at[place]))
        for ref, at, width in ((ro, 0, rec), (co, rec, con)):
            src = ref.at[pl.ds(pl.multiple_of(z * width, width), width)]
            copies.append((src, out_to.at[pl.ds(at, width)], loc_out.at[place]))
        return [pltpu.make_async_copy(*copy) for copy in copies]

    below, above = sp, n_sp - 1 - sp
    fewer = jnp.minimum(below, above)
    upward = jnp.where(below < above, 1, -1)
    edge = fewer == 0

    def near(j):
        paired = j <= 2 * fewer
        side = jnp.where(paired, upward * (1 - 2 * (j % 2)), upward)
        return sp + side * jnp.where(paired, (j + 1) // 2, j - fewer)

    def to_send(j):
        if j == 1:
            return near(1)
        return jnp.where(edge, near(n_sp + 1 - j), near(j))

    local = []
    for j in range(1, n_sp):
        local += stage(to_send(j), stage_in.at[j], stage_con.at[j], stage_out.at[j], j)
    local += stage(sp, in_rows(sp, fs, 0, rows), con_rows(sp, fs), out_slot(sp, fs), 0)
    others = [
        (tok, tokens.at[sp * 2 + tp]), (rate, rates.at[sp]),
        (init.at[pl.ds(sp * heads, heads)], first_state),
    ]
    others = [pltpu.make_async_copy(*pair, loc_sem.at[i]) for i, pair in enumerate(others)]
    for copy in local + others:
        copy.start()

    barrier = pltpu.get_barrier_semaphore()
    for j in range(1, n_sp):
        pl.semaphore_signal(barrier, inc=1, device_id=peer(sp=near(j)), device_id_type=MESH)
    for f in (left, right):
        pl.semaphore_signal(barrier, inc=1, device_id=peer(fs=f), device_id_type=MESH)
    pl.semaphore_signal(barrier, inc=1, device_id=sibling, device_id_type=MESH)
    pl.semaphore_wait(barrier, n_sp + 2)

    sent = []

    def remote(src, dst, send, recv, to):
        return pltpu.make_async_remote_copy(
            src_ref=src, dst_ref=dst, send_sem=send, recv_sem=recv, device_id=to, device_id_type=MESH,
        )

    def push(src, dst, recv, to):
        copy = remote(src, dst, send_sem.at[len(sent)], recv, to)
        copy.start()
        sent.append(copy)

    def arrived(ref, recv):
        remote(ref, ref, send_sem.at[0], recv, sibling).wait_recv()

    def tok_piece(ref, c):
        return ref.at[pl.ds(c * sub, sub)]

    def token_slot(s, t, c):
        return tok_piece(tokens.at[s * 2 + t], c)

    def own_tokens(send, to):
        return [
            remote(tok_piece(tok, c), token_slot(sp, tp, c), send.at[c], tok_z.at[sp, c], to)
            for c in range(TOKEN_PIECES)
        ]

    def own_up():
        return own_tokens(own_send.at[0], peer(sp=sp + 1))

    def own_down():
        return own_tokens(own_send.at[1], peer(sp=sp - 1))

    def to_sibling(s, c, src=None):
        slot = token_slot(s, tp, c)
        return remote(slot if src is None else src, slot, tok_t_send.at[s, c], tok_t.at[s, c], sibling)

    def relayed(s, c, send, to):
        slot = token_slot(s, tp, c)
        return remote(slot, slot, send.at[s, c], tok_z.at[s, c], to)

    def start_all(copies):
        for copy in copies:
            copy.start()

    def send_in(j):
        z = to_send(j)
        push(rate, rates.at[sp], rate_z.at[sp], peer(sp=z))
        arrived(stage_in.at[j], loc_in.at[j])
        push(stage_in.at[j], in_rows(sp, fs, 0, rows), win_z.at[sp], peer(sp=z))

    def late_copies():
        copies = []
        for j in range(1, n_sp):
            to = peer(sp=to_send(j))
            copies.append(
                remote(stage_con.at[j], con_rows(sp, fs), late_send.at[0, j], wcon_z.at[sp], to)
            )
            copies.append(
                remote(stage_out.at[j], out_slot(sp, fs), late_send.at[1, j], wout_z.at[sp], to)
            )
        return copies

    low, high = sp == 1, sp == n_sp - 2
    send_in(1)

    for j in range(2, n_sp):
        send_in(j)
    for j in range(n_sp):
        arrived(stage_con.at[j] if j else con_rows(sp, fs), loc_con.at[j])
        arrived(stage_out.at[j] if j else out_slot(sp, fs), loc_out.at[j])
    start_all(late_copies()[:2])
    for copy in others:
        copy.wait()

    @pl.when(sp == 0)
    def _():
        start_all(own_up())

    @pl.when(sp == n_sp - 1)
    def _():
        start_all(own_down())

    for c in range(TOKEN_PIECES):
        to_sibling(sp, c, tok_piece(tok, c)).start()

    arrived(in_rows(sp, fs, 0, rows), loc_in.at[0])

    def z_in(j):
        z = near(j)
        arrived(in_rows(z, fs, 0, rows), win_z.at[z])
        arrived(rates.at[z], rate_z.at[z])

    def z_late(j):
        z = near(j)
        arrived(con_rows(z, fs), wcon_z.at[z])
        arrived(out_slot(z, fs), wout_z.at[z])

    def place(j):
        return near(j) if j else sp

    def in_ring(k):
        s, half = place(k), rows // 2
        whole = in_rows(s, fs, 0, rows)
        copies = (
            (whole, right), (whole, left), (in_rows(s, left, 0, half), right),
            (in_rows(s, right, half, half), left),
        )
        return [
            remote(piece, piece, in_send.at[i, k], win_f.at[i, k], peer(fs=to))
            for i, (piece, to) in enumerate(copies)
        ]

    def ring_in(k):
        start_all(in_ring(k)[:2])

    def ring_in_on(k):
        s = place(k)
        on = in_ring(k)[2:]
        arrived(in_rows(s, left, 0, rows), win_f.at[0, k])
        on[0].start()
        arrived(in_rows(s, right, 0, rows), win_f.at[1, k])
        on[1].start()

    def ring_in_end(k):
        s, half = place(k), rows // 2
        arrived(in_rows(s, across, 0, half), win_f.at[2, k])
        arrived(in_rows(s, across, half, half), win_f.at[3, k])

    def late_ring(k):
        s = place(k)
        mine_con, mine_out = con_rows(s, fs), out_slot(s, fs)
        passed_con, passed_out = con_rows(s, left), out_slot(s, right)
        copies = (
            (mine_con, right), (mine_out, left), (mine_con, left), (mine_out, right),
            (passed_con, right), (passed_out, left),
        )
        return [
            remote(piece, piece, ring_send.at[i, k], late_f.at[i, k], peer(fs=to))
            for i, (piece, to) in enumerate(copies)
        ]

    def ring_late(k):
        start_all(late_ring(k)[:4])

    def ring_late_on(k):
        s = place(k)
        on = late_ring(k)[4:]
        arrived(con_rows(s, left), late_f.at[0, k])
        on[0].start()
        arrived(out_slot(s, right), late_f.at[1, k])
        on[1].start()

    def ring_late_end(k):
        s = place(k)
        arrived(con_rows(s, right), late_f.at[2, k])
        arrived(out_slot(s, left), late_f.at[3, k])
        arrived(con_rows(s, across), late_f.at[4, k])
        arrived(out_slot(s, across), late_f.at[5, k])

    def relay(s, c, step_by):
        arrived(token_slot(s, tp, c), tok_z.at[s, c])
        if step_by:
            relayed(s, c, down_send, peer(sp=sp + step_by)).start()
        to_sibling(s, c).start()

    def relays(when, s, step_by, pieces=range(TOKEN_PIECES)):
        @pl.when(when)
        def _():
            for c in pieces:
                relay(s, c, step_by)

    early, late = range(TOKEN_PIECES // 2), range(TOKEN_PIECES // 2, TOKEN_PIECES)
    bottom, top = 0, n_sp - 1

    def second_in():
        z_in(2)
        ring_in(2)

    def first_late():
        z_late(1)
        ring_late(1)

    inner = jnp.logical_not(edge)
    ring_in(0)
    z_in(1)
    ring_in(1)
    pl.when(inner)(second_in)
    ring_in_on(0)
    ring_late(0)

    @pl.when(low)
    def _():
        start_all(own_down())

    @pl.when(high)
    def _():
        start_all(own_up())

    ring_in_on(1)

    @pl.when(edge)
    def _():
        first_late()
        second_in()

    z_in(3)
    ring_in(3)
    start_all(late_copies()[2:])

    @pl.when(high)
    def _():
        start_all(own_down())

    pl.when(inner)(first_late)
    ring_in_on(2)
    relays(low, bottom, 1, early)
    relays(high, top, -1, early)
    ring_in_on(3)
    ring_late_on(0)
    relays(low, bottom, 1, late)
    relays(high, top, -1, late)

    @pl.when(low)
    def _():
        start_all(own_up())

    ring_late_on(1)
    z_late(2)
    ring_late(2)
    z_late(3)
    ring_late(3)
    for k in range(n_sp):
        ring_in_end(k)

    for h in range(heads):
        state[h] = first_state[h].T
    ext[0:8] = jnp.zeros((8, con), F32)
    lane_rec = pl.ds(pl.multiple_of(sp * rec, rec), rec)
    lane_con = pl.ds(pl.multiple_of(sp * con, con), con)
    row_id = lax.broadcasted_iota(jnp.int32, (span, span), 0)
    col_id = lax.broadcasted_iota(jnp.int32, (span, span), 1)
    causal = row_id >= col_id
    lower = causal.astype(F32)
    upper = (row_id <= col_id).astype(F32)
    length = 2 * span

    def sib_copy(s, c):
        return remote(sib_send.at[s, c], sib_recv.at[s, c], sib_out.at[s, c], sib_sem.at[s, c], sibling)

    def z_copy(s, c):
        return remote(z_send.at[s, c], z_recv.at[sp, c], rs_send.at[s, c], zr_sem.at[sp, c], peer(sp=s))

    def edge_copy(s, c, to):
        return remote(z_send.at[s, c], rl_recv.at[s, c], rs_send.at[s, c], rl_sem.at[s, c], peer(sp=to))

    def through_low(s):
        return jnp.logical_and(sp == 0, s >= 2)

    def through_high(s):
        return jnp.logical_and(sp == n_sp - 1, s <= n_sp - 3)

    def joins(s):
        return jnp.logical_or(
            jnp.logical_and(sp == 1, s >= 2), jnp.logical_and(sp == n_sp - 2, s <= n_sp - 3)
        )

    def plain(s):
        edge = jnp.logical_or(through_low(s), through_high(s))
        return jnp.logical_not(jnp.logical_or(jnp.logical_or(edge, joins(s)), s == sp))

    def pass_on(s):
        for c in range(chunks):
            sib_copy(s, c).wait_recv()
            total = mine[s, c] + sib_recv[s, c].astype(F32)
            mine[s, c] = total

            @pl.when(jnp.logical_not(jnp.logical_or(joins(s), s == sp)))
            def _():
                z_send[s, c] = total.astype(BF16)

            @pl.when(plain(s))
            def _():
                z_copy(s, c).start()

            @pl.when(through_low(s))
            def _():
                edge_copy(s, c, 1).start()

            @pl.when(through_high(s))
            def _():
                edge_copy(s, c, n_sp - 2).start()

    def join(s):
        for c in range(chunks):
            arrived(rl_recv.at[s, c], rl_sem.at[s, c])
            z_send[s, c] = (mine[s, c] + rl_recv[s, c].astype(F32)).astype(BF16)
            z_copy(s, c).start()

    def project_out(s):
        for c in range(chunks):
            columns = jnp.concatenate(
                [wout[c * shards_in + i] for i in range(shards_in)], axis=1
            )
            partial = jnp.dot(
                both[s], columns, preferred_element_type=F32
            )
            first = partial[:span]
            second = partial[span:]
            mine[s, c] = jnp.where(tp == 0, first, second)
            sib_send[s, c] = jnp.where(tp == 0, second, first).astype(BF16)
            sib_copy(s, c).start()

    def convolve(s):
        block = jnp.concatenate([tokens[2 * s], tokens[2 * s + 1]], axis=0)
        projected = jnp.dot(block, wcon[...], preferred_element_type=F32).astype(BF16).astype(F32)
        prod = projected[:, con : 2 * con] * projected[:, 2 * con :]
        ext[8:] = prod
        conv = jnp.broadcast_to(bias[:, lane_con], prod.shape)
        for j in range(KW):
            conv = conv + taps[j : j + 1, lane_con] * ext[pl.ds(8 - (KW - 1) + j, length)]
        ext[0:8] = ext[length:]
        both[s, :, rec:] = (projected[:, :con] * conv).astype(BF16)

    def recur(s):
        relays(jnp.logical_and(edge, s != sp), s, 0)
        for c in range(TOKEN_PIECES):
            arrived(token_slot(s, other, c), tok_t.at[s, c])
        block = jnp.concatenate([tokens[2 * s], tokens[2 * s + 1]], axis=0)

        def project(at, width):
            return jnp.dot(
                block, win[:, pl.ds(at, width)], preferred_element_type=F32
            ).astype(BF16)

        query = project(0, rec).astype(F32) * DK ** (-0.5)
        forget = project(rec, rec).astype(F32)
        value = project(2 * rec, rec)
        key_gate = headroom[:, lane_rec] * jax.nn.sigmoid(-forget)
        log_forget = jnp.log1p(-key_gate)
        gains = gain[:, lane_rec]
        mine_rate = [rates[s, pl.ds(sp * heads + h, 1), :] for h in range(heads)]
        if heads < 8:
            mine_rate.append(jnp.zeros((8 - heads, 2 * span), F32))
        mine_rate = jnp.concatenate(mine_rate, axis=0)
        halves = []
        for c in range(2):
            part = slice(c * span, (c + 1) * span)
            cum = jnp.dot(lower, log_forget[part], precision=lax.Precision.HIGHEST)
            extra = jnp.dot(mine_rate[:, part], upper, precision=lax.Precision.HIGHEST)
            extra_t = extra.T
            grow = jnp.exp(cum)
            query_grow = query[part] * grow
            key_grow = (key_gate[part] / grow).astype(BF16)
            last = cum[span - 1 :, :]
            key_last = key_gate[part] * jnp.exp(last - cum)
            last_decay = jnp.exp(last)
            pieces = []
            for h in range(heads):
                lanes = slice(h * DK, (h + 1) * DK)
                row = extra[h : h + 1]
                column = extra_t[:, h : h + 1]
                end = row[:, span - 1 :]
                scores = lax.dot_general(
                    query_grow[:, lanes].astype(BF16), key_grow[:, lanes], CONTRACT_LAST,
                    preferred_element_type=F32,
                )
                decay = jnp.exp(jnp.where(causal, column - row, 0.0))
                scores = jnp.where(causal, scores * decay, 0.0).astype(BF16)
                values = value[part, lanes]
                before = state[h]
                raw = jnp.dot(scores, values, preferred_element_type=F32)
                raw = raw + lax.dot_general(
                    (query_grow[:, lanes] * jnp.exp(column)).astype(BF16), before.astype(BF16),
                    CONTRACT_LAST, preferred_element_type=F32,
                )
                keys = (key_last[:, lanes] * jnp.exp(end - column)).astype(BF16)
                state[h] = before * (last_decay[:, lanes] * jnp.exp(end)) + lax.dot_general(
                    values, keys, CONTRACT_FIRST, preferred_element_type=F32
                )
                square = jnp.mean(raw * raw, axis=-1, keepdims=True)
                pieces.append((raw * lax.rsqrt(square + 1e-06) * gains[:, lanes]).astype(BF16))
            halves.append(jnp.concatenate(pieces, axis=1))
        both[s, :, :rec] = jnp.concatenate(halves, axis=0)

    lag = jnp.where(sp < 2, 0, 1)

    def step(i, carry):
        s = i - lag

        @pl.when(jnp.logical_and(s >= 0, s < n_sp))
        def _():
            recur(s)

        @pl.when(i == 0)
        def _():
            ring_late_on(2)
            relays(low, top - 1, -1)
            relays(high, bottom, 1)
            ring_late_on(3)

        @pl.when(i == 1)
        def _():
            relays(low, top, -1)
            relays(high, 1, 1)
            for k in range(n_sp):
                ring_late_end(k)

        @pl.when(jnp.logical_and(i == 1, lag == 0))
        def _():
            convolve(0)
            project_out(0)
            pass_on(0)

        @pl.when(jnp.logical_and(i > 0, s < n_sp))
        def _():
            convolve(s)
            project_out(s)

        @pl.when(jnp.logical_and(jnp.logical_and(i > 0, s < n_sp), jnp.logical_or(s > 1, sp > 0)))
        def _():
            pass_on(s)

        return carry

    lax.fori_loop(0, n_sp + 1, step, 0)

    @pl.when(sp == 0)
    def _():
        pass_on(1)

    @pl.when(sp == 1)
    def _():
        for s in range(2, n_sp):
            join(s)

    @pl.when(sp == n_sp - 2)
    def _():
        for s in range(n_sp - 2):
            join(s)

    for d in range(n_sp):
        comes = sp != d
        if d == 0:
            comes = jnp.logical_and(comes, sp < 2)
        if d == n_sp - 1:
            comes = jnp.logical_and(comes, sp > n_sp - 3)

        @pl.when(comes)
        def _():
            for c in range(chunks):
                arrived(z_recv.at[d, c], zr_sem.at[d, c])
                mine[sp, c] = mine[sp, c] + z_recv[d, c].astype(F32)

    for c in range(chunks):
        out[:, c * chunk : (c + 1) * chunk] = mine[sp, c].astype(BF16)

    for copy in sent + late_copies():
        copy.wait_send()
    for k in range(n_sp):
        for copy in in_ring(k) + late_ring(k):
            copy.wait_send()

    @pl.when(sp < n_sp - 1)
    def _():
        for copy in own_up():
            copy.wait_send()

    @pl.when(sp > 0)
    def _():
        for copy in own_down():
            copy.wait_send()

    for s in range(n_sp):
        for c in range(TOKEN_PIECES):
            to_sibling(s, c).wait_send()
            forwarded = jnp.logical_or(
                jnp.logical_and(sp > s, sp < n_sp - 1), jnp.logical_and(sp < s, sp > 0)
            )

            @pl.when(forwarded)
            def _():
                relayed(s, c, down_send, sibling).wait_send()

        for c in range(chunks):
            sib_copy(s, c).wait_send()

            @pl.when(sp != s)
            def _():
                remote(
                    z_send.at[s, c], rl_recv.at[s, c], rs_send.at[s, c], rl_sem.at[s, c], sibling
                ).wait_send()


def sequence_shards(n_sp, n_fs, *arrays):
    (tok, wq, wf, wv, cg, cm, ci, headroom, rate, init, gain, taps, bias, ro, co) = arrays
    span, wide = tok.shape[1:]
    rec, con = wq.shape[1] // n_sp, cg.shape[1] // n_sp
    heads = rec // DK
    chunk = wide // OUT_PIECES
    hbm = pl.BlockSpec(memory_space=pl.ANY)
    vmem = pl.BlockSpec(memory_space=pltpu.VMEM)
    dma = pltpu.SemaphoreType.DMA
    flat = (n_sp, OUT_PIECES, span, chunk)
    mixed = pl.pallas_call(
        functools.partial(layer_kernel, n_sp, n_fs),
        out_shape=jax.ShapeDtypeStruct((span, wide), BF16),
        in_specs=[hbm] * 11 + [vmem] * 4,
        out_specs=vmem,
        scratch_shapes=[
            pltpu.VMEM((2 * n_sp, span, wide), BF16),
            pltpu.VMEM((wide, 3 * rec), BF16),
            pltpu.VMEM((wide, 3 * con), BF16),
            pltpu.VMEM((n_sp * n_fs, rec + con, wide // (n_sp * n_fs)), BF16),
            pltpu.VMEM((n_sp,) + rate.shape[1:], F32),
            pltpu.VMEM((heads, DK, DK), F32),
            pltpu.VMEM((heads, DK, DK), F32),
            pltpu.VMEM((8 + 2 * span, con), F32),
            pltpu.VMEM((n_sp, 2 * span, rec + con), BF16),
            pltpu.VMEM(flat, BF16),
            pltpu.VMEM(flat, BF16),
            pltpu.VMEM(flat, F32),
            pltpu.VMEM(flat, BF16),
            pltpu.VMEM(flat, BF16),
            pltpu.VMEM(flat, BF16),
            pltpu.VMEM((n_sp, wide // (n_sp * n_fs), 3 * rec), BF16),
            pltpu.VMEM((n_sp, wide // (n_sp * n_fs), 3 * con), BF16),
            pltpu.VMEM((n_sp, rec + con, wide // (n_sp * n_fs)), BF16),
            dma((n_sp,)),
            dma((n_sp,)),
            dma((n_sp,)),
            dma((3,)),
            dma(((n_sp - 1) * 2,)),
            dma((4, n_sp)),
            dma((n_sp,)),
            dma((n_sp,)),
            dma((n_sp,)),
            dma((4, n_sp)),
            dma((6, n_sp)),
            dma((n_sp, TOKEN_PIECES)),
            dma((n_sp, TOKEN_PIECES)),
            dma((n_sp,)),
            dma((6, n_sp)),
            dma((2, n_sp)),
            dma((n_sp, TOKEN_PIECES)),
            dma((2, TOKEN_PIECES)),
            dma((n_sp, TOKEN_PIECES)),
            dma((n_sp, OUT_PIECES)),
            dma((n_sp, OUT_PIECES)),
            dma((n_sp, OUT_PIECES)),
            dma((n_sp, OUT_PIECES)),
            dma((n_sp, OUT_PIECES)),
        ],
        compiler_params=pltpu.CompilerParams(
            collective_id=0, has_side_effects=True, vmem_limit_bytes=60 * 2**20
        ),
    )(
        tok[0], wq, wf, wv, cg, cm, ci, ro, co, rate[0], init[0], headroom[None], gain[None],
        taps, bias[None],
    )
    return mixed[None]


def choose_plan(sizes, *arrays):
    n_sp, n_fs = sizes["sp"], sizes["fs"]
    rows, rec = arrays[1].shape
    con = arrays[4].shape[1]
    span = arrays[0].shape[1]
    even = (
        sizes["tp"] == 2
        and n_fs == 4
        and n_sp == 4
        and arrays[0].shape[2] % (n_fs * n_sp * 128) == 0
        and arrays[0].shape[0] == 1
        and rec % (n_sp * DK) == 0
        and rec // (n_sp * DK) <= 8
        and arrays[8].shape[1] % 8 == 0
        and con % (n_sp * 128) == 0
        and rows % 128 == 0
        and span == DK
        and arrays[13].shape[1] % 128 == 0
    )
    return sequence_shards(n_sp, n_fs, *arrays) if even else shards(*arrays)


def solution(mesh):
    in_specs = (
        P("fs", ("sp", "tp"), None),
        P(("sp", "fs"), "tp"),
        P(("sp", "fs"), "tp"),
        P(("sp", "fs"), "tp"),
        P(("sp", "fs"), "tp"),
        P(("sp", "fs"), "tp"),
        P(("sp", "fs"), "tp"),
        P("tp"),
        P("fs", "tp", "sp"),
        P("fs", "tp", None, None),
        P("tp"),
        P(None, "tp"),
        P("tp"),
        P("tp", ("sp", "fs")),
        P("tp", ("sp", "fs")),
    )
    out_specs = P("fs", ("sp", "tp"), None)
    body = functools.partial(choose_plan, dict(mesh.shape))
    return jax.shard_map(body, mesh=mesh, in_specs=in_specs, out_specs=out_specs, check_vma=False)
```

```python
import functools

import jax
import jax.numpy as jnp
from jax import lax
from jax.experimental import pallas as pl
from jax.experimental.pallas import tpu as pltpu
from jax.sharding import PartitionSpec as P

DK = 128
KW = 3
BLOCK_POSITIONS = 64


def carried_in(part, axis, combine, identity):
    place = lax.axis_index(axis)
    gathered = jax.tree.map(lambda a: lax.all_gather(a, axis), part)
    state = jax.tree.map(lambda a, e: jnp.zeros_like(a) + jnp.asarray(e, a.dtype), part, identity)

    def one(hop, state):
        return combine(
            state, jax.tree.map(lambda a: lax.dynamic_index_in_dim(a, hop, 0, False), gathered)
        )

    return lax.fori_loop(0, place, one, state)


def from_behind(block, axis, distance):
    devices = range(lax.axis_size(axis))
    route = [(i - distance, i) for i in devices if i - distance in devices]
    return lax.ppermute(block, axis, route)


def to_blocks(values, number_of_heads):
    number_of_blocks = values.shape[0] // BLOCK_POSITIONS
    return jnp.transpose(
        values.reshape(number_of_blocks, BLOCK_POSITIONS, number_of_heads, DK), (2, 0, 1, 3)
    )


def within_block_recurrence(
    query_vectors, forget_logits, value_vectors, gate_headroom, extra_rates
):
    number_of_heads = extra_rates.shape[0]
    number_of_blocks = query_vectors.shape[0] // BLOCK_POSITIONS
    query_scaled = to_blocks(query_vectors.astype(jnp.float32), number_of_heads) * DK ** (-0.5)
    gated_key = to_blocks(
        gate_headroom[None, :] * jax.nn.sigmoid(-forget_logits.astype(jnp.float32)), number_of_heads
    )
    forget_log_rate = (
        jnp.log1p(-gated_key)
        + extra_rates.reshape(number_of_heads, number_of_blocks, BLOCK_POSITIONS)[..., None]
    )
    values = to_blocks(value_vectors.astype(jnp.float32), number_of_heads)
    cumulative = jnp.cumsum(forget_log_rate, axis=2)
    query_decayed = query_scaled * jnp.exp(cumulative)
    key_decayed = gated_key * jnp.exp(-cumulative)
    scores = jnp.einsum(
        "hnik,hnjk->hnij", query_decayed, key_decayed, precision=lax.Precision.HIGHEST
    )
    causal = jnp.tril(jnp.ones((BLOCK_POSITIONS, BLOCK_POSITIONS), dtype=bool))
    scores = jnp.where(causal, scores, 0.0)
    within = jnp.einsum("hnij,hnjv->hniv", scores, values, precision=lax.Precision.HIGHEST)
    final_log = cumulative[:, :, -1, :]
    contrib = jnp.einsum(
        "hnck,hncv->hnkv",
        gated_key * jnp.exp(final_log[:, :, None, :] - cumulative),
        values,
        precision=lax.Precision.HIGHEST,
    )
    decays = jnp.exp(final_log)

    def advance(current, block_pair):
        return (block_pair[0][..., None] * current + block_pair[1], current)

    empty_state = jnp.zeros((number_of_heads, DK, DK), jnp.float32)
    local_total, entering = lax.scan(
        advance, empty_state, (jnp.moveaxis(decays, 1, 0), jnp.moveaxis(contrib, 1, 0))
    )
    entering = jnp.moveaxis(entering, 0, 1)
    before = jnp.exp(jnp.cumsum(final_log, axis=1) - final_log)
    device_decay = jnp.exp(jnp.sum(final_log, axis=1))
    return (query_decayed, within, entering, before, device_decay, local_total)


def finish(query_decayed, within, entering, before, carried, head_norm_gain):
    number_of_heads = query_decayed.shape[0]
    states = entering + before[..., None] * carried[:, None]
    carried_term = jnp.einsum(
        "hnck,hnkv->hncv", query_decayed, states, precision=lax.Precision.HIGHEST
    )
    length = query_decayed.shape[1] * BLOCK_POSITIONS
    recurrence_unnormed = jnp.transpose(within + carried_term, (1, 2, 0, 3)).reshape(
        length, number_of_heads, DK
    )
    mean_square = jnp.mean(recurrence_unnormed * recurrence_unnormed, axis=-1, keepdims=True)
    rec_out = (
        recurrence_unnormed
        * lax.rsqrt(mean_square + 1e-06)
        * head_norm_gain.reshape(number_of_heads, DK)
    )
    return rec_out.reshape(length, number_of_heads * DK).astype(jnp.bfloat16)


def chain_combine(earlier_part, later_part):
    return (
        earlier_part[0] * later_part[0],
        later_part[0][..., None] * earlier_part[1] + later_part[1],
    )


def shards(
    tokens,
    query_weight,
    forget_weight,
    value_weight,
    convolution_gate_weight,
    convolution_multiplier_weight,
    convolution_input_weight,
    gate_headroom,
    added_log_rate,
    initial_state,
    head_norm_gain,
    convolution_taps,
    convolution_bias,
    recurrence_output_weight,
    convolution_output_weight,
):
    own_rows = tokens[0]
    gathered = (
        lax.all_gather(query_weight, ("sp", "fs"), axis=0, tiled=True),
        lax.all_gather(forget_weight, ("sp", "fs"), axis=0, tiled=True),
        lax.all_gather(value_weight, ("sp", "fs"), axis=0, tiled=True),
        lax.all_gather(convolution_gate_weight, ("sp", "fs"), axis=0, tiled=True),
        lax.all_gather(convolution_multiplier_weight, ("sp", "fs"), axis=0, tiled=True),
        lax.all_gather(convolution_input_weight, ("sp", "fs"), axis=0, tiled=True),
        lax.all_gather(recurrence_output_weight, ("sp", "fs"), axis=1, tiled=True),
        lax.all_gather(convolution_output_weight, ("sp", "fs"), axis=1, tiled=True),
    )
    in_weights = gathered[:6]
    out_rec = gathered[6]
    out_conv = gathered[7]
    block_rows = lax.all_gather(own_rows, "tp", axis=0, tiled=True)
    projected = jnp.concatenate(
        [
            jnp.dot(block_rows, weight, preferred_element_type=jnp.float32).astype(jnp.bfloat16)
            for weight in in_weights
        ],
        axis=1,
    )
    rec_width = query_weight.shape[1]
    conv_width = convolution_gate_weight.shape[1]
    query_vectors = projected[:, :rec_width]
    forget_logits = projected[:, rec_width : 2 * rec_width]
    value_vectors = projected[:, 2 * rec_width : 3 * rec_width]
    conv_base = 3 * rec_width
    conv_gate = projected[:, conv_base : conv_base + conv_width]
    conv_mult = projected[:, conv_base + conv_width : conv_base + 2 * conv_width]
    conv_input = projected[:, conv_base + 2 * conv_width : conv_base + 3 * conv_width]
    query_decayed, within, entering, before, device_decay, local_total = within_block_recurrence(
        query_vectors, forget_logits, value_vectors, gate_headroom, added_log_rate[0]
    )
    conv_prod = conv_mult.astype(jnp.float32) * conv_input.astype(jnp.float32)
    length = conv_prod.shape[0]
    tail_rows = conv_prod[length - (KW - 1) :]
    unit_decay = jnp.ones_like(device_decay)
    empty_state = jnp.zeros_like(local_total)
    prior_decay, prior_state = carried_in(
        (device_decay, local_total), "sp", chain_combine, (unit_decay, empty_state)
    )
    prior_rows = from_behind(tail_rows, "sp", 1)
    carried = prior_decay[..., None] * initial_state[0] + prior_state
    rec_out = finish(query_decayed, within, entering, before, carried, head_norm_gain)
    extended = jnp.concatenate([prior_rows, conv_prod], axis=0)
    conv_y = jnp.broadcast_to(convolution_bias[None, :], conv_prod.shape)
    for j in range(KW):
        conv_y = conv_y + convolution_taps[j][None, :] * extended[j : j + length]
    conv_out = (conv_gate.astype(jnp.float32) * conv_y).astype(jnp.bfloat16)
    mixed = lax.psum_scatter(
        (
            jnp.dot(rec_out, out_rec, preferred_element_type=jnp.float32)
            + jnp.dot(conv_out, out_conv, preferred_element_type=jnp.float32)
        ).astype(jnp.bfloat16),
        "tp",
        scatter_dimension=0,
        tiled=True,
    )
    return mixed[None]


MESH = pl.DeviceIdType.MESH
F32 = jnp.float32
BF16 = jnp.bfloat16
CONTRACT_LAST = (((1,), (1,)), ((), ()))
CONTRACT_FIRST = (((0,), (0,)), ((), ()))
TOKEN_PIECES = 4
SENDS = 13
(
    UP, DOWN, ACROSS, RELAY, RATE, FIRST, CON, OUT, IN_RING, CON_RING, OUT_RING, SIBLING, SUMS,
) = range(SENDS)
OUT_PIECES = 8


def layer_kernel(
    n_sp, n_fs, tok, wq, wf, wv, cg, cm, ci, ro, co, rate, init, headroom, gain, taps, bias,
    out, tokens, win, wcon, wout, rates, first_state, state, ext, both, sib_send, sib_recv, mine,
    z_send, z_recv, rl_recv, stage_in, stage_con, stage_out, loc_in, loc_sem, out_sem, win_z,
    wcon_z, wout_z, in_f, con_f, out_f, end_f, tok_z, tok_t, sib_sem, zr_sem, rl_sem,
):
    sp, fs, tp = lax.axis_index("sp"), lax.axis_index("fs"), lax.axis_index("tp")
    other = 1 - tp
    rows = wq.shape[0]
    rec = wq.shape[1] // n_sp
    con = cg.shape[1] // n_sp
    span = tok.shape[0]
    heads = rec // DK
    wide = tok.shape[1]
    lanes_out = ro.shape[1]
    chunks, chunk = mine.shape[1], mine.shape[3]
    sub = span // TOKEN_PIECES
    shards_in = chunk // lanes_out

    def peer(**where):
        return {"sp": where.get("sp", sp), "fs": where.get("fs", fs), "tp": where.get("tp", tp)}

    half_ring = n_fs // 2

    def ring(p):
        return p + (p // half_ring) * (3 * half_ring - 1 - 2 * p)

    at_ring = ring(fs)
    left = ring(lax.rem(at_ring + n_fs - 1, n_fs))
    right = ring(lax.rem(at_ring + 1, n_fs))
    across = ring(lax.rem(at_ring + 2, n_fs))
    sibling = peer(tp=other)

    rec_parts = [(ref, i * rec, rec) for i, ref in enumerate((wq, wf, wv))]
    con_parts = [(ref, i * con, con) for i, ref in enumerate((cg, cm, ci))]

    def in_rows(s, f, first, count):
        return win.at[pl.ds(pl.multiple_of((s * n_fs + f) * rows + first, count), count)]

    def con_rows(s, f):
        return wcon.at[pl.ds(pl.multiple_of((s * n_fs + f) * rows, rows), rows)]

    def out_slot(s, f):
        return wout.at[s * n_fs + f]

    def stage(z, in_to, con_to, out_to, place):
        copies = []
        for some, to, sem in ((rec_parts, in_to, loc_in.at[place]), (con_parts, con_to, loc_sem.at[0])):
            for ref, at, width in some:
                src = ref.at[:, pl.ds(pl.multiple_of(z * width, width), width)]
                copies.append((src, to.at[:, pl.ds(at, width)], sem))
        for ref, at, width in ((ro, 0, rec), (co, rec, con)):
            src = ref.at[pl.ds(pl.multiple_of(z * width, width), width)]
            copies.append((src, out_to.at[pl.ds(at, width)], loc_sem.at[1]))
        return [pltpu.make_async_copy(*copy) for copy in copies]

    below, above = sp, n_sp - 1 - sp
    fewer = jnp.minimum(below, above)
    upward = jnp.where(below < above, 1, -1)
    edge = fewer == 0

    def near(j):
        paired = j <= 2 * fewer
        side = jnp.where(paired, upward * (1 - 2 * (j % 2)), upward)
        return sp + side * jnp.where(paired, (j + 1) // 2, j - fewer)

    def to_send(j):
        if j == 1:
            return near(1)
        return jnp.where(edge, near(n_sp + 1 - j), near(j))

    local = []
    for j in range(1, n_sp):
        local += stage(to_send(j), stage_in.at[j], stage_con.at[j], stage_out.at[j], j)
    local += stage(sp, in_rows(sp, fs, 0, rows), con_rows(sp, fs), out_slot(sp, fs), 0)
    others = [
        (tok, tokens.at[sp * 2 + tp]), (rate, rates.at[sp]),
        (init.at[pl.ds(sp * heads, heads)], first_state),
    ]
    others = [pltpu.make_async_copy(*pair, loc_sem.at[2 + i]) for i, pair in enumerate(others)]
    for copy in local + others:
        copy.start()

    barrier = pltpu.get_barrier_semaphore()
    for j in range(1, n_sp):
        pl.semaphore_signal(barrier, inc=1, device_id=peer(sp=near(j)), device_id_type=MESH)
    for f in (left, right):
        pl.semaphore_signal(barrier, inc=1, device_id=peer(fs=f), device_id_type=MESH)
    pl.semaphore_signal(barrier, inc=1, device_id=sibling, device_id_type=MESH)
    pl.semaphore_wait(barrier, n_sp + 2)

    def remote(src, dst, send, recv, to):
        return pltpu.make_async_remote_copy(
            src_ref=src, dst_ref=dst, send_sem=send, recv_sem=recv, device_id=to, device_id_type=MESH,
        )

    def arrived(ref, recv):
        remote(ref, ref, recv, recv, sibling).wait_recv()

    def gone(ref, i):
        remote(ref, ref, out_sem.at[i], out_sem.at[i], sibling).wait_send()

    def tok_piece(ref, c):
        return ref.at[pl.ds(c * sub, sub)]

    def token_slot(s, t, c):
        return tok_piece(tokens.at[s * 2 + t], c)

    def own_tokens(send, to):
        return [
            remote(tok_piece(tok, c), token_slot(sp, tp, c), send, tok_z.at[sp, c], to)
            for c in range(TOKEN_PIECES)
        ]

    def own_up():
        return own_tokens(out_sem.at[UP], peer(sp=sp + 1))

    def own_down():
        return own_tokens(out_sem.at[DOWN], peer(sp=sp - 1))

    def to_sibling(s, c, src=None):
        slot = token_slot(s, tp, c)
        return remote(slot if src is None else src, slot, out_sem.at[ACROSS], tok_t.at[s], sibling)

    def relayed(s, c, to):
        slot = token_slot(s, tp, c)
        return remote(slot, slot, out_sem.at[RELAY], tok_z.at[s, c], to)

    def start_all(copies):
        for copy in copies:
            copy.start()

    def send_in(j):
        to = peer(sp=to_send(j))
        arrived(stage_in.at[j], loc_in.at[j])
        remote(rate, rates.at[sp], out_sem.at[RATE], end_f.at[3], to).start()
        remote(
            stage_in.at[j], in_rows(sp, fs, 0, rows), out_sem.at[FIRST], win_z.at[sp], to
        ).start()

    def late_copies():
        copies = []
        for j in range(1, n_sp):
            to = peer(sp=to_send(j))
            copies.append(
                remote(stage_con.at[j], con_rows(sp, fs), out_sem.at[CON], wcon_z.at[sp], to)
            )
            copies.append(
                remote(stage_out.at[j], out_slot(sp, fs), out_sem.at[OUT], wout_z.at[sp], to)
            )
        return copies

    low, high = sp == 1, sp == n_sp - 2
    send_in(1)

    for j in range(2, n_sp):
        send_in(j)
    arrived(stage_con, loc_sem.at[0])
    arrived(stage_out, loc_sem.at[1])
    start_all(late_copies()[:2])
    for copy in others:
        copy.wait()

    @pl.when(sp == 0)
    def _():
        start_all(own_up())

    @pl.when(sp == n_sp - 1)
    def _():
        start_all(own_down())

    for c in range(TOKEN_PIECES):
        to_sibling(sp, c, tok_piece(tok, c)).start()

    arrived(in_rows(sp, fs, 0, rows), loc_in.at[0])

    def z_in(j):
        z = near(j)
        arrived(in_rows(z, fs, 0, rows), win_z.at[z])

    def z_late(j):
        z = near(j)
        arrived(con_rows(z, fs), wcon_z.at[z])
        arrived(out_slot(z, fs), wout_z.at[z])

    def place(j):
        return near(j) if j else sp

    def in_ring(k):
        s, half = place(k), rows // 2
        whole = in_rows(s, fs, 0, rows)
        copies = (
            (whole, in_f.at[0, k], right), (whole, in_f.at[1, k], left),
            (in_rows(s, left, 0, half), end_f.at[0], right),
            (in_rows(s, right, half, half), end_f.at[0], left),
        )
        return [remote(ref, ref, out_sem.at[IN_RING], sem, peer(fs=to)) for ref, sem, to in copies]

    def ring_in(k):
        start_all(in_ring(k)[:2])

    def ring_in_on(k):
        s = place(k)
        on = in_ring(k)[2:]
        arrived(in_rows(s, left, 0, rows), in_f.at[0, k])
        on[0].start()
        arrived(in_rows(s, right, 0, rows), in_f.at[1, k])
        on[1].start()

    def ring_in_end():
        arrived(win.at[pl.ds(0, n_sp * rows)], end_f.at[0])

    def late_ring(k):
        s = place(k)
        own_con, own_out = con_rows(s, fs), out_slot(s, fs)
        copies = (
            (own_con, CON_RING, con_f.at[k], right), (own_out, OUT_RING, out_f.at[k], left),
            (own_con, CON_RING, end_f.at[1], left), (own_out, OUT_RING, end_f.at[2], right),
            (con_rows(s, left), CON_RING, end_f.at[1], right),
            (out_slot(s, right), OUT_RING, end_f.at[2], left),
        )
        return [remote(ref, ref, out_sem.at[i], sem, peer(fs=to)) for ref, i, sem, to in copies]

    def ring_late(k):
        start_all(late_ring(k)[:4])

    def ring_late_on(k):
        s = place(k)
        on = late_ring(k)[4:]
        arrived(con_rows(s, left), con_f.at[k])
        on[0].start()
        arrived(out_slot(s, right), out_f.at[k])
        on[1].start()

    def ring_late_end():
        arrived(wcon.at[pl.ds(0, 2 * n_sp * rows)], end_f.at[1])
        arrived(wout.at[pl.ds(0, 2 * n_sp)], end_f.at[2])

    def relay(s, c, step_by):
        arrived(token_slot(s, tp, c), tok_z.at[s, c])
        if step_by:
            relayed(s, c, peer(sp=sp + step_by)).start()
        to_sibling(s, c).start()

    def relays(when, s, step_by, pieces=range(TOKEN_PIECES)):
        @pl.when(when)
        def _():
            for c in pieces:
                relay(s, c, step_by)

    early, late = range(TOKEN_PIECES // 2), range(TOKEN_PIECES // 2, TOKEN_PIECES)
    bottom, top = 0, n_sp - 1

    def second_in():
        z_in(2)
        ring_in(2)

    def first_late():
        z_late(1)
        ring_late(1)

    inner = jnp.logical_not(edge)
    ring_in(0)
    z_in(1)
    ring_in(1)
    pl.when(inner)(second_in)
    ring_in_on(0)
    ring_late(0)

    @pl.when(low)
    def _():
        start_all(own_down())

    @pl.when(high)
    def _():
        start_all(own_up())

    ring_in_on(1)

    @pl.when(edge)
    def _():
        first_late()
        second_in()

    z_in(3)
    ring_in(3)
    start_all(late_copies()[2:])

    @pl.when(high)
    def _():
        start_all(own_down())

    pl.when(inner)(first_late)
    ring_in_on(2)
    relays(low, bottom, 1, early)
    relays(high, top, -1, early)
    ring_in_on(3)
    ring_late_on(0)
    relays(low, bottom, 1, late)
    relays(high, top, -1, late)

    @pl.when(low)
    def _():
        start_all(own_up())

    ring_late_on(1)
    relays(sp == 0, 1, 0)
    relays(sp == top, top - 1, 0)
    z_late(2)
    ring_late(2)
    z_late(3)
    ring_late(3)
    ring_in_end()
    arrived(rates.at[pl.ds(0, n_sp - 1)], end_f.at[3])

    for h in range(heads):
        state[h] = first_state[h].T
    ext[0:8] = jnp.zeros((8, con), F32)
    lane_rec = pl.ds(pl.multiple_of(sp * rec, rec), rec)
    lane_con = pl.ds(pl.multiple_of(sp * con, con), con)
    row_id = lax.broadcasted_iota(jnp.int32, (span, span), 0)
    col_id = lax.broadcasted_iota(jnp.int32, (span, span), 1)
    causal = row_id >= col_id
    lower = causal.astype(F32)
    upper = (row_id <= col_id).astype(F32)
    length = 2 * span

    def sib_copy(s, c):
        return remote(sib_send.at[s, c], sib_recv.at[s, c], out_sem.at[SIBLING], sib_sem.at[s, c], sibling)

    def z_copy(s, c):
        return remote(z_send.at[s, c], z_recv.at[sp, c], out_sem.at[SUMS], zr_sem.at[sp], peer(sp=s))

    def edge_copy(s, c, to):
        landing, sem = rl_recv.at[s % 2, c], rl_sem.at[s % 2, c]
        return remote(z_send.at[s, c], landing, out_sem.at[SUMS], sem, peer(sp=to))

    def through_low(s):
        return jnp.logical_and(sp == 0, s >= 2)

    def through_high(s):
        return jnp.logical_and(sp == n_sp - 1, s <= n_sp - 3)

    def joins(s):
        return jnp.logical_or(
            jnp.logical_and(sp == 1, s >= 2), jnp.logical_and(sp == n_sp - 2, s <= n_sp - 3)
        )

    def plain(s):
        edge = jnp.logical_or(through_low(s), through_high(s))
        return jnp.logical_not(jnp.logical_or(jnp.logical_or(edge, joins(s)), s == sp))

    def pass_on(s, pieces=range(OUT_PIECES)):
        for c in pieces:
            sib_copy(s, c).wait_recv()
            total = mine[s, c] + sib_recv[s, c].astype(F32)
            mine[s, c] = total

            @pl.when(jnp.logical_not(jnp.logical_or(joins(s), s == sp)))
            def _():
                z_send[s, c] = total.astype(BF16)

            @pl.when(plain(s))
            def _():
                z_copy(s, c).start()

            @pl.when(through_low(s))
            def _():
                edge_copy(s, c, 1).start()

            @pl.when(through_high(s))
            def _():
                edge_copy(s, c, n_sp - 2).start()

    def join(s):
        for c in range(chunks):
            arrived(rl_recv.at[s % 2, c], rl_sem.at[s % 2, c])
            z_send[s, c] = (mine[s, c] + rl_recv[s % 2, c].astype(F32)).astype(BF16)
            z_copy(s, c).start()

    def project_out(s):
        wider = 2 * shards_in
        for n in range(0, n_sp * n_fs, wider):
            columns = jnp.concatenate([wout[n + i] for i in range(wider)], axis=1)
            partial = jnp.dot(both[s], columns, preferred_element_type=F32)
            first = partial[:span]
            second = partial[span:]
            own = jnp.where(tp == 0, first, second)
            given = jnp.where(tp == 0, second, first).astype(BF16)
            for i in range(2):
                c = n // shards_in + i
                mine[s, c] = own[:, i * chunk : (i + 1) * chunk]
                sib_send[s, c] = given[:, i * chunk : (i + 1) * chunk]
                sib_copy(s, c).start()

    def convolve(s):
        block = jnp.concatenate([tokens[2 * s], tokens[2 * s + 1]], axis=0)
        projected = jnp.dot(block, wcon[...], preferred_element_type=F32).astype(BF16).astype(F32)
        prod = projected[:, con : 2 * con] * projected[:, 2 * con :]
        ext[8:] = prod
        conv = jnp.broadcast_to(bias[:, lane_con], prod.shape)
        for j in range(KW):
            conv = conv + taps[j : j + 1, lane_con] * ext[pl.ds(8 - (KW - 1) + j, length)]
        ext[0:8] = ext[length:]
        both[s, :, rec:] = (projected[:, :con] * conv).astype(BF16)

    def recur(s):
        relays(jnp.logical_and(edge, (s - sp) * (s - sp) > 1), s, 0)
        arrived(tokens.at[2 * s + other], tok_t.at[s])
        block = jnp.concatenate([tokens[2 * s], tokens[2 * s + 1]], axis=0)

        def project(at, width):
            return jnp.dot(
                block, win[:, pl.ds(at, width)], preferred_element_type=F32
            ).astype(BF16)

        query = project(0, rec).astype(F32) * DK ** (-0.5)
        forget = project(rec, rec).astype(F32)
        value = project(2 * rec, rec)
        key_gate = headroom[:, lane_rec] * jax.nn.sigmoid(-forget)
        log_forget = jnp.log1p(-key_gate)
        gains = gain[:, lane_rec]
        mine_rate = [rates[s, pl.ds(sp * heads + h, 1), :] for h in range(heads)]
        if heads < 8:
            mine_rate.append(jnp.zeros((8 - heads, 2 * span), F32))
        mine_rate = jnp.concatenate(mine_rate, axis=0)
        halves = []
        for c in range(2):
            part = slice(c * span, (c + 1) * span)
            cum = jnp.dot(lower, log_forget[part], precision=lax.Precision.HIGHEST)
            extra = jnp.dot(mine_rate[:, part], upper, precision=lax.Precision.HIGHEST)
            extra_t = extra.T
            grow = jnp.exp(cum)
            query_grow = query[part] * grow
            key_grow = (key_gate[part] / grow).astype(BF16)
            last = cum[span - 1 :, :]
            key_last = key_gate[part] * jnp.exp(last - cum)
            last_decay = jnp.exp(last)
            pieces = []
            for h in range(heads):
                lanes = slice(h * DK, (h + 1) * DK)
                row = extra[h : h + 1]
                column = extra_t[:, h : h + 1]
                end = row[:, span - 1 :]
                scores = lax.dot_general(
                    query_grow[:, lanes].astype(BF16), key_grow[:, lanes], CONTRACT_LAST,
                    preferred_element_type=F32,
                )
                decay = jnp.exp(jnp.where(causal, column - row, 0.0))
                scores = jnp.where(causal, scores * decay, 0.0).astype(BF16)
                values = value[part, lanes]
                before = state[h]
                raw = jnp.dot(scores, values, preferred_element_type=F32)
                raw = raw + lax.dot_general(
                    (query_grow[:, lanes] * jnp.exp(column)).astype(BF16), before.astype(BF16),
                    CONTRACT_LAST, preferred_element_type=F32,
                )
                keys = (key_last[:, lanes] * jnp.exp(end - column)).astype(BF16)
                state[h] = before * (last_decay[:, lanes] * jnp.exp(end)) + lax.dot_general(
                    values, keys, CONTRACT_FIRST, preferred_element_type=F32
                )
                square = jnp.mean(raw * raw, axis=-1, keepdims=True)
                pieces.append((raw * lax.rsqrt(square + 1e-06) * gains[:, lanes]).astype(BF16))
            halves.append(jnp.concatenate(pieces, axis=1))
        both[s, :, :rec] = jnp.concatenate(halves, axis=0)

    lag = jnp.where(sp < 2, 0, 1)
    first_pieces, last_pieces = range(chunks // 2), range(chunks // 2, chunks)

    def step(i, carry):
        s = i - lag

        @pl.when(jnp.logical_and(s >= 0, s < n_sp))
        def _():
            recur(s)

        @pl.when(i == 0)
        def _():
            relays(high, bottom, 1, early)
            ring_late_on(2)
            relays(low, top - 1, -1)
            relays(high, bottom, 1, late)

        pl.when(i == 1 - lag)(functools.partial(ring_late_on, 3))
        relays(jnp.logical_and(i == 1, low), top, -1, early)
        relays(jnp.logical_and(i == 1, high), 1, 1, early)

        @pl.when(i == 1)
        def _():
            ring_late_end()
            convolve(0)

        ready = jnp.logical_and(i > 0, s < n_sp)

        @pl.when(jnp.logical_and(ready, s > 0))
        def _():
            convolve(s)

        pl.when(ready)(functools.partial(project_out, s))
        relays(jnp.logical_and(i == 1, low), top, -1, late)
        relays(jnp.logical_and(i == 1, high), 1, 1, late)

        @pl.when(ready)
        def _():
            pass_on(s, first_pieces)
            pl.when(jnp.logical_not(jnp.logical_and(sp == 0, s == 1)))(
                functools.partial(pass_on, s, last_pieces)
            )

        pl.when(jnp.logical_and(i == 3, high))(functools.partial(join, 0))
        return carry

    lax.fori_loop(0, n_sp + 1, step, 0)

    @pl.when(lag == 0)
    def _():
        pl.when(sp == 0)(functools.partial(pass_on, 1, last_pieces))
        project_out(0)
        pass_on(0)

    @pl.when(sp == 1)
    def _():
        for s in range(2, n_sp):
            join(s)

    @pl.when(sp == n_sp - 2)
    def _():
        for s in range(1, n_sp - 2):
            join(s)

    for d in range(n_sp):
        comes = sp != d
        if d == 0:
            comes = jnp.logical_and(comes, sp < 2)
        if d == n_sp - 1:
            comes = jnp.logical_and(comes, sp > n_sp - 3)

        @pl.when(comes)
        def _():
            arrived(z_recv.at[d], zr_sem.at[d])
            for c in range(chunks):
                mine[sp, c] = mine[sp, c] + z_recv[d, c].astype(F32)

    for c in range(chunks):
        out[:, c * chunk : (c + 1) * chunk] = mine[sp, c].astype(BF16)

    gone(rates.at[pl.ds(0, n_sp - 1)], RATE)
    gone(win.at[pl.ds(0, (n_sp - 1) * rows)], FIRST)
    gone(wcon.at[pl.ds(0, (n_sp - 1) * rows)], CON)
    gone(wout.at[pl.ds(0, n_sp - 1)], OUT)
    gone(win.at[pl.ds(0, 3 * n_sp * rows)], IN_RING)
    gone(wcon.at[pl.ds(0, 3 * n_sp * rows)], CON_RING)
    gone(wout.at[pl.ds(0, 3 * n_sp)], OUT_RING)
    gone(tokens.at[pl.ds(0, n_sp)], ACROSS)
    gone(sib_send, SIBLING)
    gone(z_send.at[pl.ds(0, n_sp - 1)], SUMS)

    @pl.when(sp < n_sp - 1)
    def _():
        gone(tokens.at[0], UP)

    @pl.when(sp > 0)
    def _():
        gone(tokens.at[0], DOWN)

    @pl.when(inner)
    def _():
        gone(tokens.at[pl.ds(0, n_sp - 1)], RELAY)


def sequence_shards(n_sp, n_fs, *arrays):
    (tok, wq, wf, wv, cg, cm, ci, headroom, rate, init, gain, taps, bias, ro, co) = arrays
    span, wide = tok.shape[1:]
    rec, con = wq.shape[1] // n_sp, cg.shape[1] // n_sp
    heads = rec // DK
    chunk = wide // OUT_PIECES
    hbm = pl.BlockSpec(memory_space=pl.ANY)
    vmem = pl.BlockSpec(memory_space=pltpu.VMEM)
    dma = pltpu.SemaphoreType.DMA
    flat = (n_sp, OUT_PIECES, span, chunk)
    mixed = pl.pallas_call(
        functools.partial(layer_kernel, n_sp, n_fs),
        out_shape=jax.ShapeDtypeStruct((span, wide), BF16),
        in_specs=[hbm] * 11 + [vmem] * 4,
        out_specs=vmem,
        scratch_shapes=[
            pltpu.VMEM((2 * n_sp, span, wide), BF16),
            pltpu.VMEM((wide, 3 * rec), BF16),
            pltpu.VMEM((wide, 3 * con), BF16),
            pltpu.VMEM((n_sp * n_fs, rec + con, wide // (n_sp * n_fs)), BF16),
            pltpu.VMEM((n_sp,) + rate.shape[1:], F32),
            pltpu.VMEM((heads, DK, DK), F32),
            pltpu.VMEM((heads, DK, DK), F32),
            pltpu.VMEM((8 + 2 * span, con), F32),
            pltpu.VMEM((n_sp, 2 * span, rec + con), BF16),
            pltpu.VMEM(flat, BF16),
            pltpu.VMEM(flat, BF16),
            pltpu.VMEM(flat, F32),
            pltpu.VMEM(flat, BF16),
            pltpu.VMEM(flat, BF16),
            pltpu.VMEM((2,) + flat[1:], BF16),
            pltpu.VMEM((n_sp, wide // (n_sp * n_fs), 3 * rec), BF16),
            pltpu.VMEM((n_sp, wide // (n_sp * n_fs), 3 * con), BF16),
            pltpu.VMEM((n_sp, rec + con, wide // (n_sp * n_fs)), BF16),
            dma((n_sp,)),
            dma((5,)),
            dma((SENDS,)),
            dma((n_sp,)),
            dma((n_sp,)),
            dma((n_sp,)),
            dma((2, n_sp)),
            dma((n_sp,)),
            dma((n_sp,)),
            dma((4,)),
            dma((n_sp, TOKEN_PIECES)),
            dma((n_sp,)),
            dma((n_sp, OUT_PIECES)),
            dma((n_sp,)),
            dma((2, OUT_PIECES)),
        ],
        compiler_params=pltpu.CompilerParams(
            collective_id=0, has_side_effects=True, vmem_limit_bytes=60 * 2**20
        ),
    )(
        tok[0], wq, wf, wv, cg, cm, ci, ro, co, rate[0], init[0], headroom[None], gain[None],
        taps, bias[None],
    )
    return mixed[None]


def choose_plan(sizes, *arrays):
    n_sp, n_fs = sizes["sp"], sizes["fs"]
    rows, rec = arrays[1].shape
    con = arrays[4].shape[1]
    span = arrays[0].shape[1]
    even = (
        sizes["tp"] == 2
        and n_fs == 4
        and n_sp == 4
        and arrays[0].shape[2] % (n_fs * n_sp * 128) == 0
        and arrays[0].shape[0] == 1
        and rec % (n_sp * DK) == 0
        and rec // (n_sp * DK) <= 8
        and arrays[8].shape[1] % 8 == 0
        and con % (n_sp * 128) == 0
        and rows % 128 == 0
        and span == DK
        and arrays[13].shape[1] % 128 == 0
    )
    return sequence_shards(n_sp, n_fs, *arrays) if even else shards(*arrays)


def solution(mesh):
    in_specs = (
        P("fs", ("sp", "tp"), None),
        P(("sp", "fs"), "tp"),
        P(("sp", "fs"), "tp"),
        P(("sp", "fs"), "tp"),
        P(("sp", "fs"), "tp"),
        P(("sp", "fs"), "tp"),
        P(("sp", "fs"), "tp"),
        P("tp"),
        P("fs", "tp", "sp"),
        P("fs", "tp", None, None),
        P("tp"),
        P(None, "tp"),
        P("tp"),
        P("tp", ("sp", "fs")),
        P("tp", ("sp", "fs")),
    )
    out_specs = P("fs", ("sp", "tp"), None)
    body = functools.partial(choose_plan, dict(mesh.shape))
    return jax.shard_map(body, mesh=mesh, in_specs=in_specs, out_specs=out_specs, check_vma=False)
```

```python
import functools

import jax
import jax.numpy as jnp
from jax import lax
from jax.experimental import pallas as pl
from jax.experimental.pallas import tpu as pltpu
from jax.sharding import PartitionSpec as P

DK = 128
KW = 3
BLOCK_POSITIONS = 64


def carried_in(part, axis, combine, identity):
    place = lax.axis_index(axis)
    gathered = jax.tree.map(lambda a: lax.all_gather(a, axis), part)
    state = jax.tree.map(lambda a, e: jnp.zeros_like(a) + jnp.asarray(e, a.dtype), part, identity)

    def one(hop, state):
        return combine(
            state, jax.tree.map(lambda a: lax.dynamic_index_in_dim(a, hop, 0, False), gathered)
        )

    return lax.fori_loop(0, place, one, state)


def from_behind(block, axis, distance):
    devices = range(lax.axis_size(axis))
    route = [(i - distance, i) for i in devices if i - distance in devices]
    return lax.ppermute(block, axis, route)


def to_blocks(values, number_of_heads):
    number_of_blocks = values.shape[0] // BLOCK_POSITIONS
    return jnp.transpose(
        values.reshape(number_of_blocks, BLOCK_POSITIONS, number_of_heads, DK), (2, 0, 1, 3)
    )


def within_block_recurrence(
    query_vectors, forget_logits, value_vectors, gate_headroom, extra_rates
):
    number_of_heads = extra_rates.shape[0]
    number_of_blocks = query_vectors.shape[0] // BLOCK_POSITIONS
    query_scaled = to_blocks(query_vectors.astype(jnp.float32), number_of_heads) * DK ** (-0.5)
    gated_key = to_blocks(
        gate_headroom[None, :] * jax.nn.sigmoid(-forget_logits.astype(jnp.float32)), number_of_heads
    )
    forget_log_rate = (
        jnp.log1p(-gated_key)
        + extra_rates.reshape(number_of_heads, number_of_blocks, BLOCK_POSITIONS)[..., None]
    )
    values = to_blocks(value_vectors.astype(jnp.float32), number_of_heads)
    cumulative = jnp.cumsum(forget_log_rate, axis=2)
    query_decayed = query_scaled * jnp.exp(cumulative)
    key_decayed = gated_key * jnp.exp(-cumulative)
    scores = jnp.einsum(
        "hnik,hnjk->hnij", query_decayed, key_decayed, precision=lax.Precision.HIGHEST
    )
    causal = jnp.tril(jnp.ones((BLOCK_POSITIONS, BLOCK_POSITIONS), dtype=bool))
    scores = jnp.where(causal, scores, 0.0)
    within = jnp.einsum("hnij,hnjv->hniv", scores, values, precision=lax.Precision.HIGHEST)
    final_log = cumulative[:, :, -1, :]
    contrib = jnp.einsum(
        "hnck,hncv->hnkv",
        gated_key * jnp.exp(final_log[:, :, None, :] - cumulative),
        values,
        precision=lax.Precision.HIGHEST,
    )
    decays = jnp.exp(final_log)

    def advance(current, block_pair):
        return (block_pair[0][..., None] * current + block_pair[1], current)

    empty_state = jnp.zeros((number_of_heads, DK, DK), jnp.float32)
    local_total, entering = lax.scan(
        advance, empty_state, (jnp.moveaxis(decays, 1, 0), jnp.moveaxis(contrib, 1, 0))
    )
    entering = jnp.moveaxis(entering, 0, 1)
    before = jnp.exp(jnp.cumsum(final_log, axis=1) - final_log)
    device_decay = jnp.exp(jnp.sum(final_log, axis=1))
    return (query_decayed, within, entering, before, device_decay, local_total)


def finish(query_decayed, within, entering, before, carried, head_norm_gain):
    number_of_heads = query_decayed.shape[0]
    states = entering + before[..., None] * carried[:, None]
    carried_term = jnp.einsum(
        "hnck,hnkv->hncv", query_decayed, states, precision=lax.Precision.HIGHEST
    )
    length = query_decayed.shape[1] * BLOCK_POSITIONS
    recurrence_unnormed = jnp.transpose(within + carried_term, (1, 2, 0, 3)).reshape(
        length, number_of_heads, DK
    )
    mean_square = jnp.mean(recurrence_unnormed * recurrence_unnormed, axis=-1, keepdims=True)
    rec_out = (
        recurrence_unnormed
        * lax.rsqrt(mean_square + 1e-06)
        * head_norm_gain.reshape(number_of_heads, DK)
    )
    return rec_out.reshape(length, number_of_heads * DK).astype(jnp.bfloat16)


def chain_combine(earlier_part, later_part):
    return (
        earlier_part[0] * later_part[0],
        later_part[0][..., None] * earlier_part[1] + later_part[1],
    )


def shards(
    tokens,
    query_weight,
    forget_weight,
    value_weight,
    convolution_gate_weight,
    convolution_multiplier_weight,
    convolution_input_weight,
    gate_headroom,
    added_log_rate,
    initial_state,
    head_norm_gain,
    convolution_taps,
    convolution_bias,
    recurrence_output_weight,
    convolution_output_weight,
):
    own_rows = tokens[0]
    gathered = (
        lax.all_gather(query_weight, ("sp", "fs"), axis=0, tiled=True),
        lax.all_gather(forget_weight, ("sp", "fs"), axis=0, tiled=True),
        lax.all_gather(value_weight, ("sp", "fs"), axis=0, tiled=True),
        lax.all_gather(convolution_gate_weight, ("sp", "fs"), axis=0, tiled=True),
        lax.all_gather(convolution_multiplier_weight, ("sp", "fs"), axis=0, tiled=True),
        lax.all_gather(convolution_input_weight, ("sp", "fs"), axis=0, tiled=True),
        lax.all_gather(recurrence_output_weight, ("sp", "fs"), axis=1, tiled=True),
        lax.all_gather(convolution_output_weight, ("sp", "fs"), axis=1, tiled=True),
    )
    in_weights = gathered[:6]
    out_rec = gathered[6]
    out_conv = gathered[7]
    block_rows = lax.all_gather(own_rows, "tp", axis=0, tiled=True)
    projected = jnp.concatenate(
        [
            jnp.dot(block_rows, weight, preferred_element_type=jnp.float32).astype(jnp.bfloat16)
            for weight in in_weights
        ],
        axis=1,
    )
    rec_width = query_weight.shape[1]
    conv_width = convolution_gate_weight.shape[1]
    query_vectors = projected[:, :rec_width]
    forget_logits = projected[:, rec_width : 2 * rec_width]
    value_vectors = projected[:, 2 * rec_width : 3 * rec_width]
    conv_base = 3 * rec_width
    conv_gate = projected[:, conv_base : conv_base + conv_width]
    conv_mult = projected[:, conv_base + conv_width : conv_base + 2 * conv_width]
    conv_input = projected[:, conv_base + 2 * conv_width : conv_base + 3 * conv_width]
    query_decayed, within, entering, before, device_decay, local_total = within_block_recurrence(
        query_vectors, forget_logits, value_vectors, gate_headroom, added_log_rate[0]
    )
    conv_prod = conv_mult.astype(jnp.float32) * conv_input.astype(jnp.float32)
    length = conv_prod.shape[0]
    tail_rows = conv_prod[length - (KW - 1) :]
    unit_decay = jnp.ones_like(device_decay)
    empty_state = jnp.zeros_like(local_total)
    prior_decay, prior_state = carried_in(
        (device_decay, local_total), "sp", chain_combine, (unit_decay, empty_state)
    )
    prior_rows = from_behind(tail_rows, "sp", 1)
    carried = prior_decay[..., None] * initial_state[0] + prior_state
    rec_out = finish(query_decayed, within, entering, before, carried, head_norm_gain)
    extended = jnp.concatenate([prior_rows, conv_prod], axis=0)
    conv_y = jnp.broadcast_to(convolution_bias[None, :], conv_prod.shape)
    for j in range(KW):
        conv_y = conv_y + convolution_taps[j][None, :] * extended[j : j + length]
    conv_out = (conv_gate.astype(jnp.float32) * conv_y).astype(jnp.bfloat16)
    mixed = lax.psum_scatter(
        (
            jnp.dot(rec_out, out_rec, preferred_element_type=jnp.float32)
            + jnp.dot(conv_out, out_conv, preferred_element_type=jnp.float32)
        ).astype(jnp.bfloat16),
        "tp",
        scatter_dimension=0,
        tiled=True,
    )
    return mixed[None]


MESH = pl.DeviceIdType.MESH
F32 = jnp.float32
BF16 = jnp.bfloat16
CONTRACT_LAST = (((1,), (1,)), ((), ()))
CONTRACT_FIRST = (((0,), (0,)), ((), ()))
TOKEN_PIECES = 4
SENDS = 13
(
    UP, DOWN, ACROSS, RELAY, RATE, FIRST, CON, OUT, IN_RING, CON_RING, OUT_RING, SIBLING, SUMS,
) = range(SENDS)
OUT_PIECES = 8


def layer_kernel(
    n_sp, n_fs, tok, wq, wf, wv, cg, cm, ci, ro, co, rate, init, headroom, gain, taps, bias,
    out, tokens, win, wcon, wout, rates, first_state, state, ext, both, sib_send, sib_recv, mine,
    z_send, z_recv, rl_recv, stage_in, stage_con, stage_out, loc_in, loc_sem, out_sem, win_z,
    wcon_z, wout_z, in_f, con_f, out_f, out_end, end_f, tok_z, tok_t, sib_sem, zr_sem, rl_sem,
):
    sp, fs, tp = lax.axis_index("sp"), lax.axis_index("fs"), lax.axis_index("tp")
    other = 1 - tp
    rows = wq.shape[0]
    rec = wq.shape[1] // n_sp
    con = cg.shape[1] // n_sp
    span = tok.shape[0]
    heads = rec // DK
    wide = tok.shape[1]
    lanes_out = ro.shape[1]
    chunks, chunk = mine.shape[1], mine.shape[3]
    sub = span // TOKEN_PIECES
    shards_in = chunk // lanes_out

    def peer(**where):
        return {"sp": where.get("sp", sp), "fs": where.get("fs", fs), "tp": where.get("tp", tp)}

    half_ring = n_fs // 2

    def ring(p):
        return p + (p // half_ring) * (3 * half_ring - 1 - 2 * p)

    at_ring = ring(fs)
    left = ring(lax.rem(at_ring + n_fs - 1, n_fs))
    right = ring(lax.rem(at_ring + 1, n_fs))
    across = ring(lax.rem(at_ring + 2, n_fs))
    sibling = peer(tp=other)

    depth = rec + con
    rec_parts = [(ref, i * rec, rec) for i, ref in enumerate((wq, wf, wv))]
    con_parts = [(ref, i * con, con) for i, ref in enumerate((cg, cm, ci))]

    def in_rows(s, f, first, count):
        return win.at[pl.ds(pl.multiple_of((s * n_fs + f) * rows + first, count), count)]

    def con_rows(s, f):
        return wcon.at[pl.ds(pl.multiple_of((s * n_fs + f) * rows, rows), rows)]

    def out_slot(s, f):
        return wout.at[s * n_fs + f]

    def stage(z, in_to, con_to, out_to, place):
        copies = []
        for some, to, sem in ((rec_parts, in_to, loc_in.at[place]), (con_parts, con_to, loc_sem.at[0])):
            for ref, at, width in some:
                src = ref.at[:, pl.ds(pl.multiple_of(z * width, width), width)]
                copies.append((src, to.at[:, pl.ds(at, width)], sem))
        for ref, at, width in ((ro, 0, rec), (co, rec, con)):
            src = ref.at[pl.ds(pl.multiple_of(z * width, width), width)]
            copies.append((src, out_to.at[pl.ds(at, width)], loc_sem.at[1]))
        return [pltpu.make_async_copy(*copy) for copy in copies]

    below, above = sp, n_sp - 1 - sp
    fewer = jnp.minimum(below, above)
    upward = jnp.where(below < above, 1, -1)
    edge = fewer == 0

    def near(j):
        paired = j <= 2 * fewer
        side = jnp.where(paired, upward * (1 - 2 * (j % 2)), upward)
        return sp + side * jnp.where(paired, (j + 1) // 2, j - fewer)

    def to_send(j):
        if j == 1:
            return near(1)
        return jnp.where(edge, near(n_sp + 1 - j), near(j))

    local = []
    for j in range(1, n_sp):
        local += stage(to_send(j), stage_in.at[j], stage_con.at[j], stage_out.at[j], j)
    local += stage(sp, in_rows(sp, fs, 0, rows), con_rows(sp, fs), out_slot(sp, fs), 0)
    others = [
        (tok, tokens.at[sp * 2 + tp]), (rate, rates.at[sp]),
        (init.at[pl.ds(sp * heads, heads)], first_state),
    ]
    others = [pltpu.make_async_copy(*pair, loc_sem.at[2 + i]) for i, pair in enumerate(others)]
    for copy in local + others:
        copy.start()

    barrier = pltpu.get_barrier_semaphore()
    for j in range(1, n_sp):
        pl.semaphore_signal(barrier, inc=1, device_id=peer(sp=near(j)), device_id_type=MESH)
    for f in (left, right):
        pl.semaphore_signal(barrier, inc=1, device_id=peer(fs=f), device_id_type=MESH)
    pl.semaphore_signal(barrier, inc=1, device_id=sibling, device_id_type=MESH)
    pl.semaphore_wait(barrier, n_sp + 2)

    def remote(src, dst, send, recv, to):
        return pltpu.make_async_remote_copy(
            src_ref=src, dst_ref=dst, send_sem=send, recv_sem=recv, device_id=to, device_id_type=MESH,
        )

    def arrived(ref, recv):
        remote(ref, ref, recv, recv, sibling).wait_recv()

    def gone(ref, i):
        remote(ref, ref, out_sem.at[i], out_sem.at[i], sibling).wait_send()

    def tok_piece(ref, c):
        return ref.at[pl.ds(c * sub, sub)]

    def token_slot(s, t, c):
        return tok_piece(tokens.at[s * 2 + t], c)

    def own_tokens(send, to):
        return [
            remote(tok_piece(tok, c), token_slot(sp, tp, c), send, tok_z.at[sp, c], to)
            for c in range(TOKEN_PIECES)
        ]

    def own_up():
        return own_tokens(out_sem.at[UP], peer(sp=sp + 1))

    def own_down():
        return own_tokens(out_sem.at[DOWN], peer(sp=sp - 1))

    def to_sibling(s, c, src=None):
        slot = token_slot(s, tp, c)
        return remote(slot if src is None else src, slot, out_sem.at[ACROSS], tok_t.at[s], sibling)

    def relayed(s, c, to):
        slot = token_slot(s, tp, c)
        return remote(slot, slot, out_sem.at[RELAY], tok_z.at[s, c], to)

    def start_all(copies):
        for copy in copies:
            copy.start()

    def send_in(j):
        to = peer(sp=to_send(j))
        arrived(stage_in.at[j], loc_in.at[j])
        remote(rate, rates.at[sp], out_sem.at[RATE], end_f.at[2], to).start()
        remote(
            stage_in.at[j], in_rows(sp, fs, 0, rows), out_sem.at[FIRST], win_z.at[sp], to
        ).start()

    def con_copies():
        return [
            remote(
                stage_con.at[j], con_rows(sp, fs), out_sem.at[CON], wcon_z.at[sp],
                peer(sp=to_send(j)),
            )
            for j in range(1, n_sp)
        ]

    def out_copies():
        return [
            remote(
                stage_out.at[j], out_slot(sp, fs), out_sem.at[OUT], wout_z.at[sp],
                peer(sp=to_send(j)),
            )
            for j in range(1, n_sp)
        ]

    low, high = sp == 1, sp == n_sp - 2
    send_in(1)

    for j in range(2, n_sp):
        send_in(j)
    arrived(stage_con, loc_sem.at[0])
    arrived(stage_out, loc_sem.at[1])
    start_all(con_copies()[:1])
    for copy in others:
        copy.wait()

    @pl.when(sp == 0)
    def _():
        start_all(own_up())

    @pl.when(sp == n_sp - 1)
    def _():
        start_all(own_down())

    start_all(out_copies()[:1])
    for c in range(TOKEN_PIECES):
        to_sibling(sp, c, tok_piece(tok, c)).start()

    arrived(in_rows(sp, fs, 0, rows), loc_in.at[0])

    def z_in(j):
        z = near(j)
        arrived(in_rows(z, fs, 0, rows), win_z.at[z])

    def z_con(j):
        z = near(j)
        arrived(con_rows(z, fs), wcon_z.at[z])

    def z_out(j):
        z = near(j)
        arrived(out_slot(z, fs), wout_z.at[z])

    def place(j):
        return near(j) if j else sp

    def ring_of(k, whole, part, sem, landed, last):
        s = place(k)
        copies = (
            (whole(s, fs), landed.at[0, k], right), (whole(s, fs), landed.at[1, k], left),
            (part(s, left, 0), last, right), (part(s, right, 1), last, left),
        )
        return [remote(ref, ref, out_sem.at[sem], to_sem, peer(fs=to)) for ref, to_sem, to in copies]

    def pass_ring(k, whole, landed, copies):
        s = place(k)
        arrived(whole(s, left), landed.at[0, k])
        copies[2].start()
        arrived(whole(s, right), landed.at[1, k])
        copies[3].start()

    def in_whole(s, f):
        return in_rows(s, f, 0, rows)

    def in_ring(k):
        half = rows // 2
        return ring_of(
            k, in_whole, lambda s, f, h: in_rows(s, f, h * half, half), IN_RING, in_f, end_f.at[0]
        )

    def con_ring(k):
        half = rows // 2
        return ring_of(
            k, con_rows, lambda s, f, h: con_rows(s, f).at[pl.ds(h * half, half)], CON_RING, con_f,
            end_f.at[1],
        )

    def out_ring(k):
        half = depth // 2
        return ring_of(
            k, out_slot, lambda s, f, h: out_slot(s, f).at[pl.ds(h * half, half)], OUT_RING, out_f,
            out_end.at[k],
        )

    def ring_in(k):
        start_all(in_ring(k)[:2])

    def ring_in_on(k):
        pass_ring(k, in_whole, in_f, in_ring(k))

    def ring_con(k):
        start_all(con_ring(k)[:2])

    def ring_con_on(k):
        pass_ring(k, con_rows, con_f, con_ring(k))

    def ring_out(k):
        start_all(out_ring(k)[:2])

    def ring_out_on(k):
        pass_ring(k, out_slot, out_f, out_ring(k))

    def relay(s, c, step_by):
        arrived(token_slot(s, tp, c), tok_z.at[s, c])
        if step_by:
            relayed(s, c, peer(sp=sp + step_by)).start()
        to_sibling(s, c).start()

    def relays(when, s, step_by, pieces=range(TOKEN_PIECES)):
        @pl.when(when)
        def _():
            for c in pieces:
                relay(s, c, step_by)

    early, late = range(TOKEN_PIECES // 2), range(TOKEN_PIECES // 2, TOKEN_PIECES)
    bottom, top = 0, n_sp - 1

    def second_in():
        z_in(2)
        ring_in(2)

    def first_con():
        z_con(1)
        ring_con(1)

    inner = jnp.logical_not(edge)
    ring_in(0)
    z_in(1)
    ring_in(1)
    pl.when(inner)(second_in)
    ring_in_on(0)
    ring_con(0)

    @pl.when(low)
    def _():
        start_all(own_down())

    @pl.when(high)
    def _():
        start_all(own_up())

    ring_in_on(1)

    @pl.when(edge)
    def _():
        first_con()
        second_in()

    z_in(3)
    ring_in(3)
    start_all(con_copies()[1:])

    @pl.when(high)
    def _():
        start_all(own_down())
        start_all(out_copies()[1:])

    pl.when(inner)(first_con)
    ring_in_on(2)
    relays(low, bottom, 1, early)
    relays(high, top, -1, early)
    relays(low, bottom, 1, late)
    relays(high, top, -1, late)

    @pl.when(jnp.logical_not(high))
    def _():
        start_all(out_copies()[1:])

    @pl.when(low)
    def _():
        start_all(own_up())

    ring_in_on(3)
    ring_con_on(0)
    ring_con_on(1)
    relays(sp == 0, 1, 0)
    relays(sp == top, top - 1, 0)
    z_con(2)
    ring_con(2)
    z_con(3)
    ring_con(3)
    ring_out(0)
    z_out(1)
    ring_out(1)
    relays(low, top - 1, -1)
    relays(high, bottom, 1)
    ring_con_on(2)
    ring_con_on(3)

    late_start = sp < 2
    start = jnp.where(late_start, 1, 0)

    def near_out_on():
        ring_out_on(0)
        ring_out_on(1)
        for k in (2, 3):
            z_out(k)
            ring_out(k)

    pl.when(jnp.logical_not(late_start))(near_out_on)
    arrived(win.at[pl.ds(0, n_sp * rows)], end_f.at[0])
    arrived(rates.at[pl.ds(0, n_sp - 1)], end_f.at[2])

    for h in range(heads):
        state[h] = first_state[h].T
    ext[0:8] = jnp.zeros((8, con), F32)
    lane_rec = pl.ds(pl.multiple_of(sp * rec, rec), rec)
    lane_con = pl.ds(pl.multiple_of(sp * con, con), con)
    row_id = lax.broadcasted_iota(jnp.int32, (span, span), 0)
    col_id = lax.broadcasted_iota(jnp.int32, (span, span), 1)
    causal = row_id >= col_id
    lower = causal.astype(F32)
    upper = (row_id <= col_id).astype(F32)
    length = 2 * span

    def sib_copy(s, c):
        return remote(sib_send.at[s, c], sib_recv.at[s, c], out_sem.at[SIBLING], sib_sem.at[s, c], sibling)

    def final_copy(s, c, to):
        return remote(
            z_send.at[s, c], z_recv.at[sp, c], out_sem.at[SUMS], zr_sem.at[sp], peer(sp=to)
        )

    def joint_copy(s, c, to):
        landing, sem = rl_recv.at[2, c], rl_sem.at[2, c]
        return remote(z_send.at[s, c], landing, out_sem.at[SUMS], sem, peer(sp=to))

    def edge_copy(s, c, to):
        t = lax.rem(s, 2)
        landing, sem = rl_recv.at[t, c], rl_sem.at[t, c]
        return remote(z_send.at[s, c], landing, out_sem.at[SUMS], sem, peer(sp=to))

    def through_low(s):
        return jnp.logical_and(sp == 0, s >= 2)

    def through_high(s):
        return jnp.logical_and(sp == n_sp - 1, s <= n_sp - 3)

    def plain(s):
        return jnp.logical_or(
            jnp.logical_and(sp == 0, s == 1), jnp.logical_and(sp == top, s == top - 1)
        )

    per_slot = n_fs // shards_in

    def pieces_of(slots):
        return [slot * per_slot + i for slot in slots for i in range(per_slot)]

    def own_slots(h):
        return [place(2 * h), place(2 * h + 1)]

    def pass_on(s, h):
        for c in pieces_of(own_slots(h)):
            sib_copy(s, c).wait_recv()
            total = mine[s, c] + sib_recv[s, c].astype(F32)
            mine[s, c] = total

            @pl.when(jnp.logical_and(edge, s != sp))
            def _():
                z_send[s, c] = total.astype(BF16)

            @pl.when(plain(s))
            def _():
                final_copy(s, c, s).start()

            @pl.when(through_low(s))
            def _():
                edge_copy(s, c, 1).start()

            @pl.when(through_high(s))
            def _():
                edge_copy(s, c, n_sp - 2).start()

    def join(t, h):
        s = jnp.where(low, (2, 3, 0)[t], (0, 1, 3)[t])
        to = jnp.where(low, (2, 2, 0)[t], (1, 1, 3)[t])
        rising = low if t < 2 else high
        slots = [jnp.where(rising, 2 * h + i, n_sp - 1 - 2 * h - i) for i in range(2)]
        on = (high, low, None)[t]
        for c in pieces_of(slots):
            arrived(rl_recv.at[t, c], rl_sem.at[t, c])
            z_send[s, c] = (mine[s, c] + rl_recv[t, c].astype(F32)).astype(BF16)
            if on is None:
                final_copy(s, c, to).start()
            else:
                pl.when(on)(joint_copy(s, c, to).start)
                pl.when(jnp.logical_not(on))(final_copy(s, c, to).start)

    def project_out(s, h):
        for slot in own_slots(h):
            columns = jnp.concatenate([wout[slot * n_fs + i] for i in range(n_fs)], axis=1)
            partial = jnp.dot(both[s], columns, preferred_element_type=F32)
            first = partial[:span]
            second = partial[span:]
            own = jnp.where(tp == 0, first, second)
            given = jnp.where(tp == 0, second, first).astype(BF16)
            for i in range(per_slot):
                c = slot * per_slot + i
                mine[s, c] = own[:, i * chunk : (i + 1) * chunk]
                sib_send[s, c] = given[:, i * chunk : (i + 1) * chunk]
                sib_copy(s, c).start()

    def convolve(s):
        block = jnp.concatenate([tokens[2 * s], tokens[2 * s + 1]], axis=0)
        projected = jnp.dot(block, wcon[...], preferred_element_type=F32).astype(BF16).astype(F32)
        prod = projected[:, con : 2 * con] * projected[:, 2 * con :]
        ext[8:] = prod
        conv = jnp.broadcast_to(bias[:, lane_con], prod.shape)
        for j in range(KW):
            conv = conv + taps[j : j + 1, lane_con] * ext[pl.ds(8 - (KW - 1) + j, length)]
        ext[0:8] = ext[length:]
        both[s, :, rec:] = (projected[:, :con] * conv).astype(BF16)

    def recur(s):
        relays(jnp.logical_and(edge, (s - sp) * (s - sp) > 1), s, 0)
        arrived(tokens.at[2 * s + other], tok_t.at[s])
        block = jnp.concatenate([tokens[2 * s], tokens[2 * s + 1]], axis=0)

        def project(at, width):
            return jnp.dot(
                block, win[:, pl.ds(at, width)], preferred_element_type=F32
            ).astype(BF16)

        query = project(0, rec).astype(F32) * DK ** (-0.5)
        forget = project(rec, rec).astype(F32)
        value = project(2 * rec, rec)
        key_gate = headroom[:, lane_rec] * jax.nn.sigmoid(-forget)
        log_forget = jnp.log1p(-key_gate)
        gains = gain[:, lane_rec]
        mine_rate = [rates[s, pl.ds(sp * heads + h, 1), :] for h in range(heads)]
        if heads < 8:
            mine_rate.append(jnp.zeros((8 - heads, 2 * span), F32))
        mine_rate = jnp.concatenate(mine_rate, axis=0)
        halves = []
        for c in range(2):
            part = slice(c * span, (c + 1) * span)
            cum = jnp.dot(lower, log_forget[part], precision=lax.Precision.HIGHEST)
            extra = jnp.dot(mine_rate[:, part], upper, precision=lax.Precision.HIGHEST)
            extra_t = extra.T
            grow = jnp.exp(cum)
            query_grow = query[part] * grow
            key_grow = (key_gate[part] / grow).astype(BF16)
            last = cum[span - 1 :, :]
            key_last = key_gate[part] * jnp.exp(last - cum)
            last_decay = jnp.exp(last)
            pieces = []
            for h in range(heads):
                lanes = slice(h * DK, (h + 1) * DK)
                row = extra[h : h + 1]
                column = extra_t[:, h : h + 1]
                end = row[:, span - 1 :]
                scores = lax.dot_general(
                    query_grow[:, lanes].astype(BF16), key_grow[:, lanes], CONTRACT_LAST,
                    preferred_element_type=F32,
                )
                decay = jnp.exp(jnp.where(causal, column - row, 0.0))
                scores = jnp.where(causal, scores * decay, 0.0).astype(BF16)
                values = value[part, lanes]
                before = state[h]
                raw = jnp.dot(scores, values, preferred_element_type=F32)
                raw = raw + lax.dot_general(
                    (query_grow[:, lanes] * jnp.exp(column)).astype(BF16), before.astype(BF16),
                    CONTRACT_LAST, preferred_element_type=F32,
                )
                keys = (key_last[:, lanes] * jnp.exp(end - column)).astype(BF16)
                state[h] = before * (last_decay[:, lanes] * jnp.exp(end)) + lax.dot_general(
                    values, keys, CONTRACT_FIRST, preferred_element_type=F32
                )
                square = jnp.mean(raw * raw, axis=-1, keepdims=True)
                pieces.append((raw * lax.rsqrt(square + 1e-06) * gains[:, lanes]).astype(BF16))
            halves.append(jnp.concatenate(pieces, axis=1))
        both[s, :, :rec] = jnp.concatenate(halves, axis=0)

    def out_end_of(h):
        for k in (2 * h, 2 * h + 1):
            arrived(out_slot(place(k), across), out_end.at[k])

    def give(s, *halves):
        for h in halves:
            project_out(s, h)
        for h in halves:
            pass_on(s, h)

    def step(s, carry):
        recur(s)
        pl.when(jnp.logical_and(s == 0, late_start))(near_out_on)

        @pl.when(s == 2 * start)
        def _():
            ring_out_on(2)
            ring_out_on(3)

        relays(jnp.logical_and(s == 0, high), 1, 1)
        relays(jnp.logical_and(s == 1, low), top, -1, early)
        relays(jnp.logical_and(s == 2, low), top, -1, late)

        @pl.when(s == start)
        def _():
            arrived(wcon.at[pl.ds(0, n_sp * rows)], end_f.at[1])
            pl.when(late_start)(functools.partial(convolve, 0))

        pl.when(s >= start)(functools.partial(convolve, s))
        pl.when(s == start)(functools.partial(out_end_of, 0))
        others_rows = jnp.logical_and(s >= start, s != sp)
        pl.when(others_rows)(functools.partial(give, s, 0))

        pl.when(s == 2 * start)(functools.partial(out_end_of, 1))
        held = jnp.logical_and(late_start, s == 1)
        pl.when(jnp.logical_and(others_rows, jnp.logical_not(held)))(functools.partial(give, s, 1))

        @pl.when(jnp.logical_and(s == 1, high))
        def _():
            join(0, 0)
            join(0, 1)

        pl.when(jnp.logical_and(s == 2, low))(functools.partial(join, 0, 0))
        return carry

    lax.fori_loop(0, n_sp, step, 0)
    @pl.when(sp == 0)
    def _():
        give(1, 1)
        give(0, 0, 1)

    pl.when(low)(functools.partial(give, 0, 0, 1))

    pl.when(low)(functools.partial(join, 0, 1))

    pl.when(sp > 0)(functools.partial(give, sp, 0, 1))

    @pl.when(low)
    def _():
        for h in range(2):
            join(1, h)
            join(2, h)

    @pl.when(high)
    def _():
        for h in range(2):
            join(1, h)
        for h in range(2):
            join(2, h)

    for d in range(n_sp):
        comes = (sp - d) * (sp - d) == 1

        @pl.when(comes)
        def _():
            arrived(z_recv.at[d], zr_sem.at[d])
            for c in range(chunks):
                mine[sp, c] = mine[sp, c] + z_recv[d, c].astype(F32)

    for c in range(chunks):
        out[:, c * chunk : (c + 1) * chunk] = mine[sp, c].astype(BF16)

    gone(rates.at[pl.ds(0, n_sp - 1)], RATE)
    gone(win.at[pl.ds(0, (n_sp - 1) * rows)], FIRST)
    gone(wcon.at[pl.ds(0, (n_sp - 1) * rows)], CON)
    gone(wout.at[pl.ds(0, n_sp - 1)], OUT)
    gone(win.at[pl.ds(0, 3 * n_sp * rows)], IN_RING)
    gone(wcon.at[pl.ds(0, 3 * n_sp * rows)], CON_RING)
    gone(wout.at[pl.ds(0, 3 * n_sp)], OUT_RING)
    gone(tokens.at[pl.ds(0, n_sp)], ACROSS)
    gone(sib_send, SIBLING)
    gone(z_send.at[pl.ds(0, n_sp - 1)], SUMS)

    @pl.when(sp < n_sp - 1)
    def _():
        gone(tokens.at[0], UP)

    @pl.when(sp > 0)
    def _():
        gone(tokens.at[0], DOWN)

    @pl.when(inner)
    def _():
        gone(tokens.at[pl.ds(0, n_sp - 1)], RELAY)


def sequence_shards(n_sp, n_fs, *arrays):
    (tok, wq, wf, wv, cg, cm, ci, headroom, rate, init, gain, taps, bias, ro, co) = arrays
    span, wide = tok.shape[1:]
    rec, con = wq.shape[1] // n_sp, cg.shape[1] // n_sp
    heads = rec // DK
    chunk = wide // OUT_PIECES
    hbm = pl.BlockSpec(memory_space=pl.ANY)
    vmem = pl.BlockSpec(memory_space=pltpu.VMEM)
    dma = pltpu.SemaphoreType.DMA
    flat = (n_sp, OUT_PIECES, span, chunk)
    mixed = pl.pallas_call(
        functools.partial(layer_kernel, n_sp, n_fs),
        out_shape=pltpu.VMEM((span, wide), BF16),
        in_specs=[hbm] * 11 + [vmem] * 4,
        out_specs=vmem,
        scratch_shapes=[
            pltpu.VMEM((2 * n_sp, span, wide), BF16),
            pltpu.VMEM((wide, 3 * rec), BF16),
            pltpu.VMEM((wide, 3 * con), BF16),
            pltpu.VMEM((n_sp * n_fs, rec + con, wide // (n_sp * n_fs)), BF16),
            pltpu.VMEM((n_sp,) + rate.shape[1:], F32),
            pltpu.VMEM((heads, DK, DK), F32),
            pltpu.VMEM((heads, DK, DK), F32),
            pltpu.VMEM((8 + 2 * span, con), F32),
            pltpu.VMEM((n_sp, 2 * span, rec + con), BF16),
            pltpu.VMEM(flat, BF16),
            pltpu.VMEM(flat, BF16),
            pltpu.VMEM(flat, F32),
            pltpu.VMEM(flat, BF16),
            pltpu.VMEM(flat, BF16),
            pltpu.VMEM((3,) + flat[1:], BF16),
            pltpu.VMEM((n_sp, wide // (n_sp * n_fs), 3 * rec), BF16),
            pltpu.VMEM((n_sp, wide // (n_sp * n_fs), 3 * con), BF16),
            pltpu.VMEM((n_sp, rec + con, wide // (n_sp * n_fs)), BF16),
            dma((n_sp,)),
            dma((5,)),
            dma((SENDS,)),
            dma((n_sp,)),
            dma((n_sp,)),
            dma((n_sp,)),
            dma((2, n_sp)),
            dma((2, n_sp)),
            dma((2, n_sp)),
            dma((n_sp,)),
            dma((3,)),
            dma((n_sp, TOKEN_PIECES)),
            dma((n_sp,)),
            dma((n_sp, OUT_PIECES)),
            dma((n_sp,)),
            dma((3, OUT_PIECES)),
        ],
        compiler_params=pltpu.CompilerParams(
            collective_id=0, has_side_effects=True, vmem_limit_bytes=60 * 2**20
        ),
    )(
        tok[0], wq, wf, wv, cg, cm, ci, ro, co, rate[0], init[0], headroom[None], gain[None],
        taps, bias[None],
    )
    return mixed[None]


def choose_plan(sizes, *arrays):
    n_sp, n_fs = sizes["sp"], sizes["fs"]
    rows, rec = arrays[1].shape
    con = arrays[4].shape[1]
    span = arrays[0].shape[1]
    even = (
        sizes["tp"] == 2
        and n_fs == 4
        and n_sp == 4
        and arrays[0].shape[2] % (n_fs * n_sp * 128) == 0
        and arrays[0].shape[0] == 1
        and rec % (n_sp * DK) == 0
        and rec // (n_sp * DK) <= 8
        and arrays[8].shape[1] % 8 == 0
        and con % (n_sp * 128) == 0
        and rows % 128 == 0
        and span == DK
        and arrays[13].shape[1] % 128 == 0
    )
    return sequence_shards(n_sp, n_fs, *arrays) if even else shards(*arrays)


def solution(mesh):
    in_specs = (
        P("fs", ("sp", "tp"), None),
        P(("sp", "fs"), "tp"),
        P(("sp", "fs"), "tp"),
        P(("sp", "fs"), "tp"),
        P(("sp", "fs"), "tp"),
        P(("sp", "fs"), "tp"),
        P(("sp", "fs"), "tp"),
        P("tp"),
        P("fs", "tp", "sp"),
        P("fs", "tp", None, None),
        P("tp"),
        P(None, "tp"),
        P("tp"),
        P("tp", ("sp", "fs")),
        P("tp", ("sp", "fs")),
    )
    out_specs = P("fs", ("sp", "tp"), None)
    body = functools.partial(choose_plan, dict(mesh.shape))
    return jax.shard_map(body, mesh=mesh, in_specs=in_specs, out_specs=out_specs, check_vma=False)
```

```python
import functools

import jax
import jax.numpy as jnp
from jax import lax
from jax.experimental import pallas as pl
from jax.experimental.pallas import tpu as pltpu
from jax.sharding import PartitionSpec as P

DK = 128
KW = 3
BLOCK_POSITIONS = 64


def carried_in(part, axis, combine, identity):
    place = lax.axis_index(axis)
    gathered = jax.tree.map(lambda a: lax.all_gather(a, axis), part)
    state = jax.tree.map(lambda a, e: jnp.zeros_like(a) + jnp.asarray(e, a.dtype), part, identity)

    def one(hop, state):
        return combine(
            state, jax.tree.map(lambda a: lax.dynamic_index_in_dim(a, hop, 0, False), gathered)
        )

    return lax.fori_loop(0, place, one, state)


def from_behind(block, axis, distance):
    devices = range(lax.axis_size(axis))
    route = [(i - distance, i) for i in devices if i - distance in devices]
    return lax.ppermute(block, axis, route)


def to_blocks(values, number_of_heads):
    number_of_blocks = values.shape[0] // BLOCK_POSITIONS
    return jnp.transpose(
        values.reshape(number_of_blocks, BLOCK_POSITIONS, number_of_heads, DK), (2, 0, 1, 3)
    )


def within_block_recurrence(
    query_vectors, forget_logits, value_vectors, gate_headroom, extra_rates
):
    number_of_heads = extra_rates.shape[0]
    number_of_blocks = query_vectors.shape[0] // BLOCK_POSITIONS
    query_scaled = to_blocks(query_vectors.astype(jnp.float32), number_of_heads) * DK ** (-0.5)
    gated_key = to_blocks(
        gate_headroom[None, :] * jax.nn.sigmoid(-forget_logits.astype(jnp.float32)), number_of_heads
    )
    forget_log_rate = (
        jnp.log1p(-gated_key)
        + extra_rates.reshape(number_of_heads, number_of_blocks, BLOCK_POSITIONS)[..., None]
    )
    values = to_blocks(value_vectors.astype(jnp.float32), number_of_heads)
    cumulative = jnp.cumsum(forget_log_rate, axis=2)
    query_decayed = query_scaled * jnp.exp(cumulative)
    key_decayed = gated_key * jnp.exp(-cumulative)
    scores = jnp.einsum(
        "hnik,hnjk->hnij", query_decayed, key_decayed, precision=lax.Precision.HIGHEST
    )
    causal = jnp.tril(jnp.ones((BLOCK_POSITIONS, BLOCK_POSITIONS), dtype=bool))
    scores = jnp.where(causal, scores, 0.0)
    within = jnp.einsum("hnij,hnjv->hniv", scores, values, precision=lax.Precision.HIGHEST)
    final_log = cumulative[:, :, -1, :]
    contrib = jnp.einsum(
        "hnck,hncv->hnkv",
        gated_key * jnp.exp(final_log[:, :, None, :] - cumulative),
        values,
        precision=lax.Precision.HIGHEST,
    )
    decays = jnp.exp(final_log)

    def advance(current, block_pair):
        return (block_pair[0][..., None] * current + block_pair[1], current)

    empty_state = jnp.zeros((number_of_heads, DK, DK), jnp.float32)
    local_total, entering = lax.scan(
        advance, empty_state, (jnp.moveaxis(decays, 1, 0), jnp.moveaxis(contrib, 1, 0))
    )
    entering = jnp.moveaxis(entering, 0, 1)
    before = jnp.exp(jnp.cumsum(final_log, axis=1) - final_log)
    device_decay = jnp.exp(jnp.sum(final_log, axis=1))
    return (query_decayed, within, entering, before, device_decay, local_total)


def finish(query_decayed, within, entering, before, carried, head_norm_gain):
    number_of_heads = query_decayed.shape[0]
    states = entering + before[..., None] * carried[:, None]
    carried_term = jnp.einsum(
        "hnck,hnkv->hncv", query_decayed, states, precision=lax.Precision.HIGHEST
    )
    length = query_decayed.shape[1] * BLOCK_POSITIONS
    recurrence_unnormed = jnp.transpose(within + carried_term, (1, 2, 0, 3)).reshape(
        length, number_of_heads, DK
    )
    mean_square = jnp.mean(recurrence_unnormed * recurrence_unnormed, axis=-1, keepdims=True)
    rec_out = (
        recurrence_unnormed
        * lax.rsqrt(mean_square + 1e-06)
        * head_norm_gain.reshape(number_of_heads, DK)
    )
    return rec_out.reshape(length, number_of_heads * DK).astype(jnp.bfloat16)


def chain_combine(earlier_part, later_part):
    return (
        earlier_part[0] * later_part[0],
        later_part[0][..., None] * earlier_part[1] + later_part[1],
    )


def shards(
    tokens,
    query_weight,
    forget_weight,
    value_weight,
    convolution_gate_weight,
    convolution_multiplier_weight,
    convolution_input_weight,
    gate_headroom,
    added_log_rate,
    initial_state,
    head_norm_gain,
    convolution_taps,
    convolution_bias,
    recurrence_output_weight,
    convolution_output_weight,
):
    own_rows = tokens[0]
    gathered = (
        lax.all_gather(query_weight, ("sp", "fs"), axis=0, tiled=True),
        lax.all_gather(forget_weight, ("sp", "fs"), axis=0, tiled=True),
        lax.all_gather(value_weight, ("sp", "fs"), axis=0, tiled=True),
        lax.all_gather(convolution_gate_weight, ("sp", "fs"), axis=0, tiled=True),
        lax.all_gather(convolution_multiplier_weight, ("sp", "fs"), axis=0, tiled=True),
        lax.all_gather(convolution_input_weight, ("sp", "fs"), axis=0, tiled=True),
        lax.all_gather(recurrence_output_weight, ("sp", "fs"), axis=1, tiled=True),
        lax.all_gather(convolution_output_weight, ("sp", "fs"), axis=1, tiled=True),
    )
    in_weights = gathered[:6]
    out_rec = gathered[6]
    out_conv = gathered[7]
    block_rows = lax.all_gather(own_rows, "tp", axis=0, tiled=True)
    projected = jnp.concatenate(
        [
            jnp.dot(block_rows, weight, preferred_element_type=jnp.float32).astype(jnp.bfloat16)
            for weight in in_weights
        ],
        axis=1,
    )
    rec_width = query_weight.shape[1]
    conv_width = convolution_gate_weight.shape[1]
    query_vectors = projected[:, :rec_width]
    forget_logits = projected[:, rec_width : 2 * rec_width]
    value_vectors = projected[:, 2 * rec_width : 3 * rec_width]
    conv_base = 3 * rec_width
    conv_gate = projected[:, conv_base : conv_base + conv_width]
    conv_mult = projected[:, conv_base + conv_width : conv_base + 2 * conv_width]
    conv_input = projected[:, conv_base + 2 * conv_width : conv_base + 3 * conv_width]
    query_decayed, within, entering, before, device_decay, local_total = within_block_recurrence(
        query_vectors, forget_logits, value_vectors, gate_headroom, added_log_rate[0]
    )
    conv_prod = conv_mult.astype(jnp.float32) * conv_input.astype(jnp.float32)
    length = conv_prod.shape[0]
    tail_rows = conv_prod[length - (KW - 1) :]
    unit_decay = jnp.ones_like(device_decay)
    empty_state = jnp.zeros_like(local_total)
    prior_decay, prior_state = carried_in(
        (device_decay, local_total), "sp", chain_combine, (unit_decay, empty_state)
    )
    prior_rows = from_behind(tail_rows, "sp", 1)
    carried = prior_decay[..., None] * initial_state[0] + prior_state
    rec_out = finish(query_decayed, within, entering, before, carried, head_norm_gain)
    extended = jnp.concatenate([prior_rows, conv_prod], axis=0)
    conv_y = jnp.broadcast_to(convolution_bias[None, :], conv_prod.shape)
    for j in range(KW):
        conv_y = conv_y + convolution_taps[j][None, :] * extended[j : j + length]
    conv_out = (conv_gate.astype(jnp.float32) * conv_y).astype(jnp.bfloat16)
    mixed = lax.psum_scatter(
        (
            jnp.dot(rec_out, out_rec, preferred_element_type=jnp.float32)
            + jnp.dot(conv_out, out_conv, preferred_element_type=jnp.float32)
        ).astype(jnp.bfloat16),
        "tp",
        scatter_dimension=0,
        tiled=True,
    )
    return mixed[None]


MESH = pl.DeviceIdType.MESH
F32 = jnp.float32
BF16 = jnp.bfloat16
CONTRACT_LAST = (((1,), (1,)), ((), ()))
CONTRACT_FIRST = (((0,), (0,)), ((), ()))
TOKEN_PIECES = 4
SENDS = 13
(
    UP, DOWN, ACROSS, RELAY, RATE, FIRST, CON, OUT, IN_RING, CON_RING, OUT_RING, SIBLING, SUMS,
) = range(SENDS)
OUT_PIECES = 8


def layer_kernel(
    n_sp, n_fs, tok, wq, wf, wv, cg, cm, ci, ro, co, rate, init, headroom, gain, taps, bias,
    out, tokens, win, wcon, wout, rates, first_state, state, ext, both, sib_send, sib_recv, mine,
    z_send, z_recv, rl_recv, stage_in, stage_con, stage_out, loc_in, loc_sem, out_sem, win_z,
    wcon_z, wout_z, in_f, con_f, out_f, out_end, end_f, tok_z, tok_t, sib_sem, zr_sem, rl_sem,
):
    sp, fs, tp = lax.axis_index("sp"), lax.axis_index("fs"), lax.axis_index("tp")
    other = 1 - tp
    rows = wq.shape[0]
    rec = wq.shape[1] // n_sp
    con = cg.shape[1] // n_sp
    span = tok.shape[0]
    heads = rec // DK
    wide = tok.shape[1]
    lanes_out = ro.shape[1]
    chunks, chunk = mine.shape[1], mine.shape[3]
    sub = span // TOKEN_PIECES
    shards_in = chunk // lanes_out

    def peer(**where):
        return {"sp": where.get("sp", sp), "fs": where.get("fs", fs), "tp": where.get("tp", tp)}

    half_ring = n_fs // 2

    def ring(p):
        return p + (p // half_ring) * (3 * half_ring - 1 - 2 * p)

    at_ring = ring(fs)
    left = ring(lax.rem(at_ring + n_fs - 1, n_fs))
    right = ring(lax.rem(at_ring + 1, n_fs))
    across = ring(lax.rem(at_ring + 2, n_fs))
    sibling = peer(tp=other)

    depth = rec + con
    rec_parts = [(ref, i * rec, rec) for i, ref in enumerate((wq, wf, wv))]
    con_parts = [(ref, i * con, con) for i, ref in enumerate((cg, cm, ci))]

    def in_rows(s, f, first, count):
        return win.at[pl.ds(pl.multiple_of((s * n_fs + f) * rows + first, count), count)]

    def con_rows(s, f):
        return wcon.at[pl.ds(pl.multiple_of((s * n_fs + f) * rows, rows), rows)]

    def out_slot(s, f):
        return wout.at[s * n_fs + f]

    def stage(z, in_to, con_to, out_to, place):
        copies = []
        for some, to, sem in ((rec_parts, in_to, loc_in.at[place]), (con_parts, con_to, loc_sem.at[0])):
            for ref, at, width in some:
                src = ref.at[:, pl.ds(pl.multiple_of(z * width, width), width)]
                copies.append((src, to.at[:, pl.ds(at, width)], sem))
        for ref, at, width in ((ro, 0, rec), (co, rec, con)):
            src = ref.at[pl.ds(pl.multiple_of(z * width, width), width)]
            copies.append((src, out_to.at[pl.ds(at, width)], loc_sem.at[1]))
        return [pltpu.make_async_copy(*copy) for copy in copies]

    below, above = sp, n_sp - 1 - sp
    fewer = jnp.minimum(below, above)
    upward = jnp.where(below < above, 1, -1)
    edge = fewer == 0

    def near(j):
        paired = j <= 2 * fewer
        side = jnp.where(paired, upward * (1 - 2 * (j % 2)), upward)
        return sp + side * jnp.where(paired, (j + 1) // 2, j - fewer)

    def to_send(j):
        if j == 1:
            return near(1)
        return jnp.where(edge, near(n_sp + 1 - j), near(j))

    local = []
    for j in range(1, n_sp):
        local += stage(to_send(j), stage_in.at[j], stage_con.at[j], stage_out.at[j], j)
    local += stage(sp, in_rows(sp, fs, 0, rows), con_rows(sp, fs), out_slot(sp, fs), 0)
    others = [
        (tok, tokens.at[sp * 2 + tp]), (rate, rates.at[sp]),
        (init.at[pl.ds(sp * heads, heads)], first_state),
    ]
    others = [pltpu.make_async_copy(*pair, loc_sem.at[2 + i]) for i, pair in enumerate(others)]
    for copy in local + others:
        copy.start()

    barrier = pltpu.get_barrier_semaphore()
    for j in range(1, n_sp):
        pl.semaphore_signal(barrier, inc=1, device_id=peer(sp=near(j)), device_id_type=MESH)
    for f in (left, right):
        pl.semaphore_signal(barrier, inc=1, device_id=peer(fs=f), device_id_type=MESH)
    pl.semaphore_signal(barrier, inc=1, device_id=sibling, device_id_type=MESH)
    pl.semaphore_wait(barrier, n_sp + 2)

    def remote(src, dst, send, recv, to):
        return pltpu.make_async_remote_copy(
            src_ref=src, dst_ref=dst, send_sem=send, recv_sem=recv, device_id=to, device_id_type=MESH,
        )

    def arrived(ref, recv):
        remote(ref, ref, recv, recv, sibling).wait_recv()

    def gone(ref, i):
        remote(ref, ref, out_sem.at[i], out_sem.at[i], sibling).wait_send()

    def tok_piece(ref, c):
        return ref.at[pl.ds(c * sub, sub)]

    def token_slot(s, t, c):
        return tok_piece(tokens.at[s * 2 + t], c)

    def own_tokens(send, to):
        return [
            remote(tok_piece(tok, c), token_slot(sp, tp, c), send, tok_z.at[sp, c], to)
            for c in range(TOKEN_PIECES)
        ]

    def own_up():
        return own_tokens(out_sem.at[UP], peer(sp=sp + 1))

    def own_down():
        return own_tokens(out_sem.at[DOWN], peer(sp=sp - 1))

    def to_sibling(s, c, src=None):
        slot = token_slot(s, tp, c)
        return remote(slot if src is None else src, slot, out_sem.at[ACROSS], tok_t.at[s], sibling)

    def relayed(s, c, to):
        slot = token_slot(s, tp, c)
        return remote(slot, slot, out_sem.at[RELAY], tok_z.at[s, c], to)

    def start_all(copies):
        for copy in copies:
            copy.start()

    def send_in(j):
        to = peer(sp=to_send(j))
        arrived(stage_in.at[j], loc_in.at[j])
        remote(rate, rates.at[sp], out_sem.at[RATE], end_f.at[2], to).start()
        remote(
            stage_in.at[j], in_rows(sp, fs, 0, rows), out_sem.at[FIRST], win_z.at[sp], to
        ).start()

    def con_copies():
        return [
            remote(
                stage_con.at[j], con_rows(sp, fs), out_sem.at[CON], wcon_z.at[sp],
                peer(sp=to_send(j)),
            )
            for j in range(1, n_sp)
        ]

    def out_copies():
        return [
            remote(
                stage_out.at[j], out_slot(sp, fs), out_sem.at[OUT], wout_z.at[sp],
                peer(sp=to_send(j)),
            )
            for j in range(1, n_sp)
        ]

    low, high = sp == 1, sp == n_sp - 2
    send_in(1)

    for j in range(2, n_sp):
        send_in(j)
    arrived(stage_con, loc_sem.at[0])
    arrived(stage_out, loc_sem.at[1])
    start_all(con_copies()[:1])
    for copy in others:
        copy.wait()

    @pl.when(sp == 0)
    def _():
        start_all(own_up())

    @pl.when(sp == n_sp - 1)
    def _():
        start_all(own_down())

    start_all(out_copies()[:1])
    for c in range(TOKEN_PIECES):
        to_sibling(sp, c, tok_piece(tok, c)).start()

    arrived(in_rows(sp, fs, 0, rows), loc_in.at[0])

    def z_in(j):
        z = near(j)
        arrived(in_rows(z, fs, 0, rows), win_z.at[z])

    def z_con(j):
        z = near(j)
        arrived(con_rows(z, fs), wcon_z.at[z])

    def z_out(j):
        z = near(j)
        arrived(out_slot(z, fs), wout_z.at[z])

    def place(j):
        return near(j) if j else sp

    def ring_of(k, whole, part, sem, landed, last):
        s = place(k)
        copies = (
            (whole(s, fs), landed.at[0, k], right), (whole(s, fs), landed.at[1, k], left),
            (part(s, left, 0), last, right), (part(s, right, 1), last, left),
        )
        return [remote(ref, ref, out_sem.at[sem], to_sem, peer(fs=to)) for ref, to_sem, to in copies]

    def pass_ring(k, whole, landed, copies):
        s = place(k)
        arrived(whole(s, left), landed.at[0, k])
        copies[2].start()
        arrived(whole(s, right), landed.at[1, k])
        copies[3].start()

    def in_whole(s, f):
        return in_rows(s, f, 0, rows)

    def in_ring(k):
        half = rows // 2
        return ring_of(
            k, in_whole, lambda s, f, h: in_rows(s, f, h * half, half), IN_RING, in_f, end_f.at[0]
        )

    def con_ring(k):
        half = rows // 2
        return ring_of(
            k, con_rows, lambda s, f, h: con_rows(s, f).at[pl.ds(h * half, half)], CON_RING, con_f,
            end_f.at[1],
        )

    def out_ring(k):
        half = depth // 2
        return ring_of(
            k, out_slot, lambda s, f, h: out_slot(s, f).at[pl.ds(h * half, half)], OUT_RING, out_f,
            out_end.at[k],
        )

    def ring_in(k):
        start_all(in_ring(k)[:2])

    def ring_in_on(k):
        pass_ring(k, in_whole, in_f, in_ring(k))

    def ring_con(k):
        start_all(con_ring(k)[:2])

    def ring_con_on(k):
        pass_ring(k, con_rows, con_f, con_ring(k))

    def ring_out(k):
        start_all(out_ring(k)[:2])

    def ring_out_on(k):
        pass_ring(k, out_slot, out_f, out_ring(k))

    def relay(s, c, step_by):
        arrived(token_slot(s, tp, c), tok_z.at[s, c])
        if step_by:
            relayed(s, c, peer(sp=sp + step_by)).start()
        to_sibling(s, c).start()

    def relays(when, s, step_by, pieces=range(TOKEN_PIECES)):
        @pl.when(when)
        def _():
            for c in pieces:
                relay(s, c, step_by)

    early, late = range(TOKEN_PIECES // 2), range(TOKEN_PIECES // 2, TOKEN_PIECES)
    bottom, top = 0, n_sp - 1

    def second_in():
        z_in(2)
        ring_in(2)

    def first_con():
        z_con(1)
        ring_con(1)

    inner = jnp.logical_not(edge)
    ring_in(0)
    z_in(1)
    ring_in(1)
    pl.when(inner)(second_in)
    ring_in_on(0)
    ring_con(0)

    @pl.when(low)
    def _():
        start_all(own_down())

    @pl.when(high)
    def _():
        start_all(own_up())

    ring_in_on(1)

    @pl.when(edge)
    def _():
        first_con()
        second_in()

    z_in(3)
    ring_in(3)
    start_all(con_copies()[1:])

    @pl.when(high)
    def _():
        start_all(own_down())
        start_all(out_copies()[1:])

    pl.when(inner)(first_con)
    ring_in_on(2)
    relays(low, bottom, 1, early)
    relays(high, top, -1, early)
    relays(low, bottom, 1, late)
    relays(high, top, -1, late)

    @pl.when(jnp.logical_not(high))
    def _():
        start_all(out_copies()[1:])

    @pl.when(low)
    def _():
        start_all(own_up())

    ring_in_on(3)
    ring_con_on(0)
    ring_con_on(1)
    relays(sp == 0, 1, 0)
    relays(sp == top, top - 1, 0)
    z_con(2)
    ring_con(2)
    z_con(3)
    ring_con(3)
    ring_out(0)
    z_out(1)
    ring_out(1)
    relays(low, top - 1, -1)
    relays(high, bottom, 1)
    ring_con_on(2)
    ring_con_on(3)

    late_start = sp < 2
    start = jnp.where(late_start, 1, 0)

    def near_out_on():
        ring_out_on(0)
        ring_out_on(1)
        for k in (2, 3):
            z_out(k)
            ring_out(k)

    pl.when(jnp.logical_not(late_start))(near_out_on)
    arrived(win.at[pl.ds(0, n_sp * rows)], end_f.at[0])
    arrived(rates.at[pl.ds(0, n_sp - 1)], end_f.at[2])

    for h in range(heads):
        state[h] = first_state[h].T
    ext[0:8] = jnp.zeros((8, con), F32)
    lane_rec = pl.ds(pl.multiple_of(sp * rec, rec), rec)
    lane_con = pl.ds(pl.multiple_of(sp * con, con), con)
    row_id = lax.broadcasted_iota(jnp.int32, (span, span), 0)
    col_id = lax.broadcasted_iota(jnp.int32, (span, span), 1)
    causal = row_id >= col_id
    lower = causal.astype(F32)
    upper = (row_id <= col_id).astype(F32)
    length = 2 * span

    def sib_copy(s, c):
        return remote(sib_send.at[s, c], sib_recv.at[s, c], out_sem.at[SIBLING], sib_sem.at[s, c], sibling)

    def final_copy(s, c, to):
        return remote(
            z_send.at[s, c], z_recv.at[sp, c], out_sem.at[SUMS], zr_sem.at[sp], peer(sp=to)
        )

    def joint_copy(s, c, to):
        landing, sem = rl_recv.at[2, c], rl_sem.at[2, c]
        return remote(z_send.at[s, c], landing, out_sem.at[SUMS], sem, peer(sp=to))

    def edge_copy(s, c, to):
        t = lax.rem(s, 2)
        landing, sem = rl_recv.at[t, c], rl_sem.at[t, c]
        return remote(z_send.at[s, c], landing, out_sem.at[SUMS], sem, peer(sp=to))

    def through_low(s):
        return jnp.logical_and(sp == 0, s >= 2)

    def through_high(s):
        return jnp.logical_and(sp == n_sp - 1, s <= n_sp - 3)

    def plain(s):
        return jnp.logical_or(
            jnp.logical_and(sp == 0, s == 1), jnp.logical_and(sp == top, s == top - 1)
        )

    per_slot = n_fs // shards_in

    def pieces_of(slots):
        return [slot * per_slot + i for slot in slots for i in range(per_slot)]

    def own_slots(h):
        return [place(2 * h), place(2 * h + 1)]

    def pass_on(s, h):
        for c in pieces_of(own_slots(h)):
            sib_copy(s, c).wait_recv()
            total = mine[s, c] + sib_recv[s, c].astype(F32)
            mine[s, c] = total

            @pl.when(jnp.logical_and(edge, s != sp))
            def _():
                z_send[s, c] = total.astype(BF16)

            @pl.when(plain(s))
            def _():
                final_copy(s, c, s).start()

            @pl.when(through_low(s))
            def _():
                edge_copy(s, c, 1).start()

            @pl.when(through_high(s))
            def _():
                edge_copy(s, c, n_sp - 2).start()

    def join(t, h):
        s = jnp.where(low, (2, 3, 0)[t], (0, 1, 3)[t])
        to = jnp.where(low, (2, 2, 0)[t], (1, 1, 3)[t])
        rising = low if t < 2 else high
        slots = [jnp.where(rising, 2 * h + i, n_sp - 1 - 2 * h - i) for i in range(2)]
        on = (high, low, None)[t]
        for c in pieces_of(slots):
            arrived(rl_recv.at[t, c], rl_sem.at[t, c])
            z_send[s, c] = (mine[s, c] + rl_recv[t, c].astype(F32)).astype(BF16)
            if on is None:
                final_copy(s, c, to).start()
            else:
                pl.when(on)(joint_copy(s, c, to).start)
                pl.when(jnp.logical_not(on))(final_copy(s, c, to).start)

    def project_out(s, h):
        for slot in own_slots(h):
            columns = jnp.concatenate([wout[slot * n_fs + i] for i in range(n_fs)], axis=1)
            partial = jnp.dot(both[s], columns, preferred_element_type=F32)
            first = partial[:span]
            second = partial[span:]
            own = jnp.where(tp == 0, first, second)
            given = jnp.where(tp == 0, second, first).astype(BF16)
            for i in range(per_slot):
                c = slot * per_slot + i
                mine[s, c] = own[:, i * chunk : (i + 1) * chunk]
                sib_send[s, c] = given[:, i * chunk : (i + 1) * chunk]
                sib_copy(s, c).start()

    def convolve(s):
        block = jnp.concatenate([tokens[2 * s], tokens[2 * s + 1]], axis=0)
        projected = jnp.dot(block, wcon[...], preferred_element_type=F32).astype(BF16).astype(F32)
        prod = projected[:, con : 2 * con] * projected[:, 2 * con :]
        ext[8:] = prod
        conv = jnp.broadcast_to(bias[:, lane_con], prod.shape)
        for j in range(KW):
            conv = conv + taps[j : j + 1, lane_con] * ext[pl.ds(8 - (KW - 1) + j, length)]
        ext[0:8] = ext[length:]
        both[s, :, rec:] = (projected[:, :con] * conv).astype(BF16)

    def recur(s):
        relayed_before = jnp.logical_or(
            (s - sp) * (s - sp) <= 1, jnp.logical_and(sp == 0, s == 2)
        )
        relays(jnp.logical_and(edge, jnp.logical_not(relayed_before)), s, 0)
        arrived(tokens.at[2 * s + other], tok_t.at[s])
        block = jnp.concatenate([tokens[2 * s], tokens[2 * s + 1]], axis=0)

        def project(at, width):
            return jnp.dot(
                block, win[:, pl.ds(at, width)], preferred_element_type=F32
            ).astype(BF16)

        query = project(0, rec).astype(F32) * DK ** (-0.5)
        forget = project(rec, rec).astype(F32)
        value = project(2 * rec, rec)
        key_gate = headroom[:, lane_rec] * jax.nn.sigmoid(-forget)
        log_forget = jnp.log1p(-key_gate)
        gains = gain[:, lane_rec]
        mine_rate = [rates[s, pl.ds(sp * heads + h, 1), :] for h in range(heads)]
        if heads < 8:
            mine_rate.append(jnp.zeros((8 - heads, 2 * span), F32))
        mine_rate = jnp.concatenate(mine_rate, axis=0)
        halves = []
        for c in range(2):
            part = slice(c * span, (c + 1) * span)
            cum = jnp.dot(lower, log_forget[part], precision=lax.Precision.HIGHEST)
            extra = jnp.dot(mine_rate[:, part], upper, precision=lax.Precision.HIGHEST)
            extra_t = extra.T
            grow = jnp.exp(cum)
            query_grow = query[part] * grow
            key_grow = (key_gate[part] / grow).astype(BF16)
            last = cum[span - 1 :, :]
            key_last = key_gate[part] * jnp.exp(last - cum)
            last_decay = jnp.exp(last)
            pieces = []
            for h in range(heads):
                lanes = slice(h * DK, (h + 1) * DK)
                row = extra[h : h + 1]
                column = extra_t[:, h : h + 1]
                end = row[:, span - 1 :]
                scores = lax.dot_general(
                    query_grow[:, lanes].astype(BF16), key_grow[:, lanes], CONTRACT_LAST,
                    preferred_element_type=F32,
                )
                decay = jnp.exp(jnp.where(causal, column - row, 0.0))
                scores = jnp.where(causal, scores * decay, 0.0).astype(BF16)
                values = value[part, lanes]
                before = state[h]
                raw = jnp.dot(scores, values, preferred_element_type=F32)
                raw = raw + lax.dot_general(
                    (query_grow[:, lanes] * jnp.exp(column)).astype(BF16), before.astype(BF16),
                    CONTRACT_LAST, preferred_element_type=F32,
                )
                keys = (key_last[:, lanes] * jnp.exp(end - column)).astype(BF16)
                state[h] = before * (last_decay[:, lanes] * jnp.exp(end)) + lax.dot_general(
                    values, keys, CONTRACT_FIRST, preferred_element_type=F32
                )
                square = jnp.mean(raw * raw, axis=-1, keepdims=True)
                pieces.append((raw * lax.rsqrt(square + 1e-06) * gains[:, lanes]).astype(BF16))
            halves.append(jnp.concatenate(pieces, axis=1))
        both[s, :, :rec] = jnp.concatenate(halves, axis=0)

    def out_end_of(h):
        for k in (2 * h, 2 * h + 1):
            arrived(out_slot(place(k), across), out_end.at[k])

    def give(s, *halves):
        for h in halves:
            project_out(s, h)
        for h in halves:
            pass_on(s, h)

    def step(s, carry):
        recur(s)
        relays(jnp.logical_and(s == 1, sp == 0), 2, 0)
        pl.when(jnp.logical_and(s == 0, late_start))(near_out_on)

        @pl.when(s == 2 * start)
        def _():
            ring_out_on(2)
            ring_out_on(3)

        relays(jnp.logical_and(s == 0, high), 1, 1)
        relays(jnp.logical_and(s == 1, low), top, -1, early)
        relays(jnp.logical_and(s == 2, low), top, -1, late)

        @pl.when(s == start)
        def _():
            arrived(wcon.at[pl.ds(0, n_sp * rows)], end_f.at[1])
            pl.when(late_start)(functools.partial(convolve, 0))

        pl.when(s >= start)(functools.partial(convolve, s))
        pl.when(jnp.logical_and(s == 3, low))(functools.partial(join, 0, 1))
        pl.when(s == start)(functools.partial(out_end_of, 0))
        others_rows = jnp.logical_and(s >= start, s != sp)
        pl.when(others_rows)(functools.partial(give, s, 0))

        pl.when(s == 2 * start)(functools.partial(out_end_of, 1))
        held = jnp.logical_and(late_start, s == 1)
        pl.when(jnp.logical_and(others_rows, jnp.logical_not(held)))(functools.partial(give, s, 1))

        @pl.when(jnp.logical_and(s == 1, high))
        def _():
            join(0, 0)
            join(0, 1)

        pl.when(jnp.logical_and(s == 2, low))(functools.partial(join, 0, 0))
        return carry

    lax.fori_loop(0, n_sp, step, 0)
    @pl.when(sp == 0)
    def _():
        give(1, 1)
        give(0, 0, 1)

    pl.when(low)(functools.partial(give, 0, 0, 1))


    pl.when(sp > 0)(functools.partial(give, sp, 0, 1))

    @pl.when(low)
    def _():
        for h in range(2):
            join(1, h)
            join(2, h)

    @pl.when(high)
    def _():
        for h in range(2):
            join(1, h)
        for h in range(2):
            join(2, h)

    for d in range(n_sp):
        comes = (sp - d) * (sp - d) == 1

        @pl.when(comes)
        def _():
            arrived(z_recv.at[d], zr_sem.at[d])
            for c in range(chunks):
                mine[sp, c] = mine[sp, c] + z_recv[d, c].astype(F32)

    for c in range(chunks):
        out[:, c * chunk : (c + 1) * chunk] = mine[sp, c].astype(BF16)

    gone(rates.at[pl.ds(0, n_sp - 1)], RATE)
    gone(win.at[pl.ds(0, (n_sp - 1) * rows)], FIRST)
    gone(wcon.at[pl.ds(0, (n_sp - 1) * rows)], CON)
    gone(wout.at[pl.ds(0, n_sp - 1)], OUT)
    gone(win.at[pl.ds(0, 3 * n_sp * rows)], IN_RING)
    gone(wcon.at[pl.ds(0, 3 * n_sp * rows)], CON_RING)
    gone(wout.at[pl.ds(0, 3 * n_sp)], OUT_RING)
    gone(tokens.at[pl.ds(0, n_sp)], ACROSS)
    gone(sib_send, SIBLING)
    gone(z_send.at[pl.ds(0, n_sp - 1)], SUMS)

    @pl.when(sp < n_sp - 1)
    def _():
        gone(tokens.at[0], UP)

    @pl.when(sp > 0)
    def _():
        gone(tokens.at[0], DOWN)

    @pl.when(inner)
    def _():
        gone(tokens.at[pl.ds(0, n_sp - 1)], RELAY)


def sequence_shards(n_sp, n_fs, *arrays):
    (tok, wq, wf, wv, cg, cm, ci, headroom, rate, init, gain, taps, bias, ro, co) = arrays
    span, wide = tok.shape[1:]
    rec, con = wq.shape[1] // n_sp, cg.shape[1] // n_sp
    heads = rec // DK
    chunk = wide // OUT_PIECES
    hbm = pl.BlockSpec(memory_space=pl.ANY)
    vmem = pl.BlockSpec(memory_space=pltpu.VMEM)
    dma = pltpu.SemaphoreType.DMA
    flat = (n_sp, OUT_PIECES, span, chunk)
    mixed = pl.pallas_call(
        functools.partial(layer_kernel, n_sp, n_fs),
        out_shape=pltpu.VMEM((span, wide), BF16),
        in_specs=[hbm] * 11 + [vmem] * 4,
        out_specs=vmem,
        scratch_shapes=[
            pltpu.VMEM((2 * n_sp, span, wide), BF16),
            pltpu.VMEM((wide, 3 * rec), BF16),
            pltpu.VMEM((wide, 3 * con), BF16),
            pltpu.VMEM((n_sp * n_fs, rec + con, wide // (n_sp * n_fs)), BF16),
            pltpu.VMEM((n_sp,) + rate.shape[1:], F32),
            pltpu.VMEM((heads, DK, DK), F32),
            pltpu.VMEM((heads, DK, DK), F32),
            pltpu.VMEM((8 + 2 * span, con), F32),
            pltpu.VMEM((n_sp, 2 * span, rec + con), BF16),
            pltpu.VMEM(flat, BF16),
            pltpu.VMEM(flat, BF16),
            pltpu.VMEM(flat, F32),
            pltpu.VMEM(flat, BF16),
            pltpu.VMEM(flat, BF16),
            pltpu.VMEM((3,) + flat[1:], BF16),
            pltpu.VMEM((n_sp, wide // (n_sp * n_fs), 3 * rec), BF16),
            pltpu.VMEM((n_sp, wide // (n_sp * n_fs), 3 * con), BF16),
            pltpu.VMEM((n_sp, rec + con, wide // (n_sp * n_fs)), BF16),
            dma((n_sp,)),
            dma((5,)),
            dma((SENDS,)),
            dma((n_sp,)),
            dma((n_sp,)),
            dma((n_sp,)),
            dma((2, n_sp)),
            dma((2, n_sp)),
            dma((2, n_sp)),
            dma((n_sp,)),
            dma((3,)),
            dma((n_sp, TOKEN_PIECES)),
            dma((n_sp,)),
            dma((n_sp, OUT_PIECES)),
            dma((n_sp,)),
            dma((3, OUT_PIECES)),
        ],
        compiler_params=pltpu.CompilerParams(
            collective_id=0, has_side_effects=True, vmem_limit_bytes=60 * 2**20
        ),
    )(
        tok[0], wq, wf, wv, cg, cm, ci, ro, co, rate[0], init[0], headroom[None], gain[None],
        taps, bias[None],
    )
    return mixed[None]


def choose_plan(sizes, *arrays):
    n_sp, n_fs = sizes["sp"], sizes["fs"]
    rows, rec = arrays[1].shape
    con = arrays[4].shape[1]
    span = arrays[0].shape[1]
    even = (
        sizes["tp"] == 2
        and n_fs == 4
        and n_sp == 4
        and arrays[0].shape[2] % (n_fs * n_sp * 128) == 0
        and arrays[0].shape[0] == 1
        and rec % (n_sp * DK) == 0
        and rec // (n_sp * DK) <= 8
        and arrays[8].shape[1] % 8 == 0
        and con % (n_sp * 128) == 0
        and rows % 128 == 0
        and span == DK
        and arrays[13].shape[1] % 128 == 0
    )
    return sequence_shards(n_sp, n_fs, *arrays) if even else shards(*arrays)


def solution(mesh):
    in_specs = (
        P("fs", ("sp", "tp"), None),
        P(("sp", "fs"), "tp"),
        P(("sp", "fs"), "tp"),
        P(("sp", "fs"), "tp"),
        P(("sp", "fs"), "tp"),
        P(("sp", "fs"), "tp"),
        P(("sp", "fs"), "tp"),
        P("tp"),
        P("fs", "tp", "sp"),
        P("fs", "tp", None, None),
        P("tp"),
        P(None, "tp"),
        P("tp"),
        P("tp", ("sp", "fs")),
        P("tp", ("sp", "fs")),
    )
    out_specs = P("fs", ("sp", "tp"), None)
    body = functools.partial(choose_plan, dict(mesh.shape))
    return jax.shard_map(body, mesh=mesh, in_specs=in_specs, out_specs=out_specs, check_vma=False)
```

```python
import functools

import jax
import jax.numpy as jnp
from jax import lax
from jax.experimental import pallas as pl
from jax.experimental.pallas import tpu as pltpu
from jax.sharding import PartitionSpec as P

DK = 128
KW = 3
BLOCK_POSITIONS = 64


def carried_in(part, axis, combine, identity):
    place = lax.axis_index(axis)
    gathered = jax.tree.map(lambda a: lax.all_gather(a, axis), part)
    state = jax.tree.map(lambda a, e: jnp.zeros_like(a) + jnp.asarray(e, a.dtype), part, identity)

    def one(hop, state):
        return combine(
            state, jax.tree.map(lambda a: lax.dynamic_index_in_dim(a, hop, 0, False), gathered)
        )

    return lax.fori_loop(0, place, one, state)


def from_behind(block, axis, distance):
    devices = range(lax.axis_size(axis))
    route = [(i - distance, i) for i in devices if i - distance in devices]
    return lax.ppermute(block, axis, route)


def to_blocks(values, number_of_heads):
    number_of_blocks = values.shape[0] // BLOCK_POSITIONS
    return jnp.transpose(
        values.reshape(number_of_blocks, BLOCK_POSITIONS, number_of_heads, DK), (2, 0, 1, 3)
    )


def within_block_recurrence(
    query_vectors, forget_logits, value_vectors, gate_headroom, extra_rates
):
    number_of_heads = extra_rates.shape[0]
    number_of_blocks = query_vectors.shape[0] // BLOCK_POSITIONS
    query_scaled = to_blocks(query_vectors.astype(jnp.float32), number_of_heads) * DK ** (-0.5)
    gated_key = to_blocks(
        gate_headroom[None, :] * jax.nn.sigmoid(-forget_logits.astype(jnp.float32)), number_of_heads
    )
    forget_log_rate = (
        jnp.log1p(-gated_key)
        + extra_rates.reshape(number_of_heads, number_of_blocks, BLOCK_POSITIONS)[..., None]
    )
    values = to_blocks(value_vectors.astype(jnp.float32), number_of_heads)
    cumulative = jnp.cumsum(forget_log_rate, axis=2)
    query_decayed = query_scaled * jnp.exp(cumulative)
    key_decayed = gated_key * jnp.exp(-cumulative)
    scores = jnp.einsum(
        "hnik,hnjk->hnij", query_decayed, key_decayed, precision=lax.Precision.HIGHEST
    )
    causal = jnp.tril(jnp.ones((BLOCK_POSITIONS, BLOCK_POSITIONS), dtype=bool))
    scores = jnp.where(causal, scores, 0.0)
    within = jnp.einsum("hnij,hnjv->hniv", scores, values, precision=lax.Precision.HIGHEST)
    final_log = cumulative[:, :, -1, :]
    contrib = jnp.einsum(
        "hnck,hncv->hnkv",
        gated_key * jnp.exp(final_log[:, :, None, :] - cumulative),
        values,
        precision=lax.Precision.HIGHEST,
    )
    decays = jnp.exp(final_log)

    def advance(current, block_pair):
        return (block_pair[0][..., None] * current + block_pair[1], current)

    empty_state = jnp.zeros((number_of_heads, DK, DK), jnp.float32)
    local_total, entering = lax.scan(
        advance, empty_state, (jnp.moveaxis(decays, 1, 0), jnp.moveaxis(contrib, 1, 0))
    )
    entering = jnp.moveaxis(entering, 0, 1)
    before = jnp.exp(jnp.cumsum(final_log, axis=1) - final_log)
    device_decay = jnp.exp(jnp.sum(final_log, axis=1))
    return (query_decayed, within, entering, before, device_decay, local_total)


def finish(query_decayed, within, entering, before, carried, head_norm_gain):
    number_of_heads = query_decayed.shape[0]
    states = entering + before[..., None] * carried[:, None]
    carried_term = jnp.einsum(
        "hnck,hnkv->hncv", query_decayed, states, precision=lax.Precision.HIGHEST
    )
    length = query_decayed.shape[1] * BLOCK_POSITIONS
    recurrence_unnormed = jnp.transpose(within + carried_term, (1, 2, 0, 3)).reshape(
        length, number_of_heads, DK
    )
    mean_square = jnp.mean(recurrence_unnormed * recurrence_unnormed, axis=-1, keepdims=True)
    rec_out = (
        recurrence_unnormed
        * lax.rsqrt(mean_square + 1e-06)
        * head_norm_gain.reshape(number_of_heads, DK)
    )
    return rec_out.reshape(length, number_of_heads * DK).astype(jnp.bfloat16)


def chain_combine(earlier_part, later_part):
    return (
        earlier_part[0] * later_part[0],
        later_part[0][..., None] * earlier_part[1] + later_part[1],
    )


def shards(
    tokens,
    query_weight,
    forget_weight,
    value_weight,
    convolution_gate_weight,
    convolution_multiplier_weight,
    convolution_input_weight,
    gate_headroom,
    added_log_rate,
    initial_state,
    head_norm_gain,
    convolution_taps,
    convolution_bias,
    recurrence_output_weight,
    convolution_output_weight,
):
    own_rows = tokens[0]
    gathered = (
        lax.all_gather(query_weight, ("sp", "fs"), axis=0, tiled=True),
        lax.all_gather(forget_weight, ("sp", "fs"), axis=0, tiled=True),
        lax.all_gather(value_weight, ("sp", "fs"), axis=0, tiled=True),
        lax.all_gather(convolution_gate_weight, ("sp", "fs"), axis=0, tiled=True),
        lax.all_gather(convolution_multiplier_weight, ("sp", "fs"), axis=0, tiled=True),
        lax.all_gather(convolution_input_weight, ("sp", "fs"), axis=0, tiled=True),
        lax.all_gather(recurrence_output_weight, ("sp", "fs"), axis=1, tiled=True),
        lax.all_gather(convolution_output_weight, ("sp", "fs"), axis=1, tiled=True),
    )
    in_weights = gathered[:6]
    out_rec = gathered[6]
    out_conv = gathered[7]
    block_rows = lax.all_gather(own_rows, "tp", axis=0, tiled=True)
    projected = jnp.concatenate(
        [
            jnp.dot(block_rows, weight, preferred_element_type=jnp.float32).astype(jnp.bfloat16)
            for weight in in_weights
        ],
        axis=1,
    )
    rec_width = query_weight.shape[1]
    conv_width = convolution_gate_weight.shape[1]
    query_vectors = projected[:, :rec_width]
    forget_logits = projected[:, rec_width : 2 * rec_width]
    value_vectors = projected[:, 2 * rec_width : 3 * rec_width]
    conv_base = 3 * rec_width
    conv_gate = projected[:, conv_base : conv_base + conv_width]
    conv_mult = projected[:, conv_base + conv_width : conv_base + 2 * conv_width]
    conv_input = projected[:, conv_base + 2 * conv_width : conv_base + 3 * conv_width]
    query_decayed, within, entering, before, device_decay, local_total = within_block_recurrence(
        query_vectors, forget_logits, value_vectors, gate_headroom, added_log_rate[0]
    )
    conv_prod = conv_mult.astype(jnp.float32) * conv_input.astype(jnp.float32)
    length = conv_prod.shape[0]
    tail_rows = conv_prod[length - (KW - 1) :]
    unit_decay = jnp.ones_like(device_decay)
    empty_state = jnp.zeros_like(local_total)
    prior_decay, prior_state = carried_in(
        (device_decay, local_total), "sp", chain_combine, (unit_decay, empty_state)
    )
    prior_rows = from_behind(tail_rows, "sp", 1)
    carried = prior_decay[..., None] * initial_state[0] + prior_state
    rec_out = finish(query_decayed, within, entering, before, carried, head_norm_gain)
    extended = jnp.concatenate([prior_rows, conv_prod], axis=0)
    conv_y = jnp.broadcast_to(convolution_bias[None, :], conv_prod.shape)
    for j in range(KW):
        conv_y = conv_y + convolution_taps[j][None, :] * extended[j : j + length]
    conv_out = (conv_gate.astype(jnp.float32) * conv_y).astype(jnp.bfloat16)
    mixed = lax.psum_scatter(
        (
            jnp.dot(rec_out, out_rec, preferred_element_type=jnp.float32)
            + jnp.dot(conv_out, out_conv, preferred_element_type=jnp.float32)
        ).astype(jnp.bfloat16),
        "tp",
        scatter_dimension=0,
        tiled=True,
    )
    return mixed[None]


MESH = pl.DeviceIdType.MESH
F32 = jnp.float32
BF16 = jnp.bfloat16
CONTRACT_LAST = (((1,), (1,)), ((), ()))
CONTRACT_FIRST = (((0,), (0,)), ((), ()))
TOKEN_PIECES = 4
SENDS = 13
(
    UP, DOWN, ACROSS, RELAY, RATE, FIRST, CON, OUT, IN_RING, CON_RING, OUT_RING, SIBLING, SUMS,
) = range(SENDS)
OUT_PIECES = 8


def layer_kernel(
    n_sp, n_fs, tok, wq, wf, wv, cg, cm, ci, ro, co, rate, init, headroom_in, gain_in,
    taps_in, bias_in, out, headroom, gain, taps, bias, tokens, win, wcon, wout, rates, first_state, state, ext, both, sib_send, sib_recv, mine,
    z_send, z_recv, rl_recv, stage_in, stage_con, stage_out, loc_in, loc_sem, out_sem, win_z,
    wcon_z, wout_z, in_f, con_f, out_f, out_end, end_f, tok_z, tok_t, sib_sem, zr_sem, rl_sem,
):
    sp, fs, tp = lax.axis_index("sp"), lax.axis_index("fs"), lax.axis_index("tp")
    other = 1 - tp
    rows = wq.shape[0]
    rec = wq.shape[1] // n_sp
    con = cg.shape[1] // n_sp
    span = tok.shape[0]
    heads = rec // DK
    wide = tok.shape[1]
    lanes_out = ro.shape[1]
    chunks, chunk = mine.shape[1], mine.shape[3]
    sub = span // TOKEN_PIECES
    shards_in = chunk // lanes_out

    def peer(**where):
        return {"sp": where.get("sp", sp), "fs": where.get("fs", fs), "tp": where.get("tp", tp)}

    half_ring = n_fs // 2

    def ring(p):
        return p + (p // half_ring) * (3 * half_ring - 1 - 2 * p)

    at_ring = ring(fs)
    left = ring(lax.rem(at_ring + n_fs - 1, n_fs))
    right = ring(lax.rem(at_ring + 1, n_fs))
    across = ring(lax.rem(at_ring + 2, n_fs))
    sibling = peer(tp=other)

    depth = rec + con
    rec_parts = [(ref, i * rec, rec) for i, ref in enumerate((wq, wf, wv))]
    con_parts = [(ref, i * con, con) for i, ref in enumerate((cg, cm, ci))]

    def in_rows(s, f, first, count):
        return win.at[pl.ds(pl.multiple_of((s * n_fs + f) * rows + first, count), count)]

    def con_rows(s, f):
        return wcon.at[pl.ds(pl.multiple_of((s * n_fs + f) * rows, rows), rows)]

    def out_slot(s, f):
        return wout.at[s * n_fs + f]

    def stage(z, in_to, con_to, out_to, place):
        copies = []
        for some, to, sem in ((rec_parts, in_to, loc_in.at[place]), (con_parts, con_to, loc_sem.at[0])):
            for ref, at, width in some:
                src = ref.at[:, pl.ds(pl.multiple_of(z * width, width), width)]
                copies.append((src, to.at[:, pl.ds(at, width)], sem))
        for ref, at, width in ((ro, 0, rec), (co, rec, con)):
            src = ref.at[pl.ds(pl.multiple_of(z * width, width), width)]
            copies.append((src, out_to.at[pl.ds(at, width)], loc_sem.at[1]))
        return [pltpu.make_async_copy(*copy) for copy in copies]

    below, above = sp, n_sp - 1 - sp
    fewer = jnp.minimum(below, above)
    upward = jnp.where(below < above, 1, -1)
    edge = fewer == 0

    def near(j):
        paired = j <= 2 * fewer
        side = jnp.where(paired, upward * (1 - 2 * (j % 2)), upward)
        return sp + side * jnp.where(paired, (j + 1) // 2, j - fewer)

    def to_send(j):
        if j == 1:
            return near(1)
        return jnp.where(edge, near(n_sp + 1 - j), near(j))

    local = []
    for j in range(1, n_sp):
        local += stage(to_send(j), stage_in.at[j], stage_con.at[j], stage_out.at[j], j)
    local += stage(sp, in_rows(sp, fs, 0, rows), con_rows(sp, fs), out_slot(sp, fs), 0)
    others = [
        (tok, tokens.at[sp * 2 + tp]), (rate, rates.at[sp]),
        (init.at[pl.ds(sp * heads, heads)], first_state), (headroom_in, headroom), (gain_in, gain),
        (taps_in, taps), (bias_in, bias),
    ]
    others = [pltpu.make_async_copy(*pair, loc_sem.at[2 + i]) for i, pair in enumerate(others)]
    for copy in local + others:
        copy.start()

    barrier = pltpu.get_barrier_semaphore()
    for j in range(1, n_sp):
        pl.semaphore_signal(barrier, inc=1, device_id=peer(sp=near(j)), device_id_type=MESH)
    for f in (left, right):
        pl.semaphore_signal(barrier, inc=1, device_id=peer(fs=f), device_id_type=MESH)
    pl.semaphore_signal(barrier, inc=1, device_id=sibling, device_id_type=MESH)
    pl.semaphore_wait(barrier, n_sp + 2)

    def remote(src, dst, send, recv, to):
        return pltpu.make_async_remote_copy(
            src_ref=src, dst_ref=dst, send_sem=send, recv_sem=recv, device_id=to, device_id_type=MESH,
        )

    def arrived(ref, recv):
        remote(ref, ref, recv, recv, sibling).wait_recv()

    def gone(ref, i):
        remote(ref, ref, out_sem.at[i], out_sem.at[i], sibling).wait_send()

    def tok_piece(ref, c):
        return ref.at[pl.ds(c * sub, sub)]

    def token_slot(s, t, c):
        return tok_piece(tokens.at[s * 2 + t], c)

    def own_tokens(send, to):
        return [
            remote(tok_piece(tok, c), token_slot(sp, tp, c), send, tok_z.at[sp, c], to)
            for c in range(TOKEN_PIECES)
        ]

    def own_up():
        return own_tokens(out_sem.at[UP], peer(sp=sp + 1))

    def own_down():
        return own_tokens(out_sem.at[DOWN], peer(sp=sp - 1))

    def to_sibling(s, c, src=None):
        slot = token_slot(s, tp, c)
        return remote(slot if src is None else src, slot, out_sem.at[ACROSS], tok_t.at[s], sibling)

    def relayed(s, c, to):
        slot = token_slot(s, tp, c)
        return remote(slot, slot, out_sem.at[RELAY], tok_z.at[s, c], to)

    def start_all(copies):
        for copy in copies:
            copy.start()

    def send_in(j):
        to = peer(sp=to_send(j))
        arrived(stage_in.at[j], loc_in.at[j])
        remote(rate, rates.at[sp], out_sem.at[RATE], end_f.at[2], to).start()
        remote(
            stage_in.at[j], in_rows(sp, fs, 0, rows), out_sem.at[FIRST], win_z.at[sp], to
        ).start()

    def con_copies():
        return [
            remote(
                stage_con.at[j], con_rows(sp, fs), out_sem.at[CON], wcon_z.at[sp],
                peer(sp=to_send(j)),
            )
            for j in range(1, n_sp)
        ]

    def out_copies():
        return [
            remote(
                stage_out.at[j], out_slot(sp, fs), out_sem.at[OUT], wout_z.at[sp],
                peer(sp=to_send(j)),
            )
            for j in range(1, n_sp)
        ]

    low, high = sp == 1, sp == n_sp - 2
    send_in(1)

    for j in range(2, n_sp):
        send_in(j)
    arrived(stage_con, loc_sem.at[0])
    arrived(stage_out, loc_sem.at[1])
    start_all(con_copies()[:1])
    for copy in others:
        copy.wait()

    @pl.when(sp == 0)
    def _():
        start_all(own_up())

    @pl.when(sp == n_sp - 1)
    def _():
        start_all(own_down())

    start_all(out_copies()[:1])
    for c in range(TOKEN_PIECES):
        to_sibling(sp, c, tok_piece(tok, c)).start()

    arrived(in_rows(sp, fs, 0, rows), loc_in.at[0])

    def z_in(j):
        z = near(j)
        arrived(in_rows(z, fs, 0, rows), win_z.at[z])

    def z_con(j):
        z = near(j)
        arrived(con_rows(z, fs), wcon_z.at[z])

    def z_out(j):
        z = near(j)
        arrived(out_slot(z, fs), wout_z.at[z])

    def place(j):
        return near(j) if j else sp

    def ring_of(k, whole, part, sem, landed, last):
        s = place(k)
        copies = (
            (whole(s, fs), landed.at[0, k], right), (whole(s, fs), landed.at[1, k], left),
            (part(s, left, 0), last, right), (part(s, right, 1), last, left),
        )
        return [remote(ref, ref, out_sem.at[sem], to_sem, peer(fs=to)) for ref, to_sem, to in copies]

    def pass_ring(k, whole, landed, copies):
        s = place(k)
        arrived(whole(s, left), landed.at[0, k])
        copies[2].start()
        arrived(whole(s, right), landed.at[1, k])
        copies[3].start()

    def in_whole(s, f):
        return in_rows(s, f, 0, rows)

    def in_ring(k):
        half = rows // 2
        return ring_of(
            k, in_whole, lambda s, f, h: in_rows(s, f, h * half, half), IN_RING, in_f, end_f.at[0]
        )

    def con_ring(k):
        half = rows // 2
        return ring_of(
            k, con_rows, lambda s, f, h: con_rows(s, f).at[pl.ds(h * half, half)], CON_RING, con_f,
            end_f.at[1],
        )

    def out_ring(k):
        half = depth // 2
        return ring_of(
            k, out_slot, lambda s, f, h: out_slot(s, f).at[pl.ds(h * half, half)], OUT_RING, out_f,
            out_end.at[k],
        )

    def ring_in(k):
        start_all(in_ring(k)[:2])

    def ring_in_on(k):
        pass_ring(k, in_whole, in_f, in_ring(k))

    def ring_con(k):
        start_all(con_ring(k)[:2])

    def ring_con_on(k):
        pass_ring(k, con_rows, con_f, con_ring(k))

    def ring_out(k):
        start_all(out_ring(k)[:2])

    def ring_out_on(k):
        pass_ring(k, out_slot, out_f, out_ring(k))

    def relay(s, c, step_by):
        arrived(token_slot(s, tp, c), tok_z.at[s, c])
        if step_by:
            relayed(s, c, peer(sp=sp + step_by)).start()
        to_sibling(s, c).start()

    def relays(when, s, step_by, pieces=range(TOKEN_PIECES)):
        @pl.when(when)
        def _():
            for c in pieces:
                relay(s, c, step_by)

    early, late = range(TOKEN_PIECES // 2), range(TOKEN_PIECES // 2, TOKEN_PIECES)
    bottom, top = 0, n_sp - 1

    def second_in():
        z_in(2)
        ring_in(2)

    def first_con():
        z_con(1)
        ring_con(1)

    inner = jnp.logical_not(edge)
    ring_in(0)
    z_in(1)
    ring_in(1)
    pl.when(inner)(second_in)
    ring_in_on(0)
    ring_con(0)

    @pl.when(low)
    def _():
        start_all(own_down())

    @pl.when(high)
    def _():
        start_all(own_up())

    ring_in_on(1)

    @pl.when(edge)
    def _():
        first_con()
        second_in()

    z_in(3)
    ring_in(3)
    start_all(con_copies()[1:])

    @pl.when(high)
    def _():
        start_all(own_down())
        start_all(out_copies()[1:])

    pl.when(inner)(first_con)
    ring_in_on(2)
    relays(low, bottom, 1, early)
    relays(high, top, -1, early)
    relays(low, bottom, 1, late)
    relays(high, top, -1, late)

    @pl.when(jnp.logical_not(high))
    def _():
        start_all(out_copies()[1:])

    @pl.when(low)
    def _():
        start_all(own_up())

    ring_in_on(3)
    ring_con_on(0)
    ring_con_on(1)
    relays(sp == 0, 1, 0)
    relays(sp == top, top - 1, 0)
    z_con(2)
    ring_con(2)
    z_con(3)
    ring_con(3)
    ring_out(0)
    z_out(1)
    ring_out(1)
    relays(low, top - 1, -1)
    relays(high, bottom, 1)
    ring_con_on(2)
    ring_con_on(3)

    late_start = sp < 2
    start = jnp.where(late_start, 1, 0)

    def near_out_on():
        ring_out_on(0)
        ring_out_on(1)
        for k in (2, 3):
            z_out(k)
            ring_out(k)

    pl.when(jnp.logical_not(late_start))(near_out_on)
    arrived(win.at[pl.ds(0, n_sp * rows)], end_f.at[0])
    arrived(rates.at[pl.ds(0, n_sp - 1)], end_f.at[2])

    for h in range(heads):
        state[h] = first_state[h].T
    ext[0:8] = jnp.zeros((8, con), F32)
    lane_rec = pl.ds(pl.multiple_of(sp * rec, rec), rec)
    lane_con = pl.ds(pl.multiple_of(sp * con, con), con)
    row_id = lax.broadcasted_iota(jnp.int32, (span, span), 0)
    col_id = lax.broadcasted_iota(jnp.int32, (span, span), 1)
    causal = row_id >= col_id
    lower = causal.astype(F32)
    upper = (row_id <= col_id).astype(F32)
    length = 2 * span

    def sib_copy(s, c):
        return remote(sib_send.at[s, c], sib_recv.at[s, c], out_sem.at[SIBLING], sib_sem.at[s, c], sibling)

    def final_copy(s, c, to):
        return remote(
            z_send.at[s, c], z_recv.at[sp, c], out_sem.at[SUMS], zr_sem.at[sp], peer(sp=to)
        )

    def joint_copy(s, c, to):
        landing, sem = rl_recv.at[2, c], rl_sem.at[2, c]
        return remote(z_send.at[s, c], landing, out_sem.at[SUMS], sem, peer(sp=to))

    def edge_copy(s, c, to):
        t = lax.rem(s, 2)
        landing, sem = rl_recv.at[t, c], rl_sem.at[t, c]
        return remote(z_send.at[s, c], landing, out_sem.at[SUMS], sem, peer(sp=to))

    def through_low(s):
        return jnp.logical_and(sp == 0, s >= 2)

    def through_high(s):
        return jnp.logical_and(sp == n_sp - 1, s <= n_sp - 3)

    def plain(s):
        return jnp.logical_or(
            jnp.logical_and(sp == 0, s == 1), jnp.logical_and(sp == top, s == top - 1)
        )

    per_slot = n_fs // shards_in

    def pieces_of(slots):
        return [slot * per_slot + i for slot in slots for i in range(per_slot)]

    def own_slots(h):
        return [place(2 * h), place(2 * h + 1)]

    def pass_on(s, h):
        for c in pieces_of(own_slots(h)):
            sib_copy(s, c).wait_recv()
            total = mine[s, c] + sib_recv[s, c].astype(F32)
            mine[s, c] = total

            @pl.when(jnp.logical_and(edge, s != sp))
            def _():
                z_send[s, c] = total.astype(BF16)

            @pl.when(plain(s))
            def _():
                final_copy(s, c, s).start()

            @pl.when(through_low(s))
            def _():
                edge_copy(s, c, 1).start()

            @pl.when(through_high(s))
            def _():
                edge_copy(s, c, n_sp - 2).start()

    def join(t, h):
        s = jnp.where(low, (2, 3, 0)[t], (0, 1, 3)[t])
        to = jnp.where(low, (2, 2, 0)[t], (1, 1, 3)[t])
        rising = low if t < 2 else high
        slots = [jnp.where(rising, 2 * h + i, n_sp - 1 - 2 * h - i) for i in range(2)]
        on = (high, low, None)[t]
        for c in pieces_of(slots):
            arrived(rl_recv.at[t, c], rl_sem.at[t, c])
            z_send[s, c] = (mine[s, c] + rl_recv[t, c].astype(F32)).astype(BF16)
            if on is None:
                final_copy(s, c, to).start()
            else:
                pl.when(on)(joint_copy(s, c, to).start)
                pl.when(jnp.logical_not(on))(final_copy(s, c, to).start)

    def project_out(s, h):
        for slot in own_slots(h):
            columns = jnp.concatenate([wout[slot * n_fs + i] for i in range(n_fs)], axis=1)
            partial = jnp.dot(both[s], columns, preferred_element_type=F32)
            first = partial[:span]
            second = partial[span:]
            own = jnp.where(tp == 0, first, second)
            given = jnp.where(tp == 0, second, first).astype(BF16)
            for i in range(per_slot):
                c = slot * per_slot + i
                mine[s, c] = own[:, i * chunk : (i + 1) * chunk]
                sib_send[s, c] = given[:, i * chunk : (i + 1) * chunk]
                sib_copy(s, c).start()

    def convolve(s):
        block = jnp.concatenate([tokens[2 * s], tokens[2 * s + 1]], axis=0)
        projected = jnp.dot(block, wcon[...], preferred_element_type=F32).astype(BF16).astype(F32)
        prod = projected[:, con : 2 * con] * projected[:, 2 * con :]
        ext[8:] = prod
        conv = jnp.broadcast_to(bias[:, lane_con], prod.shape)
        for j in range(KW):
            conv = conv + taps[j : j + 1, lane_con] * ext[pl.ds(8 - (KW - 1) + j, length)]
        ext[0:8] = ext[length:]
        both[s, :, rec:] = (projected[:, :con] * conv).astype(BF16)

    def recur(s):
        relayed_before = jnp.logical_or(
            (s - sp) * (s - sp) <= 1, jnp.logical_and(sp == 0, s == 2)
        )
        relays(jnp.logical_and(edge, jnp.logical_not(relayed_before)), s, 0)
        arrived(tokens.at[2 * s + other], tok_t.at[s])
        block = jnp.concatenate([tokens[2 * s], tokens[2 * s + 1]], axis=0)

        def project(at, width):
            return jnp.dot(
                block, win[:, pl.ds(at, width)], preferred_element_type=F32
            ).astype(BF16)

        query = project(0, rec).astype(F32) * DK ** (-0.5)
        forget = project(rec, rec).astype(F32)
        value = project(2 * rec, rec)
        key_gate = headroom[:, lane_rec] * jax.nn.sigmoid(-forget)
        log_forget = jnp.log1p(-key_gate)
        gains = gain[:, lane_rec]
        mine_rate = [rates[s, pl.ds(sp * heads + h, 1), :] for h in range(heads)]
        if heads < 8:
            mine_rate.append(jnp.zeros((8 - heads, 2 * span), F32))
        mine_rate = jnp.concatenate(mine_rate, axis=0)
        halves = []
        for c in range(2):
            part = slice(c * span, (c + 1) * span)
            cum = jnp.dot(lower, log_forget[part], precision=lax.Precision.HIGHEST)
            extra = jnp.dot(mine_rate[:, part], upper, precision=lax.Precision.HIGHEST)
            extra_t = extra.T
            grow = jnp.exp(cum)
            query_grow = query[part] * grow
            key_grow = (key_gate[part] / grow).astype(BF16)
            last = cum[span - 1 :, :]
            key_last = key_gate[part] * jnp.exp(last - cum)
            last_decay = jnp.exp(last)
            pieces = []
            for h in range(heads):
                lanes = slice(h * DK, (h + 1) * DK)
                row = extra[h : h + 1]
                column = extra_t[:, h : h + 1]
                end = row[:, span - 1 :]
                scores = lax.dot_general(
                    query_grow[:, lanes].astype(BF16), key_grow[:, lanes], CONTRACT_LAST,
                    preferred_element_type=F32,
                )
                decay = jnp.exp(jnp.where(causal, column - row, 0.0))
                scores = jnp.where(causal, scores * decay, 0.0).astype(BF16)
                values = value[part, lanes]
                before = state[h]
                raw = jnp.dot(scores, values, preferred_element_type=F32)
                raw = raw + lax.dot_general(
                    (query_grow[:, lanes] * jnp.exp(column)).astype(BF16), before.astype(BF16),
                    CONTRACT_LAST, preferred_element_type=F32,
                )
                keys = (key_last[:, lanes] * jnp.exp(end - column)).astype(BF16)
                state[h] = before * (last_decay[:, lanes] * jnp.exp(end)) + lax.dot_general(
                    values, keys, CONTRACT_FIRST, preferred_element_type=F32
                )
                square = jnp.mean(raw * raw, axis=-1, keepdims=True)
                pieces.append((raw * lax.rsqrt(square + 1e-06) * gains[:, lanes]).astype(BF16))
            halves.append(jnp.concatenate(pieces, axis=1))
        both[s, :, :rec] = jnp.concatenate(halves, axis=0)

    def out_end_of(h):
        for k in (2 * h, 2 * h + 1):
            arrived(out_slot(place(k), across), out_end.at[k])

    def give(s, *halves):
        for h in halves:
            project_out(s, h)
        for h in halves:
            pass_on(s, h)

    def step(s, carry):
        recur(s)
        relays(jnp.logical_and(s == 1, sp == 0), 2, 0)
        pl.when(jnp.logical_and(s == 0, late_start))(near_out_on)

        relays(jnp.logical_and(s == 0, high), 1, 1, early)

        @pl.when(s == 2 * start)
        def _():
            ring_out_on(2)
            ring_out_on(3)

        relays(jnp.logical_and(s == 0, high), 1, 1, late)
        relays(jnp.logical_and(s == 1, low), top, -1, early)
        relays(jnp.logical_and(s == 2, low), top, -1, late)

        @pl.when(s == start)
        def _():
            arrived(wcon.at[pl.ds(0, n_sp * rows)], end_f.at[1])
            pl.when(late_start)(functools.partial(convolve, 0))

        pl.when(s >= start)(functools.partial(convolve, s))
        pl.when(jnp.logical_and(s == 3, low))(functools.partial(join, 0, 1))
        pl.when(s == start)(functools.partial(out_end_of, 0))
        others_rows = jnp.logical_and(s >= start, s != sp)
        pl.when(others_rows)(functools.partial(give, s, 0))

        pl.when(s == 2 * start)(functools.partial(out_end_of, 1))
        held = jnp.logical_and(late_start, s == 1)
        pl.when(jnp.logical_and(others_rows, jnp.logical_not(held)))(functools.partial(give, s, 1))

        @pl.when(jnp.logical_and(s == 1, high))
        def _():
            join(0, 0)
            join(0, 1)

        pl.when(jnp.logical_and(s == 2, low))(functools.partial(join, 0, 0))
        return carry

    lax.fori_loop(0, n_sp, step, 0)
    @pl.when(sp == 0)
    def _():
        give(1, 1)
        give(0, 0, 1)

    pl.when(low)(functools.partial(give, 0, 0, 1))


    pl.when(sp > 0)(functools.partial(give, sp, 0, 1))

    @pl.when(low)
    def _():
        for h in range(2):
            join(1, h)
            join(2, h)

    @pl.when(high)
    def _():
        for h in range(2):
            join(1, h)
        for h in range(2):
            join(2, h)

    for d in range(n_sp):
        comes = (sp - d) * (sp - d) == 1

        @pl.when(comes)
        def _():
            arrived(z_recv.at[d], zr_sem.at[d])
            for c in range(chunks):
                mine[sp, c] = mine[sp, c] + z_recv[d, c].astype(F32)

    for c in range(chunks):
        out[:, c * chunk : (c + 1) * chunk] = mine[sp, c].astype(BF16)

    gone(rates.at[pl.ds(0, n_sp - 1)], RATE)
    gone(win.at[pl.ds(0, (n_sp - 1) * rows)], FIRST)
    gone(wcon.at[pl.ds(0, (n_sp - 1) * rows)], CON)
    gone(wout.at[pl.ds(0, n_sp - 1)], OUT)
    gone(win.at[pl.ds(0, 3 * n_sp * rows)], IN_RING)
    gone(wcon.at[pl.ds(0, 3 * n_sp * rows)], CON_RING)
    gone(wout.at[pl.ds(0, 3 * n_sp)], OUT_RING)
    gone(tokens.at[pl.ds(0, n_sp)], ACROSS)
    gone(sib_send, SIBLING)
    gone(z_send.at[pl.ds(0, n_sp - 1)], SUMS)

    @pl.when(sp < n_sp - 1)
    def _():
        gone(tokens.at[0], UP)

    @pl.when(sp > 0)
    def _():
        gone(tokens.at[0], DOWN)

    @pl.when(inner)
    def _():
        gone(tokens.at[pl.ds(0, n_sp - 1)], RELAY)


def sequence_shards(n_sp, n_fs, *arrays):
    (tok, wq, wf, wv, cg, cm, ci, headroom, rate, init, gain, taps, bias, ro, co) = arrays
    span, wide = tok.shape[1:]
    rec, con = wq.shape[1] // n_sp, cg.shape[1] // n_sp
    heads = rec // DK
    chunk = wide // OUT_PIECES
    hbm = pl.BlockSpec(memory_space=pl.ANY)
    vmem = pl.BlockSpec(memory_space=pltpu.VMEM)
    dma = pltpu.SemaphoreType.DMA
    flat = (n_sp, OUT_PIECES, span, chunk)
    mixed = pl.pallas_call(
        functools.partial(layer_kernel, n_sp, n_fs),
        out_shape=pltpu.VMEM((span, wide), BF16),
        in_specs=[hbm] * 15,
        out_specs=vmem,
        scratch_shapes=[
            pltpu.VMEM((1, headroom.shape[0]), F32),
            pltpu.VMEM((1, gain.shape[0]), F32),
            pltpu.VMEM(taps.shape, F32),
            pltpu.VMEM((1, bias.shape[0]), F32),
            pltpu.VMEM((2 * n_sp, span, wide), BF16),
            pltpu.VMEM((wide, 3 * rec), BF16),
            pltpu.VMEM((wide, 3 * con), BF16),
            pltpu.VMEM((n_sp * n_fs, rec + con, wide // (n_sp * n_fs)), BF16),
            pltpu.VMEM((n_sp,) + rate.shape[1:], F32),
            pltpu.VMEM((heads, DK, DK), F32),
            pltpu.VMEM((heads, DK, DK), F32),
            pltpu.VMEM((8 + 2 * span, con), F32),
            pltpu.VMEM((n_sp, 2 * span, rec + con), BF16),
            pltpu.VMEM(flat, BF16),
            pltpu.VMEM(flat, BF16),
            pltpu.VMEM(flat, F32),
            pltpu.VMEM(flat, BF16),
            pltpu.VMEM(flat, BF16),
            pltpu.VMEM((3,) + flat[1:], BF16),
            pltpu.VMEM((n_sp, wide // (n_sp * n_fs), 3 * rec), BF16),
            pltpu.VMEM((n_sp, wide // (n_sp * n_fs), 3 * con), BF16),
            pltpu.VMEM((n_sp, rec + con, wide // (n_sp * n_fs)), BF16),
            dma((n_sp,)),
            dma((9,)),
            dma((SENDS,)),
            dma((n_sp,)),
            dma((n_sp,)),
            dma((n_sp,)),
            dma((2, n_sp)),
            dma((2, n_sp)),
            dma((2, n_sp)),
            dma((n_sp,)),
            dma((3,)),
            dma((n_sp, TOKEN_PIECES)),
            dma((n_sp,)),
            dma((n_sp, OUT_PIECES)),
            dma((n_sp,)),
            dma((3, OUT_PIECES)),
        ],
        compiler_params=pltpu.CompilerParams(
            collective_id=0, has_side_effects=True, vmem_limit_bytes=60 * 2**20
        ),
    )(
        tok[0], wq, wf, wv, cg, cm, ci, ro, co, rate[0], init[0], headroom[None], gain[None],
        taps, bias[None],
    )
    return mixed[None]


def choose_plan(sizes, *arrays):
    n_sp, n_fs = sizes["sp"], sizes["fs"]
    rows, rec = arrays[1].shape
    con = arrays[4].shape[1]
    span = arrays[0].shape[1]
    even = (
        sizes["tp"] == 2
        and n_fs == 4
        and n_sp == 4
        and arrays[0].shape[2] % (n_fs * n_sp * 128) == 0
        and arrays[0].shape[0] == 1
        and rec % (n_sp * DK) == 0
        and rec // (n_sp * DK) <= 8
        and arrays[8].shape[1] % 8 == 0
        and con % (n_sp * 128) == 0
        and rows % 128 == 0
        and span == DK
        and arrays[13].shape[1] % 128 == 0
    )
    return sequence_shards(n_sp, n_fs, *arrays) if even else shards(*arrays)


def solution(mesh):
    in_specs = (
        P("fs", ("sp", "tp"), None),
        P(("sp", "fs"), "tp"),
        P(("sp", "fs"), "tp"),
        P(("sp", "fs"), "tp"),
        P(("sp", "fs"), "tp"),
        P(("sp", "fs"), "tp"),
        P(("sp", "fs"), "tp"),
        P("tp"),
        P("fs", "tp", "sp"),
        P("fs", "tp", None, None),
        P("tp"),
        P(None, "tp"),
        P("tp"),
        P("tp", ("sp", "fs")),
        P("tp", ("sp", "fs")),
    )
    out_specs = P("fs", ("sp", "tp"), None)
    body = functools.partial(choose_plan, dict(mesh.shape))
    return jax.shard_map(body, mesh=mesh, in_specs=in_specs, out_specs=out_specs, check_vma=False)
```
